32 devices in a mesh: sp: 8 (over z, x), tp: 4 (over y, core).
Axes of the slice: x: 2, y: 2, z: 4, core: 2. Of those that a mesh axis runs over, the one named last changes fastest.
Arguments:
- residual: bfloat16 [4096, 2048], P('sp'), may hold values from -6 to 6
- queries: bfloat16 [4096, 1024], P('sp', 'tp'), may hold values from -384 to 384
- key_pairs: bfloat16 [4096, 1024], P('sp', 'tp'), may hold values from -384 to 384
- values: bfloat16 [4096, 1024], P('sp', 'tp'), may hold values from -6 to 6
- lambdas: float32 [8], P('tp'), may hold values from 0.3 to 0.8
- head_gain: float32 [128], replicated, may hold values from 0.1 to 1.9
- w_out: bfloat16 [1024, 2048], replicated, may hold values from -0.1875 to 0.1875
- norm_gain: float32 [2048], replicated, may hold values from 0.1 to 1.9
- w_gate: bfloat16 [2048, 5632], P('sp', 'tp'), may hold values from -0.125 to 0.125
- w_up: bfloat16 [2048, 5632], P('sp', 'tp'), may hold values from -0.125 to 0.125
- w_down: bfloat16 [5632, 2048], P('tp', 'sp'), may hold values from -0.078125 to 0.078125
Outputs:
- layer_out: bfloat16 [4096, 2048], P(('sp', 'tp'))
The draws below stay inside these ranges and needn't reach their ends.
All inputs are finite; a program needn't handle non-finite values.
Results may differ from the reference program's by a relative error of at most 0.018.
Values may be sent and summed in bfloat16 or wider, within the bound.
A program may use at most 128 MiB of HBM per device.

```python
import math
import jax
import jax.numpy as jnp
from jax import lax

D = 2048
HEADS = 8
HD = 64
VD = 128
FF = 5632
SEQ = 4096
N_TP = 4


def drawn_pair(key):
    query_key, pair_key = jax.random.split(jax.random.fold_in(key, 11), 2)
    query_draw = jnp.clip(jax.random.normal(query_key, (SEQ, HEADS, 2, HD), jnp.float32), -6.0, 6.0) * 1.3
    key_draw = jnp.clip(jax.random.normal(pair_key, (SEQ, HEADS, 2, HD), jnp.float32), -6.0, 6.0) * 1.3
    return (query_draw.reshape(SEQ, HEADS * 2 * HD), key_draw.reshape(SEQ, HEADS * 2 * HD))


def draw_queries(key, part):
    return drawn_pair(key)[0].astype(jnp.bfloat16)


def draw_key_pairs(key, part):
    return drawn_pair(key)[1].astype(jnp.bfloat16)


def shard_levels(rng, dims, cuts, low, top_value):
    def one(position, blocks):
        draws = jax.random.uniform(jax.random.fold_in(jax.random.fold_in(rng, 6), position), (blocks,), jnp.float32, low / len(cuts), top_value / len(cuts))
        return jnp.repeat(jnp.exp(draws), dims[position] // blocks).reshape((-1,) + (1,) * (len(dims) - position - 1))

    factor_of = one(*cuts[0])
    for cut in cuts[1:]:
        factor_of = factor_of * one(*cut)
    return factor_of


def scatter_about(own_key, shape, deviation, bound, cuts=(), kind=jnp.bfloat16):
    loudness = shard_levels(own_key, shape, cuts, -0.22, 0.18) if cuts else 1.0
    result = jax.random.normal(own_key, shape, jnp.float32) * deviation * loudness
    return jnp.minimum(jnp.maximum(result, -bound), bound).astype(kind)


def setup_inputs(seed: int = 0) -> dict:
    arg_keys = jax.random.split(jax.random.key(seed), 12)
    residual = scatter_about(arg_keys[0], (SEQ, D), 1.0, 6.0, ((0, 8),))
    queries = draw_queries(jax.random.fold_in(arg_keys[11], 71), 0)
    key_pairs = draw_key_pairs(jax.random.fold_in(arg_keys[11], 71), 0)
    values = scatter_about(arg_keys[3], (SEQ, HEADS * VD), 1.0, 6.0, ((0, 8), (1, 4)))
    lambdas = jnp.clip(0.3 + 0.5 * jax.random.uniform(arg_keys[4], (HEADS,), jnp.float32) ** shard_levels(arg_keys[4], (HEADS,), ((0, 4),), -0.2, 0.2), 0.3, 0.8)
    head_gain = jnp.clip(1.0 + 0.18 * jax.random.normal(arg_keys[5], (VD,), jnp.float32), 0.1, 1.9)
    w_out = scatter_about(arg_keys[6], (HEADS * VD, D), (HEADS * VD) ** -0.5, 0.1875)
    norm_gain = jnp.clip(1.0 + 0.18 * jax.random.normal(arg_keys[7], (D,), jnp.float32), 0.1, 1.9)
    w_gate = scatter_about(arg_keys[8], (D, FF), D ** -0.5, 0.125, ((0, 8), (1, 4)))
    w_up = scatter_about(arg_keys[9], (D, FF), D ** -0.5, 0.125, ((0, 8), (1, 4)))
    w_down = scatter_about(arg_keys[10], (FF, D), FF ** -0.5, 0.078125, ((0, 4), (1, 8)))
    return {"residual": residual, "queries": queries, "key_pairs": key_pairs, "values": values, "lambdas": lambdas, "head_gain": head_gain, "w_out": w_out, "norm_gain": norm_gain, "w_gate": w_gate, "w_up": w_up, "w_down": w_down}


def reference(residual, queries, key_pairs, values, lambdas, head_gain, w_out, norm_gain, w_gate, w_up, w_down):
    score_scale = HD ** (-0.5)
    value_width = 2 * HD
    key_all = key_pairs.reshape(SEQ, HEADS, 2, HD).astype(jnp.float32)
    value_all = values.reshape(SEQ, HEADS, value_width).astype(jnp.float32)
    query_rows = math.gcd(SEQ, 256)

    def attend(query_block):
        scores = jnp.einsum('qhmd,khmd->hmqk', query_block.astype(jnp.float32), key_all) * score_scale
        highest = lax.optimization_barrier(jnp.max(scores, axis=-1, keepdims=True))
        weights = jnp.exp(scores - highest)
        totals = lax.optimization_barrier(jnp.sum(weights, axis=-1))
        rounded = lax.optimization_barrier(weights.astype(jnp.bfloat16)).astype(jnp.float32)
        mixture = jnp.einsum('hmqk,khe->hmqe', rounded, value_all) / totals[..., None]
        differ = mixture[:, 0] - lambdas[:, None, None] * mixture[:, 1]
        normed_heads = differ * lax.rsqrt(lax.optimization_barrier(jnp.mean(differ * differ, axis=-1, keepdims=True)) + 1e-05) * head_gain
        return jnp.transpose(normed_heads, (1, 0, 2)).reshape(query_rows, HEADS * value_width).astype(jnp.bfloat16)
    query_blocks = queries.reshape(SEQ // query_rows, query_rows, HEADS, 2, HD)
    heads_out = lax.map(attend, query_blocks).reshape(SEQ, HEADS * value_width)
    projected = jnp.dot(heads_out, w_out, preferred_element_type=jnp.float32)
    hidden_state = (residual.astype(jnp.float32) + projected).astype(jnp.bfloat16)
    stream_f = hidden_state.astype(jnp.float32)
    normed = (stream_f * lax.rsqrt(lax.optimization_barrier(jnp.mean(stream_f * stream_f, axis=-1, keepdims=True)) + 1e-05) * norm_gain).astype(jnp.bfloat16)
    group_width = FF // N_TP
    summed = jnp.zeros((SEQ, D), jnp.float32)
    for member in range(N_TP):
        lower = member * group_width
        gate_part = jnp.dot(normed, w_gate[:, lower:lower + group_width], preferred_element_type=jnp.float32)
        up_part = jnp.dot(normed, w_up[:, lower:lower + group_width], preferred_element_type=jnp.float32)
        hidden_part = (jax.nn.silu(gate_part) * up_part).astype(jnp.bfloat16)
        partial_sum = jnp.dot(hidden_part, w_down[lower:lower + group_width], preferred_element_type=jnp.float32)
        summed = summed + lax.optimization_barrier(partial_sum.astype(jnp.bfloat16)).astype(jnp.float32)
    return (stream_f + summed).astype(jnp.bfloat16)
```

```python
import functools

import jax
import jax.numpy as jnp
import numpy as np
from jax import lax
from jax.experimental import pallas as pl
from jax.experimental.pallas import tpu as pltpu
from jax.sharding import Mesh, PartitionSpec as P

HD = 64


def attend_chunk(q, k, v, m_ref, l_ref, acc_ref, slot, rows):
    scores = lax.dot_general(
        q, k, (((1,), (1,)), ((), ())), preferred_element_type=jnp.float32
    )
    old = m_ref[slot, rows, :]
    high = jnp.maximum(old, jnp.max(scores, axis=1, keepdims=True))
    shrink = jnp.exp(old - high)
    weights = jnp.exp(scores - high[:, :1])
    l_ref[slot, rows, :] = l_ref[slot, rows, :] * shrink + jnp.sum(weights, axis=1, keepdims=True)
    m_ref[slot, rows, :] = high
    acc_ref[slot, rows, :] = acc_ref[slot, rows, :] * shrink + jnp.dot(
        weights.astype(jnp.bfloat16), v, preferred_element_type=jnp.float32
    )


def finish_heads(heads, width, lam_ref, gain_ref, l_ref, acc_ref, out_ref):
    for h in range(heads):
        first = acc_ref[2 * h] / l_ref[2 * h]
        second = acc_ref[2 * h + 1] / l_ref[2 * h + 1]
        differ = first - lam_ref[h] * second
        scale = lax.rsqrt(jnp.mean(differ * differ, axis=1, keepdims=True) + 1e-05)
        out_ref[:, h * width : (h + 1) * width] = (differ * scale * gain_ref[...]).astype(out_ref.dtype)


def nearest(k, me, n):
    low, high = me, n - 1 - me
    edge = jnp.minimum(low, high)
    side = jnp.where(high >= low, 1, -1)
    near = jnp.where(k % 2 == 1, 1, -1) * ((k + 1) // 2)
    off = side * jnp.where(k <= 2 * edge, near, k - edge)
    return me + off, off


def gather_attend_kernel(
    nz, nx, heads, block,
    lam_ref, q_ref, kv_ref, gain_ref, pair_ref, down_ref,
    out_ref, pair_out, down_out,
    kv_all, m_ref, l_ref, acc_ref,
    up_sem, low_sem, side_sem, kv_sem, pz_sem, dz_sem, px_sem, dx_sem, p_sem, d_sem,
):
    z, x = lax.axis_index("z"), lax.axis_index("x")
    rows_all = q_ref.shape[0]
    width = out_ref.shape[1] // heads
    keys = heads * 2 * HD
    depth = pair_ref.shape[2]

    def remote(src, dst, send, recv, zz, xx):
        return pltpu.make_async_remote_copy(
            src_ref=src, dst_ref=dst, send_sem=send, recv_sem=recv,
            device_id={"z": zz, "x": xx}, device_id_type=pl.DeviceIdType.MESH,
        )

    barrier = pltpu.get_barrier_semaphore()
    for a in range(nz):
        for b in range(nx):
            if a + b > 0:
                pl.semaphore_signal(
                    barrier, inc=1,
                    device_id={"z": lax.rem(z + a, nz), "x": lax.rem(x + b, nx)},
                    device_id_type=pl.DeviceIdType.MESH,
                )
    pl.semaphore_wait(barrier, nz * nx - 1)

    def slot(zz, xx):
        return zz * nx + xx

    def flow(src, k, zz, go):
        off = zz - z
        here = kv_all.at[slot(zz, x)]

        @pl.when(jnp.logical_and(off <= 0, z < nz - 1))
        def _():
            go(remote(src, here, up_sem.at[k], kv_sem.at[slot(zz, x)], jnp.minimum(z + 1, nz - 1), x))

        @pl.when(jnp.logical_and(off >= 0, z > 0))
        def _():
            go(remote(src, here, low_sem.at[k], kv_sem.at[slot(zz, x)], jnp.maximum(z - 1, 0), x))

        for e in range(1, nx):
            go(remote(src, here, side_sem.at[e - 1, k], kv_sem.at[slot(zz, x)], z, lax.rem(x + e, nx)))

    def pair_place(s):
        return pair_out.at[:, pl.ds(pl.multiple_of(s * depth, depth), depth), :]

    def along(d, go):
        to = lax.rem(z + d, nz)
        s = slot(z, x)
        go(remote(pair_ref.at[to], pair_place(s), pz_sem.at[d], p_sem.at[s], to, x))
        go(remote(down_ref.at[to], down_out.at[s], dz_sem.at[d], d_sem.at[s], to, x))

    def across(src_pair, src_down, d, s, go):
        for e in range(1, nx):
            to = lax.rem(x + e, nx)
            go(remote(src_pair, pair_place(s), px_sem.at[e - 1, d], p_sem.at[s], z, to))
            go(remote(src_down, down_out.at[s], dx_sem.at[e - 1, d], d_sem.at[s], z, to))

    def arrived(src_pair, src_down, s):
        remote(src_pair, pair_place(s), pz_sem.at[0], p_sem.at[s], z, x).wait_recv()
        remote(src_down, down_out.at[s], dz_sem.at[0], d_sem.at[s], z, x).wait_recv()

    start = lambda copy: copy.start()
    sent = lambda copy: copy.wait_send()

    flow(kv_ref, 0, z, start)
    mine = slot(z, x)
    pair_out[:, pl.ds(pl.multiple_of(mine * depth, depth), depth), :] = pair_ref[z]
    down_out[mine] = down_ref[z]
    kv_all[mine] = kv_ref[...]
    m_ref[...] = jnp.full_like(m_ref, -jnp.inf)
    l_ref[...] = jnp.zeros_like(l_ref)
    acc_ref[...] = jnp.zeros_like(acc_ref)

    def attend(s):
        for h in range(heads):
            v = kv_all[s, :, keys + h * width : keys + (h + 1) * width]
            for m in range(2):
                lane = (2 * h + m) * HD
                k = kv_all[s, :, lane : lane + HD]
                for r in range(0, rows_all, block):
                    rows = pl.ds(r, block)
                    q = q_ref[rows, lane : lane + HD] * jnp.bfloat16(HD**-0.5)
                    attend_chunk(q, k, v, m_ref, l_ref, acc_ref, 2 * h + m, rows)

    def step(k, _):
        zz, _off = nearest(k, z, nz)
        here = kv_all.at[slot(zz, x)]

        @pl.when(k > 0)
        def _():
            remote(kv_ref, here, up_sem.at[k], kv_sem.at[slot(zz, x)], z, x).wait_recv()
            flow(here, k, zz, start)

        @pl.when(k == min(1, nz - 1))
        def _():
            for d in range(1, nz):
                along(d, start)
            across(pair_ref.at[z], down_ref.at[z], 0, mine, start)

        def column(e, _):
            other = lax.rem(x - e + nx, nx)

            @pl.when(e > 0)
            def _():
                remote(kv_ref, here, up_sem.at[k], kv_sem.at[slot(zz, other)], z, x).wait_recv()

            attend(slot(zz, other))
            return 0

        lax.fori_loop(0, nx, column, 0)
        return 0

    lax.fori_loop(0, nz, step, 0)
    for d in range(1, nz):
        zz = lax.rem(z - d + nz, nz)
        s = slot(zz, x)
        arrived(pair_ref.at[z], down_ref.at[z], s)
        across(pair_place(s), down_out.at[s], d, s, start)
    finish_heads(heads, width, lam_ref, gain_ref, l_ref, acc_ref, out_ref)
    for d in range(nz):
        zz = lax.rem(z - d + nz, nz)
        for e in range(1, nx):
            arrived(pair_ref.at[z], down_ref.at[z], slot(zz, lax.rem(x - e + nx, nx)))
    for d in range(nz):
        zz = lax.rem(z - d + nz, nz)
        s = slot(zz, x)
        across(pair_place(s), down_out.at[s], d, s, sent)
        if d:
            along(d, sent)

    def settle(k, _):
        zz, _off = nearest(k, z, nz)
        flow(kv_ref, k, zz, sent)
        return 0

    lax.fori_loop(0, nz, settle, 0)


def gather_attend(nz, nx, queries, kv, lambdas, head_gain, pairs, downs):
    rows = queries.shape[0]
    heads = lambdas.shape[0]
    width = head_gain.shape[0]
    _, _, depth, mine = pairs.shape
    blocks = nz * nx
    vmem = pl.BlockSpec(memory_space=pltpu.VMEM)
    dma = pltpu.SemaphoreType.DMA
    side = max(nx - 1, 1)
    return pl.pallas_call(
        functools.partial(gather_attend_kernel, nz, nx, heads, 256),
        out_shape=[
            jax.ShapeDtypeStruct((rows, heads * width), jnp.bfloat16),
            jax.ShapeDtypeStruct((2, blocks * depth, mine), jnp.bfloat16),
            jax.ShapeDtypeStruct((blocks,) + downs.shape[1:], jnp.bfloat16),
        ],
        in_specs=[pl.BlockSpec(memory_space=pltpu.SMEM)] + [vmem] * 5,
        out_specs=[vmem] * 3,
        scratch_shapes=[pltpu.VMEM((blocks,) + kv.shape, jnp.bfloat16)]
        + [pltpu.VMEM((2 * heads, rows, width), jnp.float32)] * 3
        + [
            dma((nz,)), dma((nz,)), dma((side, nz)), dma((blocks,)),
            dma((nz,)), dma((nz,)), dma((side, nz)), dma((side, nz)), dma((blocks,)), dma((blocks,)),
        ],
        compiler_params=pltpu.CompilerParams(
            collective_id=0, has_side_effects=True, vmem_limit_bytes=60 * 1024 * 1024
        ),
        cost_estimate=pl.CostEstimate(
            flops=rows * rows * blocks * heads * 4096, bytes_accessed=4000000, transcendentals=0
        ),
        name="gather_attend",
    )(lambdas, queries, kv, head_gain.reshape(1, width), pairs, downs)


def gather_rows_kernel(nz, nt, own_ref, out_ref, up_sem, low_sem, y_sem, c_sem, got_sem):
    z, t = lax.axis_index("z"), lax.axis_index("tp")
    rows = own_ref.shape[0]
    partner = t + 1 - 2 * lax.rem(t, 2)

    barrier = pltpu.get_barrier_semaphore()
    for a in range(nz):
        for b in range(nt):
            if a + b > 0:
                pl.semaphore_signal(
                    barrier, inc=1,
                    device_id={"z": lax.rem(z + a, nz), "tp": lax.rem(t + b, nt)},
                    device_id_type=pl.DeviceIdType.MESH,
                )
    pl.semaphore_wait(barrier, nz * nt - 1)

    def place(zz, tt):
        s = zz * nt + tt
        return out_ref.at[pl.ds(pl.multiple_of(s * rows, rows), rows), :], got_sem.at[s]

    def remote(src, zz, tt, send, to_z, to_t):
        dst, recv = place(zz, tt)
        return pltpu.make_async_remote_copy(
            src_ref=src, dst_ref=dst, send_sem=send, recv_sem=recv,
            device_id={"z": to_z, "tp": to_t}, device_id_type=pl.DeviceIdType.MESH,
        )

    def flow(src, k, zz, go):
        @pl.when(jnp.logical_and(zz <= z, z < nz - 1))
        def _():
            go(remote(src, zz, t, up_sem.at[k], jnp.minimum(z + 1, nz - 1), t))

        @pl.when(jnp.logical_and(zz >= z, z > 0))
        def _():
            go(remote(src, zz, t, low_sem.at[k], jnp.maximum(z - 1, 0), t))

        for e in range(1, nt // 2):
            go(remote(src, zz, t, y_sem.at[k, e], z, lax.rem(t + 2 * e, nt)))
        go(remote(src, zz, t, c_sem.at[k, 0], z, partner))

    start = lambda copy: copy.start()
    sent = lambda copy: copy.wait_send()

    def await_block(zz, tt):
        remote(own_ref, zz, tt, c_sem.at[0, 0], z, partner).wait_recv()

    flow(own_ref, 0, z, start)
    mine, _sem = place(z, t)
    mine[...] = own_ref[...]

    def same_core(e):
        return lax.rem(t - 2 * e + nt, nt)

    def step(k, _):
        zz, _off = nearest(k, z, nz)

        @pl.when(k > 0)
        def _():
            await_block(zz, t)
            flow(place(zz, t)[0], k, zz, start)

        for e in range(1, nt // 2):
            tt = same_core(e)
            await_block(zz, tt)
            remote(place(zz, tt)[0], zz, tt, c_sem.at[k, e], z, partner).start()
        return 0

    lax.fori_loop(0, nz, step, 0)

    def settle(k, _):
        zz, _off = nearest(k, z, nz)
        flow(own_ref, k, zz, sent)
        for e in range(nt // 2):
            await_block(zz, lax.rem(partner - 2 * e + nt, nt))
            if e:
                tt = same_core(e)
                remote(own_ref, zz, tt, c_sem.at[k, e], z, partner).wait_send()
        return 0

    lax.fori_loop(0, nz, settle, 0)


def gather_rows(nz, nt, own):
    rows, width = own.shape
    if nt % 2:
        return lax.all_gather(own, ("z", "tp"), axis=0, tiled=True)
    vmem = pl.BlockSpec(memory_space=pltpu.VMEM)
    dma = pltpu.SemaphoreType.DMA
    return pl.pallas_call(
        functools.partial(gather_rows_kernel, nz, nt),
        out_shape=jax.ShapeDtypeStruct((nz * nt * rows, width), own.dtype),
        in_specs=[vmem],
        out_specs=vmem,
        scratch_shapes=[dma((nz,)), dma((nz,)), dma((nz, nt // 2)), dma((nz, nt // 2)), dma((nz * nt,))],
        compiler_params=pltpu.CompilerParams(
            collective_id=1, has_side_effects=True, vmem_limit_bytes=32 * 1024 * 1024
        ),
        cost_estimate=pl.CostEstimate(flops=10**10, bytes_accessed=4000000, transcendentals=0),
        name="gather_rows",
    )(own)


def per_device(
    nz, nx, residual, queries, key_pairs, values, lambdas, head_gain, w_out, norm_gain, w_gate, w_up, w_down
):
    local_rows = queries.shape[0]
    heads_here = lambdas.shape[0]
    value_width = head_gain.shape[0]
    d_rows, units = w_gate.shape
    mine = units // nz
    width = residual.shape[1]

    kv = jnp.concatenate([key_pairs, values], axis=1)
    pairs = jnp.stack([w_gate.reshape(d_rows, nz, mine), w_up.reshape(d_rows, nz, mine)], axis=2)
    pairs = jnp.transpose(pairs, (1, 2, 0, 3))
    heads_out, both, downs = gather_attend(
        nz, nx, queries, kv, lambdas, head_gain, pairs, w_down.reshape(nz, mine, w_down.shape[1])
    )
    gate, up = both[0], both[1]
    down = jnp.transpose(downs, (1, 0, 2)).reshape(mine, width)
    tp_index = lax.axis_index("tp")
    own_rows = local_rows // lax.axis_size("tp")
    w_mine = lax.dynamic_slice_in_dim(
        w_out, tp_index * heads_here * value_width, heads_here * value_width, 0
    )
    projected = lax.psum_scatter(
        jnp.dot(heads_out, w_mine, preferred_element_type=jnp.float32).astype(jnp.bfloat16),
        "tp",
        scatter_dimension=0,
        tiled=True,
    ).astype(jnp.float32)
    residual_own = lax.dynamic_slice_in_dim(residual, tp_index * own_rows, own_rows, 0)
    hidden_own = (residual_own.astype(jnp.float32) + projected).astype(jnp.bfloat16)
    stream_f = hidden_own.astype(jnp.float32)
    scaled = stream_f * lax.rsqrt(jnp.mean(stream_f * stream_f, axis=-1, keepdims=True) + 1e-05)
    normed_rows = gather_rows(nz, lax.axis_size("tp"), (scaled * norm_gain).astype(jnp.bfloat16))
    gate_sum = jnp.dot(normed_rows, gate, preferred_element_type=jnp.float32)
    up_sum = jnp.dot(normed_rows, up, preferred_element_type=jnp.float32)
    hidden_units = (jax.nn.silu(gate_sum) * up_sum).astype(jnp.bfloat16)
    ffn_out = lax.psum_scatter(
        jnp.dot(hidden_units, down, preferred_element_type=jnp.float32).astype(jnp.bfloat16),
        ("z", "tp"),
        scatter_dimension=0,
        tiled=True,
    ).astype(jnp.float32)
    return (hidden_own.astype(jnp.float32) + ffn_out).astype(jnp.bfloat16)


def layer_kernel(
    nz, nx, ny, nc,
    lam_ref, q_ref, k_ref, v_ref, gain_ref, norm_ref, res_ref, wout_ref, wg_ref, wu_ref, wd_ref,
    out_ref,
    q_all, qm, kv, vt, m_ref, l_ref, acc, ho, hg, wout, res, hidden, xs, wgu, wd, hb, part, r1, r2, r3,
    q_sem, kx_sem, up_sem, low_sem, kv_sem,
    gs_sem, gr_sem, gp_sem, gq_sem, ds_sem, dr_sem, dp_sem, dq_sem,
    hs_sem, hr_sem, in_sem, xs_sem, xr_sem, rs_sem, rr_sem,
):
    z, x = lax.axis_index("z"), lax.axis_index("x")
    y, c = lax.axis_index("y"), lax.axis_index("c")
    z0 = lax.rem(z, 2)
    tokens = q_ref.shape[0]
    wide = v_ref.shape[1] // nx
    own_rows, width = out_ref.shape
    depth = wg_ref.shape[0]
    units, quarter = wg_ref.shape[1], wgu.shape[3]
    tp = y * nc + c
    xo, co = 1 - x, 1 - c
    here = dict(z=z, x=x, y=y, c=c)

    def remote(src, dst, send, recv, **to):
        return pltpu.make_async_remote_copy(
            src_ref=src, dst_ref=dst, send_sem=send, recv_sem=recv,
            device_id={**here, **to}, device_id_type=pl.DeviceIdType.MESH,
        )

    def lanes(i, n):
        return pl.ds(pl.multiple_of(i * n, n), n)

    local_in = [
        pltpu.make_async_copy(wout_ref, wout, in_sem.at[0]),
        pltpu.make_async_copy(res_ref.at[lanes(tp, own_rows), :], res, in_sem.at[1]),
    ]
    for copy in local_in:
        copy.start()

    barrier = pltpu.get_barrier_semaphore()
    peers = [dict(z=lax.rem(z + a, nz), x=lax.rem(x + b, nx)) for a in range(nz) for b in range(nx) if a + b]
    peers += [
        dict(x=lax.rem(x + b, nx), y=lax.rem(y + e, ny), c=lax.rem(c + f, nc))
        for b in range(nx) for e in range(ny) for f in range(nc) if e + f
    ]
    for to in peers:
        pl.semaphore_signal(barrier, inc=1, device_id={**here, **to}, device_id_type=pl.DeviceIdType.MESH)
    pl.semaphore_wait(barrier, len(peers))

    start = lambda copy: copy.start()
    sent = lambda copy: copy.wait_send()

    def slot(zz, xx):
        return zz * nx + xx

    mine = slot(z, x)

    def swap(go):
        go(remote(q_ref.at[:, lanes(xo, wide)], q_all.at[x], q_sem.at[0], q_sem.at[1], x=xo))
        go(remote(k_ref.at[:, lanes(xo, wide)], kv.at[mine, 0], kx_sem.at[0], kv_sem.at[mine], x=xo))
        go(remote(v_ref.at[:, lanes(xo, wide)], kv.at[mine, 1], kx_sem.at[1], kv_sem.at[mine], x=xo))

    def up_down(zz, go_up, go_low):
        @pl.when(jnp.logical_and(zz <= z, z < nz - 1))
        def _():
            go_up(jnp.minimum(z + 1, nz - 1))

        @pl.when(jnp.logical_and(zz >= z, z > 0))
        def _():
            go_low(jnp.maximum(z - 1, 0))

    def own_flow(sem, to):
        for i, ref in enumerate((k_ref, v_ref)):
            remote(ref.at[:, lanes(x, wide)], kv.at[mine, i], sem.at[mine], kv_sem.at[mine], z=to).start()

    def flow(s, zz, go):
        up_down(
            zz,
            lambda to: go(remote(kv.at[s], kv.at[s], up_sem.at[s], kv_sem.at[s], z=to)),
            lambda to: go(remote(kv.at[s], kv.at[s], low_sem.at[s], kv_sem.at[s], z=to)),
        )

    def offset(q):
        return pl.multiple_of(jnp.minimum(q * quarter, units - quarter), 128)

    def target(j):
        return lax.rem(z + j // nx, nz), lax.rem(x + lax.rem(j, nx), nx)

    def gate_up(j, go):
        zd, xd = target(j)
        cols = pl.ds(offset(xd * 2 + lax.rem(zd, 2)), quarter)
        rows = lanes(mine, depth)
        for i, ref in enumerate((wg_ref, wu_ref)):
            go(remote(ref.at[:, cols], wgu.at[c, i, rows, :], gs_sem.at[j, i], gr_sem.at[mine], z=zd, x=xd))

    def downward(j, go):
        zd, xd = target(j)
        rows = pl.ds(offset(xd * 2 + lax.rem(zd, 2)), quarter)
        go(remote(wd_ref.at[rows, :], wd.at[c, :, lanes(mine, depth)], ds_sem.at[j], dr_sem.at[mine], z=zd, x=xd))

    q_me = x * 2 + z0
    own_weights = [
        pltpu.make_async_copy(ref.at[:, pl.ds(offset(q_me), quarter)], wgu.at[c, i, lanes(mine, depth), :], in_sem.at[2 + i])
        for i, ref in enumerate((wg_ref, wu_ref))
    ]
    own_weights.append(
        pltpu.make_async_copy(wd_ref.at[pl.ds(offset(q_me), quarter), :], wd.at[c, :, lanes(mine, depth)], in_sem.at[4])
    )

    swap(start)
    up_down(z, lambda to: own_flow(up_sem, to), lambda to: own_flow(low_sem, to))
    for copy in own_weights:
        copy.start()

    kv[mine, 0] = k_ref[:, lanes(x, wide)]
    kv[mine, 1] = v_ref[:, lanes(x, wide)]
    q_all[x] = q_ref[:, lanes(x, wide)]
    m_ref[...] = jnp.full_like(m_ref, -jnp.inf)
    l_ref[...] = jnp.zeros_like(l_ref)
    acc[...] = jnp.zeros_like(acc)

    remote(q_all.at[x], q_all.at[xo], q_sem.at[0], q_sem.at[1], x=xo).wait_recv()
    first_map = lax.broadcasted_iota(jnp.int32, (tokens, 2 * HD), 1) < HD
    for h in range(nx):
        q = q_all[h].astype(jnp.float32) * HD**-0.5
        qm[2 * h] = jnp.where(first_map, q, 0.0).astype(jnp.bfloat16)
        qm[2 * h + 1] = jnp.where(first_map, 0.0, q).astype(jnp.bfloat16)

    def attend(s):
        vt[...] = kv[s, 1].astype(jnp.float32).T.astype(jnp.bfloat16)

        def one(i, _):
            scores = lax.dot_general(
                kv[s, 0], qm[i], (((1,), (1,)), ((), ())), preferred_element_type=jnp.float32
            )
            old = m_ref[i]
            high = jnp.maximum(old, jnp.max(scores, axis=0, keepdims=True))
            shrink = jnp.exp(old - high)
            weights = jnp.exp(scores - high)
            l_ref[i] = l_ref[i] * shrink + jnp.sum(weights, axis=0, keepdims=True)
            m_ref[i] = high
            acc[i] = acc[i] * shrink + jnp.dot(
                vt[...], weights.astype(jnp.bfloat16), preferred_element_type=jnp.float32
            )
            return 0

        lax.fori_loop(0, 2 * nx, one, 0)

    def step(j, _):
        zz, _off = nearest(j // nx, z, nz)
        xx = lax.rem(x + lax.rem(j, nx), nx)
        s = slot(zz, xx)

        @pl.when(j > 0)
        def _():
            remote(kv.at[s], kv.at[s], kx_sem.at[0], kv_sem.at[s], x=xo).wait_recv()
            flow(s, zz, start)

        for k, at in enumerate(GATE_STEPS, 1):
            @pl.when(j == at)
            def _():
                gate_up(k, start)

        attend(s)
        return 0

    lax.fori_loop(0, nz * nx, step, 0)

    for h in range(nx):
        first = acc[2 * h] / l_ref[2 * h]
        second = acc[2 * h + 1] / l_ref[2 * h + 1]
        differ = first - lam_ref[x] * second
        scale = lax.rsqrt(jnp.mean(differ * differ, axis=0, keepdims=True) + 1e-05)
        ho[h] = (differ * scale * gain_ref[...]).T.astype(jnp.bfloat16)

    head = tp * nx + x
    me = (x * ny + y) * nc + c

    def spread(go):
        n = 0
        for b in range(nx):
            for e in range(ny):
                for f in range(nc):
                    if b + e + f:
                        xd, yd, cd = lax.rem(x + b, nx), lax.rem(y + e, ny), lax.rem(c + f, nc)
                        src = ho.at[xd, lanes(yd * nc + cd, own_rows), :]
                        go(remote(src, hg.at[:, lanes(head, wide)], hs_sem.at[n], hr_sem.at[me], x=xd, y=yd, c=cd))
                        n += 1

    spread(start)
    hg[:, lanes(head, wide)] = ho[x, lanes(tp, own_rows), :]
    for copy in local_in:
        copy.wait()
    for b in range(nx):
        for e in range(ny):
            for f in range(nc):
                if b + e + f:
                    xd, yd, cd = lax.rem(x + b, nx), lax.rem(y + e, ny), lax.rem(c + f, nc)
                    other = (xd * ny + yd) * nc + cd
                    block = hg.at[:, lanes((yd * nc + cd) * nx + xd, wide)]
                    remote(block, block, hs_sem.at[0], hr_sem.at[other], x=xo).wait_recv()

    state = res[...].astype(jnp.float32) + jnp.dot(hg[...], wout[...], preferred_element_type=jnp.float32)
    hidden[...] = state.astype(jnp.bfloat16)
    stream = hidden[...].astype(jnp.float32)
    scaled = stream * lax.rsqrt(jnp.mean(stream * stream, axis=1, keepdims=True) + 1e-05)
    cube = z0 * 4 + x * 2 + y
    xs[cube] = (scaled * norm_ref[...]).astype(jnp.bfloat16)

    bits = dict(z=(z0, 4), x=(x, 2), y=(y, 1))
    across = dict(z=dict(z=z + 1 - 2 * z0), x=dict(x=xo), y=dict(y=1 - y))
    orders = (("x", "y", "z"), ("y", "z", "x"), ("z", "x", "y"))
    tiles = width // 128
    cuts = [0] + [128 * ((tiles * (i + 1) + 2) // 3) for i in range(3)]
    columns = [pl.ds(cuts[i], cuts[i + 1] - cuts[i]) for i in range(3)]

    def flip(axis):
        bit, mask = bits[axis]
        return (1 - 2 * bit) * mask

    def gather(p, k, go):
        held = [cube]
        for axis in orders[p][:k]:
            held += [i + flip(axis) for i in held]
        axis = orders[p][k]
        for n, i in enumerate(held):
            block = xs.at[i, :, columns[p]]
            go(remote(block, block, xs_sem.at[p, k, n], xr_sem.at[p, k], **across[axis]))

    def gathered(p, k):
        block = xs.at[pl.ds(0, 2**k), :, columns[p]]
        remote(block, block, xs_sem.at[p, k, 0], xr_sem.at[p, k], x=xo).wait_recv()

    for k in range(3):
        for p in range(3):
            if k:
                gathered(p, k - 1)
            gather(p, k, start)

    for j in range(1, nz * nx):
        downward(j, start)
    for copy in own_weights:
        copy.wait()

    def fill(weights, recv, pass_s, pass_r, take):
        def one(j, _):
            s = lax.rem(mine + j, nz * nx)

            @pl.when(j > 0)
            def _():
                remote(take(c, s), take(c, s), pass_s.at[s], recv.at[s], c=co).wait_recv()

            remote(take(c, s), take(c, s), pass_s.at[s], pass_r.at[s], c=co).start()
            return 0

        lax.fori_loop(0, nz * nx, one, 0)

        def end(s, _):
            remote(take(co, s), take(co, s), pass_s.at[s], pass_r.at[s], c=co).wait_recv()
            return 0

        lax.fori_loop(0, nz * nx, end, 0)

    fill(wgu, gr_sem, gp_sem, gq_sem, lambda cc, s: wgu.at[cc, :, lanes(s, depth), :])
    for p in range(3):
        gathered(p, 2)

    rows = 2 * own_rows
    blocks = 8
    spare = q_me * quarter - jnp.minimum(q_me * quarter, units - quarter)
    keep = lax.broadcasted_iota(jnp.int32, (rows, quarter), 1) >= spare

    def expand(i, _):
        both = xs[pl.ds(2 * i, 2)].reshape(rows, width)
        for cc in range(nc):
            gate = jnp.dot(both, wgu[cc, 0], preferred_element_type=jnp.float32)
            up = jnp.dot(both, wgu[cc, 1], preferred_element_type=jnp.float32)
            made = gate / (1.0 + jnp.exp(-gate)) * up
            hb[lanes(i, rows), cc * quarter : (cc + 1) * quarter] = jnp.where(keep, made, 0.0).astype(jnp.bfloat16)
        return 0

    lax.fori_loop(0, blocks // 2, expand, 0)
    fill(wd, dr_sem, dp_sem, dq_sem, lambda cc, s: wd.at[cc, :, lanes(s, depth)])

    def place(p, flips):
        return cube + sum(flip(axis) for axis in flips)

    def choices(axes):
        sets = [()]
        for axis in axes:
            sets = sets + [t + (axis,) for t in sets]
        return sets

    held_in = (r1, r2, r3)

    def reduce_send(p, k, go):
        axis, rest = orders[p][k], orders[p][k + 1 :]
        for n, t in enumerate(choices(rest)):
            spot = sum((bits[a][0] if a not in t else 1 - bits[a][0]) * 2**i for i, a in enumerate(rest))
            src = part.at[place(p, t + (axis,)), :, columns[p]]
            dst = held_in[k].at[spot, :, columns[p]]
            go(remote(src, dst, rs_sem.at[p, k, n], rr_sem.at[p, k], **across[axis]))

    def reduce_take(p, k):
        axis, rest = orders[p][k], orders[p][k + 1 :]
        block = held_in[k].at[:, :, columns[p]]
        remote(block, block, rs_sem.at[p, k, 0], rr_sem.at[p, k], x=xo).wait_recv()
        if not rest:
            return
        for t in reversed(choices(rest)):
            spot = sum((bits[a][0] if a not in t else 1 - bits[a][0]) * 2**i for i, a in enumerate(rest))
            i = place(p, t)
            part[i, :, columns[p]] = (
                part[i, :, columns[p]].astype(jnp.float32)
                + held_in[k][spot, :, columns[p]].astype(jnp.float32)
            ).astype(jnp.bfloat16)

    for p in range(3):
        def contract(i, _):
            weights = wd[:, :, columns[p]].reshape(nc * quarter, columns[p].size)
            made = jnp.dot(hb[lanes(i, rows), :], weights, preferred_element_type=jnp.float32)
            part[pl.ds(2 * i, 2), :, columns[p]] = made.astype(jnp.bfloat16).reshape(2, own_rows, columns[p].size)
            return 0

        lax.fori_loop(0, blocks // 2, contract, 0)
        reduce_send(p, 0, start)
    for k in range(2):
        for p in range(3):
            reduce_take(p, k)
            reduce_send(p, k + 1, start)
    for p in range(3):
        reduce_take(p, 2)
        cols = columns[p]
        out_ref[:, cols] = (
            hidden[:, cols].astype(jnp.float32)
            + part[cube, :, cols].astype(jnp.float32)
            + r3[0, :, cols].astype(jnp.float32)
        ).astype(jnp.bfloat16)

    swap(sent)

    def settle(j, _):
        zz, _off = nearest(j // nx, z, nz)
        flow(slot(zz, lax.rem(x + lax.rem(j, nx), nx)), zz, sent)
        return 0

    lax.fori_loop(0, nz * nx, settle, 0)
    for j in range(1, nz * nx):
        gate_up(j, sent)
        downward(j, sent)
    spread(sent)
    for p in range(3):
        for k in range(3):
            gather(p, k, sent)
            reduce_send(p, k, sent)

    def passed(s, _):
        block = wgu.at[c, :, lanes(s, depth), :]
        remote(block, block, gp_sem.at[s], gq_sem.at[s], c=co).wait_send()
        block = wd.at[c, :, lanes(s, depth)]
        remote(block, block, dp_sem.at[s], dq_sem.at[s], c=co).wait_send()
        return 0

    lax.fori_loop(0, nz * nx, passed, 0)


GATE_STEPS = (2, 3, 4, 5, 6, 7, 7)


def layer(
    nz, nx, ny, nc, residual, queries, key_pairs, values, lambdas, head_gain, w_out, norm_gain, w_gate, w_up, w_down
):
    tokens = queries.shape[0]
    wide = head_gain.shape[0]
    width = residual.shape[1]
    depth, units = w_gate.shape
    own_rows = tokens // (ny * nc)
    quarter = -(-units // (2 * nx * 128)) * 128
    vmem = pl.BlockSpec(memory_space=pltpu.VMEM)
    hbm = pl.BlockSpec(memory_space=pl.ANY)
    dma = pltpu.SemaphoreType.DMA
    bf16 = lambda *shape: pltpu.VMEM(shape, jnp.bfloat16)
    f32 = lambda *shape: pltpu.VMEM(shape, jnp.float32)
    n = nz * nx
    return pl.pallas_call(
        functools.partial(layer_kernel, nz, nx, ny, nc),
        out_shape=jax.ShapeDtypeStruct((own_rows, width), jnp.bfloat16),
        in_specs=[pl.BlockSpec(memory_space=pltpu.SMEM)] + [vmem] * 5 + [hbm] * 5,
        out_specs=vmem,
        scratch_shapes=[
            bf16(nx, tokens, wide), bf16(2 * nx, tokens, wide), bf16(n, 2, tokens, wide), bf16(wide, tokens),
            f32(2 * nx, 1, tokens), f32(2 * nx, 1, tokens), f32(2 * nx, wide, tokens),
            bf16(nx, tokens, wide), bf16(own_rows, w_out.shape[0]),
            bf16(*w_out.shape), bf16(own_rows, width), bf16(own_rows, width),
            bf16(8, own_rows, width), bf16(nc, 2, width, quarter), bf16(nc, quarter, width),
            bf16(8 * own_rows, nc * quarter), bf16(8, own_rows, width),
            bf16(4, own_rows, width), bf16(2, own_rows, width), bf16(1, own_rows, width),
            dma((2,)), dma((2,)), dma((n,)), dma((n,)), dma((n,)),
            dma((n, 2)), dma((n,)), dma((n,)), dma((n,)), dma((n,)), dma((n,)), dma((n,)), dma((n,)),
            dma((nx * ny * nc,)), dma((nx * ny * nc,)), dma((5,)),
            dma((3, 3, 4)), dma((3, 3)), dma((3, 3, 4)), dma((3, 3)),
        ],
        compiler_params=pltpu.CompilerParams(
            collective_id=2, has_side_effects=True, vmem_limit_bytes=62 * 1024 * 1024
        ),
        name="layer",
    )(
        lambdas, queries, key_pairs, values, head_gain.reshape(wide, 1), norm_gain.reshape(1, width),
        residual, w_out, w_gate, w_up, w_down,
    )


def solution(mesh):
    sp, tp = mesh.shape["sp"], mesh.shape["tp"]
    coords = [getattr(d, "coords", None) for d in mesh.devices.flat]
    known = all(p is not None for p in coords)
    nx = len({p[0] for p in coords}) if known else 2
    ny = len({p[1] for p in coords}) if known else 2
    if sp % nx:
        nx = 1
    if tp % ny:
        ny = 1
    nz, nc = sp // nx, tp // ny
    zx, yc = ("z", "x"), ("y", "c")

    def placed(tp_axes):
        split = P(zx, tp_axes)
        return (P(zx, None), split, split, split, P(tp_axes), P(), P(), P(), split, split, P(tp_axes, zx))

    def run(*args):
        heads, units = args[4].shape[0], args[8].shape[1] // tp
        if nx == ny == nc == 2 and nz % 2 == 0 and heads == tp * nx and units % 128 == 0:
            box = Mesh(np.asarray(mesh.devices).reshape(nz, nx, ny, nc), ("z", "x", "y", "c"))
            body, tp_axes = functools.partial(layer, nz, nx, ny, nc), yc
        else:
            box = Mesh(np.asarray(mesh.devices).reshape(nz, nx, tp), ("z", "x", "tp"))
            body, tp_axes = functools.partial(per_device, nz, nx), ("tp",)
        return jax.shard_map(
            body, mesh=box, in_specs=placed(tp_axes), out_specs=P(zx + tp_axes, None), check_vma=False
        )(*args)

    return run
```

```python
import functools

import jax
import jax.numpy as jnp
import numpy as np
from jax import lax
from jax.experimental import pallas as pl
from jax.experimental.pallas import tpu as pltpu
from jax.sharding import Mesh, PartitionSpec as P

HD = 64


def attend_chunk(q, k, v, m_ref, l_ref, acc_ref, slot, rows):
    scores = lax.dot_general(
        q, k, (((1,), (1,)), ((), ())), preferred_element_type=jnp.float32
    )
    old = m_ref[slot, rows, :]
    high = jnp.maximum(old, jnp.max(scores, axis=1, keepdims=True))
    shrink = jnp.exp(old - high)
    weights = jnp.exp(scores - high[:, :1])
    l_ref[slot, rows, :] = l_ref[slot, rows, :] * shrink + jnp.sum(weights, axis=1, keepdims=True)
    m_ref[slot, rows, :] = high
    acc_ref[slot, rows, :] = acc_ref[slot, rows, :] * shrink + jnp.dot(
        weights.astype(jnp.bfloat16), v, preferred_element_type=jnp.float32
    )


def finish_heads(heads, width, lam_ref, gain_ref, l_ref, acc_ref, out_ref):
    for h in range(heads):
        first = acc_ref[2 * h] / l_ref[2 * h]
        second = acc_ref[2 * h + 1] / l_ref[2 * h + 1]
        differ = first - lam_ref[h] * second
        scale = lax.rsqrt(jnp.mean(differ * differ, axis=1, keepdims=True) + 1e-05)
        out_ref[:, h * width : (h + 1) * width] = (differ * scale * gain_ref[...]).astype(out_ref.dtype)


def nearest(k, me, n):
    low, high = me, n - 1 - me
    edge = jnp.minimum(low, high)
    side = jnp.where(high >= low, 1, -1)
    near = jnp.where(k % 2 == 1, 1, -1) * ((k + 1) // 2)
    off = side * jnp.where(k <= 2 * edge, near, k - edge)
    return me + off, off


def gather_attend_kernel(
    nz, nx, heads, block,
    lam_ref, q_ref, kv_ref, gain_ref, pair_ref, down_ref,
    out_ref, pair_out, down_out,
    kv_all, m_ref, l_ref, acc_ref,
    up_sem, low_sem, side_sem, kv_sem, pz_sem, dz_sem, px_sem, dx_sem, p_sem, d_sem,
):
    z, x = lax.axis_index("z"), lax.axis_index("x")
    rows_all = q_ref.shape[0]
    width = out_ref.shape[1] // heads
    keys = heads * 2 * HD
    depth = pair_ref.shape[2]

    def remote(src, dst, send, recv, zz, xx):
        return pltpu.make_async_remote_copy(
            src_ref=src, dst_ref=dst, send_sem=send, recv_sem=recv,
            device_id={"z": zz, "x": xx}, device_id_type=pl.DeviceIdType.MESH,
        )

    barrier = pltpu.get_barrier_semaphore()
    for a in range(nz):
        for b in range(nx):
            if a + b > 0:
                pl.semaphore_signal(
                    barrier, inc=1,
                    device_id={"z": lax.rem(z + a, nz), "x": lax.rem(x + b, nx)},
                    device_id_type=pl.DeviceIdType.MESH,
                )
    pl.semaphore_wait(barrier, nz * nx - 1)

    def slot(zz, xx):
        return zz * nx + xx

    def flow(src, k, zz, go):
        off = zz - z
        here = kv_all.at[slot(zz, x)]

        @pl.when(jnp.logical_and(off <= 0, z < nz - 1))
        def _():
            go(remote(src, here, up_sem.at[k], kv_sem.at[slot(zz, x)], jnp.minimum(z + 1, nz - 1), x))

        @pl.when(jnp.logical_and(off >= 0, z > 0))
        def _():
            go(remote(src, here, low_sem.at[k], kv_sem.at[slot(zz, x)], jnp.maximum(z - 1, 0), x))

        for e in range(1, nx):
            go(remote(src, here, side_sem.at[e - 1, k], kv_sem.at[slot(zz, x)], z, lax.rem(x + e, nx)))

    def pair_place(s):
        return pair_out.at[:, pl.ds(pl.multiple_of(s * depth, depth), depth), :]

    def along(d, go):
        to = lax.rem(z + d, nz)
        s = slot(z, x)
        go(remote(pair_ref.at[to], pair_place(s), pz_sem.at[d], p_sem.at[s], to, x))
        go(remote(down_ref.at[to], down_out.at[s], dz_sem.at[d], d_sem.at[s], to, x))

    def across(src_pair, src_down, d, s, go):
        for e in range(1, nx):
            to = lax.rem(x + e, nx)
            go(remote(src_pair, pair_place(s), px_sem.at[e - 1, d], p_sem.at[s], z, to))
            go(remote(src_down, down_out.at[s], dx_sem.at[e - 1, d], d_sem.at[s], z, to))

    def arrived(src_pair, src_down, s):
        remote(src_pair, pair_place(s), pz_sem.at[0], p_sem.at[s], z, x).wait_recv()
        remote(src_down, down_out.at[s], dz_sem.at[0], d_sem.at[s], z, x).wait_recv()

    start = lambda copy: copy.start()
    sent = lambda copy: copy.wait_send()

    flow(kv_ref, 0, z, start)
    mine = slot(z, x)
    pair_out[:, pl.ds(pl.multiple_of(mine * depth, depth), depth), :] = pair_ref[z]
    down_out[mine] = down_ref[z]
    kv_all[mine] = kv_ref[...]
    m_ref[...] = jnp.full_like(m_ref, -jnp.inf)
    l_ref[...] = jnp.zeros_like(l_ref)
    acc_ref[...] = jnp.zeros_like(acc_ref)

    def attend(s):
        for h in range(heads):
            v = kv_all[s, :, keys + h * width : keys + (h + 1) * width]
            for m in range(2):
                lane = (2 * h + m) * HD
                k = kv_all[s, :, lane : lane + HD]
                for r in range(0, rows_all, block):
                    rows = pl.ds(r, block)
                    q = q_ref[rows, lane : lane + HD] * jnp.bfloat16(HD**-0.5)
                    attend_chunk(q, k, v, m_ref, l_ref, acc_ref, 2 * h + m, rows)

    def step(k, _):
        zz, _off = nearest(k, z, nz)
        here = kv_all.at[slot(zz, x)]

        @pl.when(k > 0)
        def _():
            remote(kv_ref, here, up_sem.at[k], kv_sem.at[slot(zz, x)], z, x).wait_recv()
            flow(here, k, zz, start)

        @pl.when(k == min(1, nz - 1))
        def _():
            for d in range(1, nz):
                along(d, start)
            across(pair_ref.at[z], down_ref.at[z], 0, mine, start)

        def column(e, _):
            other = lax.rem(x - e + nx, nx)

            @pl.when(e > 0)
            def _():
                remote(kv_ref, here, up_sem.at[k], kv_sem.at[slot(zz, other)], z, x).wait_recv()

            attend(slot(zz, other))
            return 0

        lax.fori_loop(0, nx, column, 0)
        return 0

    lax.fori_loop(0, nz, step, 0)
    for d in range(1, nz):
        zz = lax.rem(z - d + nz, nz)
        s = slot(zz, x)
        arrived(pair_ref.at[z], down_ref.at[z], s)
        across(pair_place(s), down_out.at[s], d, s, start)
    finish_heads(heads, width, lam_ref, gain_ref, l_ref, acc_ref, out_ref)
    for d in range(nz):
        zz = lax.rem(z - d + nz, nz)
        for e in range(1, nx):
            arrived(pair_ref.at[z], down_ref.at[z], slot(zz, lax.rem(x - e + nx, nx)))
    for d in range(nz):
        zz = lax.rem(z - d + nz, nz)
        s = slot(zz, x)
        across(pair_place(s), down_out.at[s], d, s, sent)
        if d:
            along(d, sent)

    def settle(k, _):
        zz, _off = nearest(k, z, nz)
        flow(kv_ref, k, zz, sent)
        return 0

    lax.fori_loop(0, nz, settle, 0)


def gather_attend(nz, nx, queries, kv, lambdas, head_gain, pairs, downs):
    rows = queries.shape[0]
    heads = lambdas.shape[0]
    width = head_gain.shape[0]
    _, _, depth, mine = pairs.shape
    blocks = nz * nx
    vmem = pl.BlockSpec(memory_space=pltpu.VMEM)
    dma = pltpu.SemaphoreType.DMA
    side = max(nx - 1, 1)
    return pl.pallas_call(
        functools.partial(gather_attend_kernel, nz, nx, heads, 256),
        out_shape=[
            jax.ShapeDtypeStruct((rows, heads * width), jnp.bfloat16),
            jax.ShapeDtypeStruct((2, blocks * depth, mine), jnp.bfloat16),
            jax.ShapeDtypeStruct((blocks,) + downs.shape[1:], jnp.bfloat16),
        ],
        in_specs=[pl.BlockSpec(memory_space=pltpu.SMEM)] + [vmem] * 5,
        out_specs=[vmem] * 3,
        scratch_shapes=[pltpu.VMEM((blocks,) + kv.shape, jnp.bfloat16)]
        + [pltpu.VMEM((2 * heads, rows, width), jnp.float32)] * 3
        + [
            dma((nz,)), dma((nz,)), dma((side, nz)), dma((blocks,)),
            dma((nz,)), dma((nz,)), dma((side, nz)), dma((side, nz)), dma((blocks,)), dma((blocks,)),
        ],
        compiler_params=pltpu.CompilerParams(
            collective_id=0, has_side_effects=True, vmem_limit_bytes=60 * 1024 * 1024
        ),
        cost_estimate=pl.CostEstimate(
            flops=rows * rows * blocks * heads * 4096, bytes_accessed=4000000, transcendentals=0
        ),
        name="gather_attend",
    )(lambdas, queries, kv, head_gain.reshape(1, width), pairs, downs)


def gather_rows_kernel(nz, nt, own_ref, out_ref, up_sem, low_sem, y_sem, c_sem, got_sem):
    z, t = lax.axis_index("z"), lax.axis_index("tp")
    rows = own_ref.shape[0]
    partner = t + 1 - 2 * lax.rem(t, 2)

    barrier = pltpu.get_barrier_semaphore()
    for a in range(nz):
        for b in range(nt):
            if a + b > 0:
                pl.semaphore_signal(
                    barrier, inc=1,
                    device_id={"z": lax.rem(z + a, nz), "tp": lax.rem(t + b, nt)},
                    device_id_type=pl.DeviceIdType.MESH,
                )
    pl.semaphore_wait(barrier, nz * nt - 1)

    def place(zz, tt):
        s = zz * nt + tt
        return out_ref.at[pl.ds(pl.multiple_of(s * rows, rows), rows), :], got_sem.at[s]

    def remote(src, zz, tt, send, to_z, to_t):
        dst, recv = place(zz, tt)
        return pltpu.make_async_remote_copy(
            src_ref=src, dst_ref=dst, send_sem=send, recv_sem=recv,
            device_id={"z": to_z, "tp": to_t}, device_id_type=pl.DeviceIdType.MESH,
        )

    def flow(src, k, zz, go):
        @pl.when(jnp.logical_and(zz <= z, z < nz - 1))
        def _():
            go(remote(src, zz, t, up_sem.at[k], jnp.minimum(z + 1, nz - 1), t))

        @pl.when(jnp.logical_and(zz >= z, z > 0))
        def _():
            go(remote(src, zz, t, low_sem.at[k], jnp.maximum(z - 1, 0), t))

        for e in range(1, nt // 2):
            go(remote(src, zz, t, y_sem.at[k, e], z, lax.rem(t + 2 * e, nt)))
        go(remote(src, zz, t, c_sem.at[k, 0], z, partner))

    start = lambda copy: copy.start()
    sent = lambda copy: copy.wait_send()

    def await_block(zz, tt):
        remote(own_ref, zz, tt, c_sem.at[0, 0], z, partner).wait_recv()

    flow(own_ref, 0, z, start)
    mine, _sem = place(z, t)
    mine[...] = own_ref[...]

    def same_core(e):
        return lax.rem(t - 2 * e + nt, nt)

    def step(k, _):
        zz, _off = nearest(k, z, nz)

        @pl.when(k > 0)
        def _():
            await_block(zz, t)
            flow(place(zz, t)[0], k, zz, start)

        for e in range(1, nt // 2):
            tt = same_core(e)
            await_block(zz, tt)
            remote(place(zz, tt)[0], zz, tt, c_sem.at[k, e], z, partner).start()
        return 0

    lax.fori_loop(0, nz, step, 0)

    def settle(k, _):
        zz, _off = nearest(k, z, nz)
        flow(own_ref, k, zz, sent)
        for e in range(nt // 2):
            await_block(zz, lax.rem(partner - 2 * e + nt, nt))
            if e:
                tt = same_core(e)
                remote(own_ref, zz, tt, c_sem.at[k, e], z, partner).wait_send()
        return 0

    lax.fori_loop(0, nz, settle, 0)


def gather_rows(nz, nt, own):
    rows, width = own.shape
    if nt % 2:
        return lax.all_gather(own, ("z", "tp"), axis=0, tiled=True)
    vmem = pl.BlockSpec(memory_space=pltpu.VMEM)
    dma = pltpu.SemaphoreType.DMA
    return pl.pallas_call(
        functools.partial(gather_rows_kernel, nz, nt),
        out_shape=jax.ShapeDtypeStruct((nz * nt * rows, width), own.dtype),
        in_specs=[vmem],
        out_specs=vmem,
        scratch_shapes=[dma((nz,)), dma((nz,)), dma((nz, nt // 2)), dma((nz, nt // 2)), dma((nz * nt,))],
        compiler_params=pltpu.CompilerParams(
            collective_id=1, has_side_effects=True, vmem_limit_bytes=32 * 1024 * 1024
        ),
        cost_estimate=pl.CostEstimate(flops=10**10, bytes_accessed=4000000, transcendentals=0),
        name="gather_rows",
    )(own)


def per_device(
    nz, nx, residual, queries, key_pairs, values, lambdas, head_gain, w_out, norm_gain, w_gate, w_up, w_down
):
    local_rows = queries.shape[0]
    heads_here = lambdas.shape[0]
    value_width = head_gain.shape[0]
    d_rows, units = w_gate.shape
    mine = units // nz
    width = residual.shape[1]

    kv = jnp.concatenate([key_pairs, values], axis=1)
    pairs = jnp.stack([w_gate.reshape(d_rows, nz, mine), w_up.reshape(d_rows, nz, mine)], axis=2)
    pairs = jnp.transpose(pairs, (1, 2, 0, 3))
    heads_out, both, downs = gather_attend(
        nz, nx, queries, kv, lambdas, head_gain, pairs, w_down.reshape(nz, mine, w_down.shape[1])
    )
    gate, up = both[0], both[1]
    down = jnp.transpose(downs, (1, 0, 2)).reshape(mine, width)
    tp_index = lax.axis_index("tp")
    own_rows = local_rows // lax.axis_size("tp")
    w_mine = lax.dynamic_slice_in_dim(
        w_out, tp_index * heads_here * value_width, heads_here * value_width, 0
    )
    projected = lax.psum_scatter(
        jnp.dot(heads_out, w_mine, preferred_element_type=jnp.float32).astype(jnp.bfloat16),
        "tp",
        scatter_dimension=0,
        tiled=True,
    ).astype(jnp.float32)
    residual_own = lax.dynamic_slice_in_dim(residual, tp_index * own_rows, own_rows, 0)
    hidden_own = (residual_own.astype(jnp.float32) + projected).astype(jnp.bfloat16)
    stream_f = hidden_own.astype(jnp.float32)
    scaled = stream_f * lax.rsqrt(jnp.mean(stream_f * stream_f, axis=-1, keepdims=True) + 1e-05)
    normed_rows = gather_rows(nz, lax.axis_size("tp"), (scaled * norm_gain).astype(jnp.bfloat16))
    gate_sum = jnp.dot(normed_rows, gate, preferred_element_type=jnp.float32)
    up_sum = jnp.dot(normed_rows, up, preferred_element_type=jnp.float32)
    hidden_units = (jax.nn.silu(gate_sum) * up_sum).astype(jnp.bfloat16)
    ffn_out = lax.psum_scatter(
        jnp.dot(hidden_units, down, preferred_element_type=jnp.float32).astype(jnp.bfloat16),
        ("z", "tp"),
        scatter_dimension=0,
        tiled=True,
    ).astype(jnp.float32)
    return (hidden_own.astype(jnp.float32) + ffn_out).astype(jnp.bfloat16)


def layer_kernel(
    nz, nx, ny, nc,
    lam_ref, q_ref, k_ref, v_ref, gain_ref, norm_ref, res_ref, wout_ref, wg_ref, wu_ref, wd_ref,
    out_ref,
    q_all, qm, kv, vt, m_ref, l_ref, acc, ho, hg, wout, res, hidden, xs, wgu, wd, stage, stage_d, hb, part, r1, r2, r3,
    q_sem, kx_sem, up_sem, low_sem, kv_sem,
    gs_sem, gr_sem, gp_sem, gq_sem, ds_sem, dr_sem, dp_sem, dq_sem,
    wx_sem, st_sem, hs_sem, hr_sem, in_sem, xz_sem, xs_sem, xr_sem, rs_sem, rr_sem,
):
    z, x = lax.axis_index("z"), lax.axis_index("x")
    y, c = lax.axis_index("y"), lax.axis_index("c")
    z0 = lax.rem(z, 2)
    tokens = q_ref.shape[0]
    wide = v_ref.shape[1] // nx
    own_rows, width = out_ref.shape
    depth = wg_ref.shape[0]
    units, quarter = wg_ref.shape[1], wgu.shape[3]
    tp = y * nc + c
    xo, co = 1 - x, 1 - c
    here = dict(z=z, x=x, y=y, c=c)

    def remote(src, dst, send, recv, **to):
        return pltpu.make_async_remote_copy(
            src_ref=src, dst_ref=dst, send_sem=send, recv_sem=recv,
            device_id={**here, **to}, device_id_type=pl.DeviceIdType.MESH,
        )

    def lanes(i, n):
        return pl.ds(pl.multiple_of(i * n, n), n)

    local_in = [
        pltpu.make_async_copy(wout_ref, wout, in_sem.at[0]),
        pltpu.make_async_copy(res_ref.at[lanes(tp, own_rows), :], res, in_sem.at[1]),
    ]
    for copy in local_in:
        copy.start()

    barrier = pltpu.get_barrier_semaphore()
    peers = [dict(z=lax.rem(z + a, nz), x=lax.rem(x + b, nx)) for a in range(nz) for b in range(nx) if a + b]
    peers += [
        dict(x=lax.rem(x + b, nx), y=lax.rem(y + e, ny), c=lax.rem(c + f, nc))
        for b in range(nx) for e in range(ny) for f in range(nc) if e + f
    ]
    for to in peers:
        pl.semaphore_signal(barrier, inc=1, device_id={**here, **to}, device_id_type=pl.DeviceIdType.MESH)
    pl.semaphore_wait(barrier, len(peers))

    start = lambda copy: copy.start()
    sent = lambda copy: copy.wait_send()

    def slot(zz, xx):
        return zz * nx + xx

    mine = slot(z, x)

    def swap(go):
        go(remote(q_ref.at[:, lanes(xo, wide)], q_all.at[x], q_sem.at[0], q_sem.at[1], x=xo))
        go(remote(k_ref.at[:, lanes(xo, wide)], kv.at[mine, 0], kx_sem.at[0], kv_sem.at[mine], x=xo))
        go(remote(v_ref.at[:, lanes(xo, wide)], kv.at[mine, 1], kx_sem.at[1], kv_sem.at[mine], x=xo))

    def up_down(zz, go_up, go_low):
        @pl.when(jnp.logical_and(zz <= z, z < nz - 1))
        def _():
            go_up(jnp.minimum(z + 1, nz - 1))

        @pl.when(jnp.logical_and(zz >= z, z > 0))
        def _():
            go_low(jnp.maximum(z - 1, 0))

    def own_flow(sem, to):
        for i, ref in enumerate((k_ref, v_ref)):
            remote(ref.at[:, lanes(x, wide)], kv.at[mine, i], sem.at[mine], kv_sem.at[mine], z=to).start()

    def flow(s, zz, go):
        up_down(
            zz,
            lambda to: go(remote(kv.at[s], kv.at[s], up_sem.at[s], kv_sem.at[s], z=to)),
            lambda to: go(remote(kv.at[s], kv.at[s], low_sem.at[s], kv_sem.at[s], z=to)),
        )

    def offset(q):
        return pl.multiple_of(jnp.minimum(q * quarter, units - quarter), 128)

    halves = nz // 2

    def half(g):
        return lax.rem(z // 2 + g, halves)

    near = [(0, 1, b) for b in range(nx)]
    far = [(g, t, b) for b in range(nx) for g in range(1, halves) for t in range(2)]

    def units_of(xd, t):
        return pl.ds(offset(xd * 2 + lax.rem(z0 + t, 2)), quarter)

    def aside(go):
        rows = lanes(mine, depth)
        for i, ref in enumerate((wg_ref, wu_ref)):
            go(remote(ref.at[:, units_of(xo, 0)], wgu.at[c, i, rows, :], wx_sem.at[0, i], gr_sem.at[mine], x=xo))
        for i, ref in enumerate((wg_ref, wu_ref)):
            go(remote(ref.at[:, units_of(xo, 1)], stage.at[i], wx_sem.at[1, i], st_sem.at[0], x=xo))
        go(remote(wd_ref.at[units_of(xo, 0), :], wd.at[c, :, rows], wx_sem.at[0, 2], dr_sem.at[mine], x=xo))
        go(remote(wd_ref.at[units_of(xo, 1), :], stage_d, wx_sem.at[1, 2], st_sem.at[1], x=xo))

    def gate_up(to, go):
        g, t, b = to
        s = slot(z, lax.rem(x + b, nx))
        rows = lanes(s, depth)
        for i, ref in enumerate((wg_ref, wu_ref)):
            src = stage.at[i] if b and t else wgu.at[c, i, rows, :] if b else ref.at[:, units_of(x, t)]
            zd = half(g) * 2 + lax.rem(z0 + t, 2)
            go(remote(src, wgu.at[c, i, rows, :], gs_sem.at[g, t, b, i], gr_sem.at[s], z=zd))

    def downward(to, go):
        g, t, b = to
        s = slot(z, lax.rem(x + b, nx))
        cols = lanes(s, depth)
        src = stage_d if b and t else wd.at[c, :, cols] if b else wd_ref.at[units_of(x, t), :]
        zd = half(g) * 2 + lax.rem(z0 + t, 2)
        go(remote(src, wd.at[c, :, cols], ds_sem.at[g, t, b], dr_sem.at[s], z=zd))

    def aside_came():
        rows = lanes(slot(z, xo), depth)
        for block, sem in (
            (wgu.at[c, :, rows, :], gr_sem.at[slot(z, xo)]), (stage, st_sem.at[0]),
            (wd.at[c, :, rows], dr_sem.at[slot(z, xo)]), (stage_d, st_sem.at[1]),
        ):
            remote(block, block, wx_sem.at[0, 0], sem, x=xo).wait_recv()

    inner = z0 == jnp.where(z < nz // 2, 1, 0)
    outer = jnp.logical_not(inner)
    q_me = x * 2 + z0
    own_weights = [
        pltpu.make_async_copy(ref.at[:, pl.ds(offset(q_me), quarter)], wgu.at[c, i, lanes(mine, depth), :], in_sem.at[2 + i])
        for i, ref in enumerate((wg_ref, wu_ref))
    ]
    own_weights.append(
        pltpu.make_async_copy(wd_ref.at[pl.ds(offset(q_me), quarter), :], wd.at[c, :, lanes(mine, depth)], in_sem.at[4])
    )

    swap(start)
    up_down(z, lambda to: own_flow(up_sem, to), lambda to: own_flow(low_sem, to))
    aside(start)
    for copy in own_weights:
        copy.start()

    kv[mine, 0] = k_ref[:, lanes(x, wide)]
    kv[mine, 1] = v_ref[:, lanes(x, wide)]
    q_all[x] = q_ref[:, lanes(x, wide)]
    m_ref[...] = jnp.full_like(m_ref, -jnp.inf)
    l_ref[...] = jnp.zeros_like(l_ref)
    acc[...] = jnp.zeros_like(acc)

    remote(q_all.at[x], q_all.at[xo], q_sem.at[0], q_sem.at[1], x=xo).wait_recv()
    first_map = lax.broadcasted_iota(jnp.int32, (tokens, 2 * HD), 1) < HD
    for h in range(nx):
        q = q_all[h].astype(jnp.float32) * HD**-0.5
        qm[2 * h] = jnp.where(first_map, q, 0.0).astype(jnp.bfloat16)
        qm[2 * h + 1] = jnp.where(first_map, 0.0, q).astype(jnp.bfloat16)

    def attend(s):
        vt[...] = kv[s, 1].astype(jnp.float32).T.astype(jnp.bfloat16)

        def one(i, _):
            scores = lax.dot_general(
                kv[s, 0], qm[i], (((1,), (1,)), ((), ())), preferred_element_type=jnp.float32
            )
            old = m_ref[i]
            high = jnp.maximum(old, jnp.max(scores, axis=0, keepdims=True))
            shrink = jnp.exp(old - high)
            weights = jnp.exp(scores - high)
            l_ref[i] = l_ref[i] * shrink + jnp.sum(weights, axis=0, keepdims=True)
            m_ref[i] = high
            acc[i] = acc[i] * shrink + jnp.dot(
                vt[...], weights.astype(jnp.bfloat16), preferred_element_type=jnp.float32
            )
            return 0

        lax.fori_loop(0, 2 * nx, one, 0)

    def turn(j):
        mixed = jnp.logical_and(j >= nx, j < 3 * nx) if nz > 2 else False
        k = jnp.where(mixed, 1 + lax.rem(j, 2), j // nx)
        e = jnp.where(mixed, (j - nx) // 2, lax.rem(j, nx))
        zz, _off = nearest(k, z, nz)
        return zz, slot(zz, lax.rem(x + e, nx))

    def step(j, _):
        zz, s = turn(j)

        @pl.when(j > 0)
        def _():
            remote(kv.at[s], kv.at[s], kx_sem.at[0], kv_sem.at[s], x=xo).wait_recv()
            flow(s, zz, start)

        def issue(at, where, some):
            @pl.when(jnp.logical_and(where, j == min(at, nz * nx - 1)))
            def _():
                for to in some:
                    gate_up(to, start)

        issue(2, outer, [to for to in far if to[1:] == (0, 0)])

        @pl.when(j == min(5, nz * nx - 1))
        def _():
            aside_came()

        issue(5, outer, [to for to in far if to[1:] == (0, 1)])
        issue(5, inner, [to for to in far if to[1:] == (1, 0)])
        issue(5, outer, [to for to in far if to[1] == 1])
        issue(7, inner, [to for to in far if to[1:] == (1, 1)])
        attend(s)
        return 0

    lax.fori_loop(0, nz * nx, step, 0)

    for h in range(nx):
        first = acc[2 * h] / l_ref[2 * h]
        second = acc[2 * h + 1] / l_ref[2 * h + 1]
        differ = first - lam_ref[x] * second
        scale = lax.rsqrt(jnp.mean(differ * differ, axis=0, keepdims=True) + 1e-05)
        ho[h] = (differ * scale * gain_ref[...]).T.astype(jnp.bfloat16)

    head = tp * nx + x
    me = (x * ny + y) * nc + c

    def spread(go):
        n = 0
        for b in range(nx):
            for e in range(ny):
                for f in range(nc):
                    if b + e + f:
                        xd, yd, cd = lax.rem(x + b, nx), lax.rem(y + e, ny), lax.rem(c + f, nc)
                        src = ho.at[xd, lanes(yd * nc + cd, own_rows), :]
                        go(remote(src, hg.at[:, lanes(head, wide)], hs_sem.at[n], hr_sem.at[me], x=xd, y=yd, c=cd))
                        n += 1

    spread(start)
    hg[:, lanes(head, wide)] = ho[x, lanes(tp, own_rows), :]
    for copy in local_in:
        copy.wait()
    for b in range(nx):
        for e in range(ny):
            for f in range(nc):
                if b + e + f:
                    xd, yd, cd = lax.rem(x + b, nx), lax.rem(y + e, ny), lax.rem(c + f, nc)
                    other = (xd * ny + yd) * nc + cd
                    block = hg.at[:, lanes((yd * nc + cd) * nx + xd, wide)]
                    remote(block, block, hs_sem.at[0], hr_sem.at[other], x=xo).wait_recv()

    state = res[...].astype(jnp.float32) + jnp.dot(hg[...], wout[...], preferred_element_type=jnp.float32)
    hidden[...] = state.astype(jnp.bfloat16)
    stream = hidden[...].astype(jnp.float32)
    scaled = stream * lax.rsqrt(jnp.mean(stream * stream, axis=1, keepdims=True) + 1e-05)
    cube = z0 * 4 + x * 2 + y
    xs[cube] = (scaled * norm_ref[...]).astype(jnp.bfloat16)

    bits = dict(z=(z0, 4), x=(x, 2), y=(y, 1))
    across = dict(z=dict(z=z + 1 - 2 * z0), x=dict(x=xo), y=dict(y=1 - y))
    paths = (("x", "y"), ("y", "x"))
    split = width // 256 * 128
    columns = (pl.ds(0, split), pl.ds(split, width - split))

    def flip(axis):
        bit, mask = bits[axis]
        return (1 - 2 * bit) * mask

    over = cube + flip("z")

    def lend(go):
        go(remote(xs.at[cube], xs.at[cube], xz_sem.at[0], xz_sem.at[1], **across["z"]))

    def gather(h, p, k, go):
        held = [(cube, over)[h]]
        if k:
            held += [held[0] + flip(paths[p][0])]
        for n, i in enumerate(held):
            block = xs.at[i, :, columns[p]]
            go(remote(block, block, xs_sem.at[h, p, k, n], xr_sem.at[h, p, k], **across[paths[p][k]]))

    def gathered(h, p, k):
        block = xs.at[pl.ds(0, 2**k), :, columns[p]]
        remote(block, block, xs_sem.at[h, p, k, 0], xr_sem.at[h, p, k], x=xo).wait_recv()

    lend(start)
    for p in range(2):
        gather(0, p, 0, start)
    for to in near:
        gate_up(to, start)
    for p in range(2):
        gathered(0, p, 0)
        gather(0, p, 1, start)

    @pl.when(inner)
    def _():
        for to in far:
            if to[1] == 0:
                gate_up(to, start)

    remote(xs.at[over], xs.at[over], xz_sem.at[0], xz_sem.at[1], x=xo).wait_recv()
    for p in range(2):
        gather(1, p, 0, start)
    for p in range(2):
        gathered(1, p, 0)
        gather(1, p, 1, start)

    @pl.when(outer)
    def _():
        for to in near:
            downward(to, start)

    for copy in own_weights:
        copy.wait()

    def pass_on(s, go):
        block = wgu.at[c, :, lanes(s, depth), :]
        go(remote(block, block, gp_sem.at[s], gq_sem.at[s], c=co))

    def fill(j, _):
        s = lax.rem(half(0) * 2 * nx + j, nz * nx)

        @pl.when(s // nx != z)
        def _():
            block = wgu.at[c, :, lanes(s, depth), :]
            remote(block, block, gp_sem.at[s], gr_sem.at[s], c=co).wait_recv()

        pass_on(s, start)
        return 0

    def filled(s, _):
        block = wgu.at[co, :, lanes(s, depth), :]
        remote(block, block, gp_sem.at[s], gq_sem.at[s], c=co).wait_recv()
        return 0

    lax.fori_loop(0, nz * nx, fill, 0)
    lax.fori_loop(0, nz * nx, filled, 0)
    for h in range(2):
        for p in range(2):
            gathered(h, p, 1)

    blocks, group = 8, 4
    rows = group * own_rows
    spare = q_me * quarter - jnp.minimum(q_me * quarter, units - quarter)
    keep = lax.broadcasted_iota(jnp.int32, (rows, quarter), 1) >= spare

    def expand(i, _):
        both = xs[pl.ds(group * i, group)].reshape(rows, width)
        for cc in range(nc):
            gate = jnp.dot(both, wgu[cc, 0], preferred_element_type=jnp.float32)
            up = jnp.dot(both, wgu[cc, 1], preferred_element_type=jnp.float32)
            made = gate / (1.0 + jnp.exp(-gate)) * up
            hb[lanes(i, rows), cc * quarter : (cc + 1) * quarter] = jnp.where(keep, made, 0.0).astype(jnp.bfloat16)
        return 0

    @pl.when(inner)
    def _():
        for to in near:
            downward(to, start)

    for to in far:
        downward(to, start)
    lax.fori_loop(0, blocks // group, expand, 0)
    def place(p, flips):
        return cube + sum(flip(axis) for axis in flips)

    def choices(axes):
        sets = [()]
        for axis in axes:
            sets = sets + [t + (axis,) for t in sets]
        return sets

    held_in = (r1, r2, r3)
    orders = (("x", "y", "z"), ("y", "z", "x"), ("z", "x", "y"))
    span = width // halves
    tiles = span // 128
    cuts = [0] + [128 * ((tiles * (i + 1) + 2) // 3) for i in range(3)]

    def share(g, p):
        return pl.ds(pl.multiple_of(half(g) * span + cuts[p], 128), cuts[p + 1] - cuts[p])

    def down_on(g, go):
        block = wd.at[c, :, lanes(half(g), span)]
        go(remote(block, block, dp_sem.at[g], dq_sem.at[g], c=co))

    def down_fill(g):
        for n in range(2 * nx):
            s = half(g) * 2 * nx + n

            @pl.when(s // nx != z)
            def _():
                block = wd.at[c, :, lanes(s, depth)]
                remote(block, block, dp_sem.at[g], dr_sem.at[s], c=co).wait_recv()

        down_on(g, start)
        block = wd.at[co, :, lanes(half(g), span)]
        remote(block, block, dp_sem.at[g], dq_sem.at[g], c=co).wait_recv()

    def reduce_send(g, p, k, go):
        axis, rest = orders[p][k], orders[p][k + 1 :]
        for n, t in enumerate(choices(rest)):
            spot = sum((bits[a][0] if a not in t else 1 - bits[a][0]) * 2**i for i, a in enumerate(rest))
            src = part.at[place(p, t + (axis,)), :, share(g, p)]
            dst = held_in[k].at[spot, :, share(g, p)]
            go(remote(src, dst, rs_sem.at[g, p, k, n], rr_sem.at[g, p, k], **across[axis]))

    def reduce_take(g, p, k):
        axis, rest = orders[p][k], orders[p][k + 1 :]
        cols = share(g, p)
        block = held_in[k].at[:, :, cols]
        remote(block, block, rs_sem.at[g, p, k, 0], rr_sem.at[g, p, k], x=xo).wait_recv()
        for t in reversed(choices(rest)) if rest else ():
            spot = sum((bits[a][0] if a not in t else 1 - bits[a][0]) * 2**i for i, a in enumerate(rest))
            i = place(p, t)
            part[i, :, cols] = (
                part[i, :, cols].astype(jnp.float32) + held_in[k][spot, :, cols].astype(jnp.float32)
            ).astype(jnp.bfloat16)
        if not rest:
            out_ref[:, cols] = (
                hidden[:, cols].astype(jnp.float32)
                + part[cube, :, cols].astype(jnp.float32)
                + held_in[k][0, :, cols].astype(jnp.float32)
            ).astype(jnp.bfloat16)

    for g in range(halves):
        down_fill(g)
        for p in range(3):
            def contract(i, _):
                weights = wd[:, :, share(g, p)].reshape(nc * quarter, cuts[p + 1] - cuts[p])
                made = jnp.dot(hb[lanes(i, rows), :], weights, preferred_element_type=jnp.float32)
                part[pl.ds(group * i, group), :, share(g, p)] = made.astype(jnp.bfloat16).reshape(group, own_rows, -1)
                return 0

            lax.fori_loop(0, blocks // group, contract, 0)
            reduce_send(g, p, 0, start)
        for p in range(3):
            reduce_take(g, p, 0)
            reduce_send(g, p, 1, start)
        if g:
            for p in range(3):
                reduce_take(g - 1, p, 1)
                reduce_send(g - 1, p, 2, start)
    for p in range(3):
        reduce_take(halves - 1, p, 1)
        reduce_send(halves - 1, p, 2, start)
    for g in range(halves):
        for p in range(3):
            reduce_take(g, p, 2)

    swap(sent)

    def settle(j, _):
        zz, s = turn(j)
        flow(s, zz, sent)
        return 0

    lax.fori_loop(0, nz * nx, settle, 0)
    aside(sent)
    for to in near + far:
        gate_up(to, sent)
        downward(to, sent)
    spread(sent)
    lend(sent)
    for p in range(2):
        for h in range(2):
            for k in range(2):
                gather(h, p, k, sent)
    for k in range(3):
        for p in range(3):
            for g in range(halves):
                reduce_send(g, p, k, sent)
    for g in range(halves):
        down_on(g, sent)

    def passed(s, _):
        pass_on(s, sent)
        return 0

    lax.fori_loop(0, nz * nx, passed, 0)


def layer(
    nz, nx, ny, nc, residual, queries, key_pairs, values, lambdas, head_gain, w_out, norm_gain, w_gate, w_up, w_down
):
    tokens = queries.shape[0]
    wide = head_gain.shape[0]
    width = residual.shape[1]
    depth, units = w_gate.shape
    own_rows = tokens // (ny * nc)
    quarter = -(-units // (2 * nx * 128)) * 128
    vmem = pl.BlockSpec(memory_space=pltpu.VMEM)
    hbm = pl.BlockSpec(memory_space=pl.ANY)
    dma = pltpu.SemaphoreType.DMA
    bf16 = lambda *shape: pltpu.VMEM(shape, jnp.bfloat16)
    f32 = lambda *shape: pltpu.VMEM(shape, jnp.float32)
    n = nz * nx
    return pl.pallas_call(
        functools.partial(layer_kernel, nz, nx, ny, nc),
        out_shape=jax.ShapeDtypeStruct((own_rows, width), jnp.bfloat16),
        in_specs=[pl.BlockSpec(memory_space=pltpu.SMEM)] + [vmem] * 5 + [hbm] * 5,
        out_specs=vmem,
        scratch_shapes=[
            bf16(nx, tokens, wide), bf16(2 * nx, tokens, wide), bf16(n, 2, tokens, wide), bf16(wide, tokens),
            f32(2 * nx, 1, tokens), f32(2 * nx, 1, tokens), f32(2 * nx, wide, tokens),
            bf16(nx, tokens, wide), bf16(own_rows, w_out.shape[0]),
            bf16(*w_out.shape), bf16(own_rows, width), bf16(own_rows, width),
            bf16(8, own_rows, width), bf16(nc, 2, width, quarter), bf16(nc, quarter, width),
            bf16(2, depth, quarter), bf16(quarter, depth),
            bf16(8 * own_rows, nc * quarter), bf16(8, own_rows, width),
            bf16(4, own_rows, width), bf16(2, own_rows, width), bf16(1, own_rows, width),
            dma((2,)), dma((2,)), dma((n,)), dma((n,)), dma((n,)),
            dma((nz // 2, 2, nx, 2)), dma((n,)), dma((n,)), dma((n,)),
            dma((nz // 2, 2, nx)), dma((n,)), dma((nz // 2,)), dma((nz // 2,)),
            dma((2, 3)), dma((2,)), dma((nx * ny * nc,)), dma((nx * ny * nc,)), dma((5,)),
            dma((2,)), dma((2, 2, 2, 2)), dma((2, 2, 2)), dma((nz // 2, 3, 3, 4)), dma((nz // 2, 3, 3)),
        ],
        compiler_params=pltpu.CompilerParams(
            collective_id=2, has_side_effects=True, vmem_limit_bytes=62 * 1024 * 1024
        ),
        name="layer",
    )(
        lambdas, queries, key_pairs, values, head_gain.reshape(wide, 1), norm_gain.reshape(1, width),
        residual, w_out, w_gate, w_up, w_down,
    )


def solution(mesh):
    sp, tp = mesh.shape["sp"], mesh.shape["tp"]
    coords = [getattr(d, "coords", None) for d in mesh.devices.flat]
    known = all(p is not None for p in coords)
    nx = len({p[0] for p in coords}) if known else 2
    ny = len({p[1] for p in coords}) if known else 2
    if sp % nx:
        nx = 1
    if tp % ny:
        ny = 1
    nz, nc = sp // nx, tp // ny
    zx, yc = ("z", "x"), ("y", "c")

    def placed(tp_axes):
        split = P(zx, tp_axes)
        return (P(zx, None), split, split, split, P(tp_axes), P(), P(), P(), split, split, P(tp_axes, zx))

    def run(*args):
        heads, units = args[4].shape[0], args[8].shape[1] // tp
        if nx == ny == nc == 2 and nz % 2 == 0 and heads == tp * nx and units % 128 == 0:
            box = Mesh(np.asarray(mesh.devices).reshape(nz, nx, ny, nc), ("z", "x", "y", "c"))
            body, tp_axes = functools.partial(layer, nz, nx, ny, nc), yc
        else:
            box = Mesh(np.asarray(mesh.devices).reshape(nz, nx, tp), ("z", "x", "tp"))
            body, tp_axes = functools.partial(per_device, nz, nx), ("tp",)
        return jax.shard_map(
            body, mesh=box, in_specs=placed(tp_axes), out_specs=P(zx + tp_axes, None), check_vma=False
        )(*args)

    return run
```

```python
import functools

import jax
import jax.numpy as jnp
import numpy as np
from jax import lax
from jax.experimental import pallas as pl
from jax.experimental.pallas import tpu as pltpu
from jax.sharding import Mesh, PartitionSpec as P

HD = 64


def attend_chunk(q, k, v, m_ref, l_ref, acc_ref, slot, rows):
    scores = lax.dot_general(
        q, k, (((1,), (1,)), ((), ())), preferred_element_type=jnp.float32
    )
    old = m_ref[slot, rows, :]
    high = jnp.maximum(old, jnp.max(scores, axis=1, keepdims=True))
    shrink = jnp.exp(old - high)
    weights = jnp.exp(scores - high[:, :1])
    l_ref[slot, rows, :] = l_ref[slot, rows, :] * shrink + jnp.sum(weights, axis=1, keepdims=True)
    m_ref[slot, rows, :] = high
    acc_ref[slot, rows, :] = acc_ref[slot, rows, :] * shrink + jnp.dot(
        weights.astype(jnp.bfloat16), v, preferred_element_type=jnp.float32
    )


def finish_heads(heads, width, lam_ref, gain_ref, l_ref, acc_ref, out_ref):
    for h in range(heads):
        first = acc_ref[2 * h] / l_ref[2 * h]
        second = acc_ref[2 * h + 1] / l_ref[2 * h + 1]
        differ = first - lam_ref[h] * second
        scale = lax.rsqrt(jnp.mean(differ * differ, axis=1, keepdims=True) + 1e-05)
        out_ref[:, h * width : (h + 1) * width] = (differ * scale * gain_ref[...]).astype(out_ref.dtype)


def nearest(k, me, n):
    low, high = me, n - 1 - me
    edge = jnp.minimum(low, high)
    side = jnp.where(high >= low, 1, -1)
    near = jnp.where(k % 2 == 1, 1, -1) * ((k + 1) // 2)
    off = side * jnp.where(k <= 2 * edge, near, k - edge)
    return me + off, off


def gather_attend_kernel(
    nz, nx, heads, block,
    lam_ref, q_ref, kv_ref, gain_ref, pair_ref, down_ref,
    out_ref, pair_out, down_out,
    kv_all, m_ref, l_ref, acc_ref,
    up_sem, low_sem, side_sem, kv_sem, pz_sem, dz_sem, px_sem, dx_sem, p_sem, d_sem,
):
    z, x = lax.axis_index("z"), lax.axis_index("x")
    rows_all = q_ref.shape[0]
    width = out_ref.shape[1] // heads
    keys = heads * 2 * HD
    depth = pair_ref.shape[2]

    def remote(src, dst, send, recv, zz, xx):
        return pltpu.make_async_remote_copy(
            src_ref=src, dst_ref=dst, send_sem=send, recv_sem=recv,
            device_id={"z": zz, "x": xx}, device_id_type=pl.DeviceIdType.MESH,
        )

    barrier = pltpu.get_barrier_semaphore()
    for a in range(nz):
        for b in range(nx):
            if a + b > 0:
                pl.semaphore_signal(
                    barrier, inc=1,
                    device_id={"z": lax.rem(z + a, nz), "x": lax.rem(x + b, nx)},
                    device_id_type=pl.DeviceIdType.MESH,
                )
    pl.semaphore_wait(barrier, nz * nx - 1)

    def slot(zz, xx):
        return zz * nx + xx

    def flow(src, k, zz, go):
        off = zz - z
        here = kv_all.at[slot(zz, x)]

        @pl.when(jnp.logical_and(off <= 0, z < nz - 1))
        def _():
            go(remote(src, here, up_sem.at[k], kv_sem.at[slot(zz, x)], jnp.minimum(z + 1, nz - 1), x))

        @pl.when(jnp.logical_and(off >= 0, z > 0))
        def _():
            go(remote(src, here, low_sem.at[k], kv_sem.at[slot(zz, x)], jnp.maximum(z - 1, 0), x))

        for e in range(1, nx):
            go(remote(src, here, side_sem.at[e - 1, k], kv_sem.at[slot(zz, x)], z, lax.rem(x + e, nx)))

    def pair_place(s):
        return pair_out.at[:, pl.ds(pl.multiple_of(s * depth, depth), depth), :]

    def along(d, go):
        to = lax.rem(z + d, nz)
        s = slot(z, x)
        go(remote(pair_ref.at[to], pair_place(s), pz_sem.at[d], p_sem.at[s], to, x))
        go(remote(down_ref.at[to], down_out.at[s], dz_sem.at[d], d_sem.at[s], to, x))

    def across(src_pair, src_down, d, s, go):
        for e in range(1, nx):
            to = lax.rem(x + e, nx)
            go(remote(src_pair, pair_place(s), px_sem.at[e - 1, d], p_sem.at[s], z, to))
            go(remote(src_down, down_out.at[s], dx_sem.at[e - 1, d], d_sem.at[s], z, to))

    def arrived(src_pair, src_down, s):
        remote(src_pair, pair_place(s), pz_sem.at[0], p_sem.at[s], z, x).wait_recv()
        remote(src_down, down_out.at[s], dz_sem.at[0], d_sem.at[s], z, x).wait_recv()

    start = lambda copy: copy.start()
    sent = lambda copy: copy.wait_send()

    flow(kv_ref, 0, z, start)
    mine = slot(z, x)
    pair_out[:, pl.ds(pl.multiple_of(mine * depth, depth), depth), :] = pair_ref[z]
    down_out[mine] = down_ref[z]
    kv_all[mine] = kv_ref[...]
    m_ref[...] = jnp.full_like(m_ref, -jnp.inf)
    l_ref[...] = jnp.zeros_like(l_ref)
    acc_ref[...] = jnp.zeros_like(acc_ref)

    def attend(s):
        for h in range(heads):
            v = kv_all[s, :, keys + h * width : keys + (h + 1) * width]
            for m in range(2):
                lane = (2 * h + m) * HD
                k = kv_all[s, :, lane : lane + HD]
                for r in range(0, rows_all, block):
                    rows = pl.ds(r, block)
                    q = q_ref[rows, lane : lane + HD] * jnp.bfloat16(HD**-0.5)
                    attend_chunk(q, k, v, m_ref, l_ref, acc_ref, 2 * h + m, rows)

    def step(k, _):
        zz, _off = nearest(k, z, nz)
        here = kv_all.at[slot(zz, x)]

        @pl.when(k > 0)
        def _():
            remote(kv_ref, here, up_sem.at[k], kv_sem.at[slot(zz, x)], z, x).wait_recv()
            flow(here, k, zz, start)

        @pl.when(k == min(1, nz - 1))
        def _():
            for d in range(1, nz):
                along(d, start)
            across(pair_ref.at[z], down_ref.at[z], 0, mine, start)

        def column(e, _):
            other = lax.rem(x - e + nx, nx)

            @pl.when(e > 0)
            def _():
                remote(kv_ref, here, up_sem.at[k], kv_sem.at[slot(zz, other)], z, x).wait_recv()

            attend(slot(zz, other))
            return 0

        lax.fori_loop(0, nx, column, 0)
        return 0

    lax.fori_loop(0, nz, step, 0)
    for d in range(1, nz):
        zz = lax.rem(z - d + nz, nz)
        s = slot(zz, x)
        arrived(pair_ref.at[z], down_ref.at[z], s)
        across(pair_place(s), down_out.at[s], d, s, start)
    finish_heads(heads, width, lam_ref, gain_ref, l_ref, acc_ref, out_ref)
    for d in range(nz):
        zz = lax.rem(z - d + nz, nz)
        for e in range(1, nx):
            arrived(pair_ref.at[z], down_ref.at[z], slot(zz, lax.rem(x - e + nx, nx)))
    for d in range(nz):
        zz = lax.rem(z - d + nz, nz)
        s = slot(zz, x)
        across(pair_place(s), down_out.at[s], d, s, sent)
        if d:
            along(d, sent)

    def settle(k, _):
        zz, _off = nearest(k, z, nz)
        flow(kv_ref, k, zz, sent)
        return 0

    lax.fori_loop(0, nz, settle, 0)


def gather_attend(nz, nx, queries, kv, lambdas, head_gain, pairs, downs):
    rows = queries.shape[0]
    heads = lambdas.shape[0]
    width = head_gain.shape[0]
    _, _, depth, mine = pairs.shape
    blocks = nz * nx
    vmem = pl.BlockSpec(memory_space=pltpu.VMEM)
    dma = pltpu.SemaphoreType.DMA
    side = max(nx - 1, 1)
    return pl.pallas_call(
        functools.partial(gather_attend_kernel, nz, nx, heads, 256),
        out_shape=[
            jax.ShapeDtypeStruct((rows, heads * width), jnp.bfloat16),
            jax.ShapeDtypeStruct((2, blocks * depth, mine), jnp.bfloat16),
            jax.ShapeDtypeStruct((blocks,) + downs.shape[1:], jnp.bfloat16),
        ],
        in_specs=[pl.BlockSpec(memory_space=pltpu.SMEM)] + [vmem] * 5,
        out_specs=[vmem] * 3,
        scratch_shapes=[pltpu.VMEM((blocks,) + kv.shape, jnp.bfloat16)]
        + [pltpu.VMEM((2 * heads, rows, width), jnp.float32)] * 3
        + [
            dma((nz,)), dma((nz,)), dma((side, nz)), dma((blocks,)),
            dma((nz,)), dma((nz,)), dma((side, nz)), dma((side, nz)), dma((blocks,)), dma((blocks,)),
        ],
        compiler_params=pltpu.CompilerParams(
            collective_id=0, has_side_effects=True, vmem_limit_bytes=60 * 1024 * 1024
        ),
        cost_estimate=pl.CostEstimate(
            flops=rows * rows * blocks * heads * 4096, bytes_accessed=4000000, transcendentals=0
        ),
        name="gather_attend",
    )(lambdas, queries, kv, head_gain.reshape(1, width), pairs, downs)


def gather_rows_kernel(nz, nt, own_ref, out_ref, up_sem, low_sem, y_sem, c_sem, got_sem):
    z, t = lax.axis_index("z"), lax.axis_index("tp")
    rows = own_ref.shape[0]
    partner = t + 1 - 2 * lax.rem(t, 2)

    barrier = pltpu.get_barrier_semaphore()
    for a in range(nz):
        for b in range(nt):
            if a + b > 0:
                pl.semaphore_signal(
                    barrier, inc=1,
                    device_id={"z": lax.rem(z + a, nz), "tp": lax.rem(t + b, nt)},
                    device_id_type=pl.DeviceIdType.MESH,
                )
    pl.semaphore_wait(barrier, nz * nt - 1)

    def place(zz, tt):
        s = zz * nt + tt
        return out_ref.at[pl.ds(pl.multiple_of(s * rows, rows), rows), :], got_sem.at[s]

    def remote(src, zz, tt, send, to_z, to_t):
        dst, recv = place(zz, tt)
        return pltpu.make_async_remote_copy(
            src_ref=src, dst_ref=dst, send_sem=send, recv_sem=recv,
            device_id={"z": to_z, "tp": to_t}, device_id_type=pl.DeviceIdType.MESH,
        )

    def flow(src, k, zz, go):
        @pl.when(jnp.logical_and(zz <= z, z < nz - 1))
        def _():
            go(remote(src, zz, t, up_sem.at[k], jnp.minimum(z + 1, nz - 1), t))

        @pl.when(jnp.logical_and(zz >= z, z > 0))
        def _():
            go(remote(src, zz, t, low_sem.at[k], jnp.maximum(z - 1, 0), t))

        for e in range(1, nt // 2):
            go(remote(src, zz, t, y_sem.at[k, e], z, lax.rem(t + 2 * e, nt)))
        go(remote(src, zz, t, c_sem.at[k, 0], z, partner))

    start = lambda copy: copy.start()
    sent = lambda copy: copy.wait_send()

    def await_block(zz, tt):
        remote(own_ref, zz, tt, c_sem.at[0, 0], z, partner).wait_recv()

    flow(own_ref, 0, z, start)
    mine, _sem = place(z, t)
    mine[...] = own_ref[...]

    def same_core(e):
        return lax.rem(t - 2 * e + nt, nt)

    def step(k, _):
        zz, _off = nearest(k, z, nz)

        @pl.when(k > 0)
        def _():
            await_block(zz, t)
            flow(place(zz, t)[0], k, zz, start)

        for e in range(1, nt // 2):
            tt = same_core(e)
            await_block(zz, tt)
            remote(place(zz, tt)[0], zz, tt, c_sem.at[k, e], z, partner).start()
        return 0

    lax.fori_loop(0, nz, step, 0)

    def settle(k, _):
        zz, _off = nearest(k, z, nz)
        flow(own_ref, k, zz, sent)
        for e in range(nt // 2):
            await_block(zz, lax.rem(partner - 2 * e + nt, nt))
            if e:
                tt = same_core(e)
                remote(own_ref, zz, tt, c_sem.at[k, e], z, partner).wait_send()
        return 0

    lax.fori_loop(0, nz, settle, 0)


def gather_rows(nz, nt, own):
    rows, width = own.shape
    if nt % 2:
        return lax.all_gather(own, ("z", "tp"), axis=0, tiled=True)
    vmem = pl.BlockSpec(memory_space=pltpu.VMEM)
    dma = pltpu.SemaphoreType.DMA
    return pl.pallas_call(
        functools.partial(gather_rows_kernel, nz, nt),
        out_shape=jax.ShapeDtypeStruct((nz * nt * rows, width), own.dtype),
        in_specs=[vmem],
        out_specs=vmem,
        scratch_shapes=[dma((nz,)), dma((nz,)), dma((nz, nt // 2)), dma((nz, nt // 2)), dma((nz * nt,))],
        compiler_params=pltpu.CompilerParams(
            collective_id=1, has_side_effects=True, vmem_limit_bytes=32 * 1024 * 1024
        ),
        cost_estimate=pl.CostEstimate(flops=10**10, bytes_accessed=4000000, transcendentals=0),
        name="gather_rows",
    )(own)


def per_device(
    nz, nx, residual, queries, key_pairs, values, lambdas, head_gain, w_out, norm_gain, w_gate, w_up, w_down
):
    local_rows = queries.shape[0]
    heads_here = lambdas.shape[0]
    value_width = head_gain.shape[0]
    d_rows, units = w_gate.shape
    mine = units // nz
    width = residual.shape[1]

    kv = jnp.concatenate([key_pairs, values], axis=1)
    pairs = jnp.stack([w_gate.reshape(d_rows, nz, mine), w_up.reshape(d_rows, nz, mine)], axis=2)
    pairs = jnp.transpose(pairs, (1, 2, 0, 3))
    heads_out, both, downs = gather_attend(
        nz, nx, queries, kv, lambdas, head_gain, pairs, w_down.reshape(nz, mine, w_down.shape[1])
    )
    gate, up = both[0], both[1]
    down = jnp.transpose(downs, (1, 0, 2)).reshape(mine, width)
    tp_index = lax.axis_index("tp")
    own_rows = local_rows // lax.axis_size("tp")
    w_mine = lax.dynamic_slice_in_dim(
        w_out, tp_index * heads_here * value_width, heads_here * value_width, 0
    )
    projected = lax.psum_scatter(
        jnp.dot(heads_out, w_mine, preferred_element_type=jnp.float32).astype(jnp.bfloat16),
        "tp",
        scatter_dimension=0,
        tiled=True,
    ).astype(jnp.float32)
    residual_own = lax.dynamic_slice_in_dim(residual, tp_index * own_rows, own_rows, 0)
    hidden_own = (residual_own.astype(jnp.float32) + projected).astype(jnp.bfloat16)
    stream_f = hidden_own.astype(jnp.float32)
    scaled = stream_f * lax.rsqrt(jnp.mean(stream_f * stream_f, axis=-1, keepdims=True) + 1e-05)
    normed_rows = gather_rows(nz, lax.axis_size("tp"), (scaled * norm_gain).astype(jnp.bfloat16))
    gate_sum = jnp.dot(normed_rows, gate, preferred_element_type=jnp.float32)
    up_sum = jnp.dot(normed_rows, up, preferred_element_type=jnp.float32)
    hidden_units = (jax.nn.silu(gate_sum) * up_sum).astype(jnp.bfloat16)
    ffn_out = lax.psum_scatter(
        jnp.dot(hidden_units, down, preferred_element_type=jnp.float32).astype(jnp.bfloat16),
        ("z", "tp"),
        scatter_dimension=0,
        tiled=True,
    ).astype(jnp.float32)
    return (hidden_own.astype(jnp.float32) + ffn_out).astype(jnp.bfloat16)


FIRST = 3


def layer_kernel(
    nz, nx, ny, nc,
    lam_ref, q_ref, k_ref, v_ref, gain_ref, norm_ref, res_ref, wout_ref, wg_ref, wu_ref, wd_ref,
    out_ref,
    q_all, qm, kv, vt, m_ref, l_ref, acc, ho, hg, wout, res, hidden, xs, wgu, wd, stage, stage_d, hb, part, r1, r2, r3,
    q_sem, qo_sem, qr_sem, kx_sem, kf_sem, kv_sem,
    gs_sem, gr_sem, gp_sem, gq_sem, ds_sem, dr_sem, dp_sem, dq_sem,
    wx_sem, st_sem, hs_sem, hr_sem, in_sem, xz_sem, xs_sem, xr_sem, rs_sem, rr_sem,
):
    z, x = lax.axis_index("z"), lax.axis_index("x")
    y, c = lax.axis_index("y"), lax.axis_index("c")
    z0 = lax.rem(z, 2)
    tokens = q_ref.shape[0]
    wide = v_ref.shape[1] // nx
    own_rows, width = out_ref.shape
    depth = wg_ref.shape[0]
    units, quarter = wg_ref.shape[1], wgu.shape[3]
    tp = y * nc + c
    xo, co = 1 - x, 1 - c
    here = dict(z=z, x=x, y=y, c=c)

    def remote(src, dst, send, recv, **to):
        return pltpu.make_async_remote_copy(
            src_ref=src, dst_ref=dst, send_sem=send, recv_sem=recv,
            device_id={**here, **to}, device_id_type=pl.DeviceIdType.MESH,
        )

    def lanes(i, n):
        return pl.ds(pl.multiple_of(i * n, n), n)

    local_in = [
        pltpu.make_async_copy(wout_ref, wout, in_sem.at[0]),
        pltpu.make_async_copy(res_ref.at[lanes(tp, own_rows), :], res, in_sem.at[1]),
    ]
    for copy in local_in:
        copy.start()

    barrier = pltpu.get_barrier_semaphore()
    peers = [dict(z=lax.rem(z + a, nz), x=lax.rem(x + b, nx)) for a in range(nz) for b in range(nx) if a + b]
    peers += [
        dict(x=lax.rem(x + b, nx), y=lax.rem(y + e, ny), c=lax.rem(c + f, nc))
        for b in range(nx) for e in range(ny) for f in range(nc) if e + f
    ]
    peers += [dict(p, z=z + 1 - 2 * z0) for p in peers if "y" in p]
    for to in peers:
        pl.semaphore_signal(barrier, inc=1, device_id={**here, **to}, device_id_type=pl.DeviceIdType.MESH)
    pl.semaphore_wait(barrier, len(peers))

    start = lambda copy: copy.start()
    sent = lambda copy: copy.wait_send()

    def slot(zz, xx):
        return zz * nx + xx

    mine = slot(z, x)

    def swap(go):
        go(remote(q_ref.at[:, lanes(xo, wide)], q_all.at[x], q_sem.at[0], q_sem.at[1], x=xo))
        go(remote(k_ref.at[:, lanes(xo, wide)], kv.at[mine, 0], kx_sem.at[0], kv_sem.at[mine], x=xo))
        go(remote(v_ref.at[:, lanes(xo, wide)], kv.at[mine, 1], kx_sem.at[1], kv_sem.at[mine], x=xo))

    halves = nz // 2
    inner = z0 == jnp.where(z < nz // 2, 1, 0)
    outer = jnp.logical_not(inner)

    def half(g):
        return lax.rem(z // 2 + g, halves)

    def flow(e, g, go):
        s = slot(z, lax.rem(x + e, nx))
        zd = 2 * half(g) + jnp.where(2 * half(g) < nz // 2, 1, 0)
        if e or go is sent:
            go(remote(kv.at[s], kv.at[s], kf_sem.at[g, e], kv_sem.at[s], z=zd))
        else:
            for i, ref in enumerate((k_ref, v_ref)):
                go(remote(ref.at[:, lanes(x, wide)], kv.at[s, i], kf_sem.at[g, e], kv_sem.at[s], z=zd))

    def ask(e, go):
        src = q_all.at[xo] if e else q_ref.at[:, lanes(x, wide)]
        go(remote(src, q_all.at[nx + (xo if e else x)], qo_sem.at[e], qr_sem.at[xo if e else x], z=z + 1 - 2 * z0))

    def swapped():
        remote(kv.at[slot(z, xo)], kv.at[slot(z, xo)], kx_sem.at[0], kv_sem.at[slot(z, xo)], x=xo).wait_recv()

    def offset(q):
        return pl.multiple_of(jnp.minimum(q * quarter, units - quarter), 128)

    near = [(0, 1, b) for b in range(nx)]
    far = [(g, t, b) for b in range(nx) for g in range(1, halves) for t in range(2)]

    def units_of(xd, t):
        return pl.ds(offset(xd * 2 + lax.rem(z0 + t, 2)), quarter)

    def aside(go):
        rows = lanes(mine, depth)
        for i, ref in enumerate((wg_ref, wu_ref)):
            go(remote(ref.at[:, units_of(xo, 0)], wgu.at[c, i, rows, :], wx_sem.at[0, i], gr_sem.at[mine], x=xo))
        for i, ref in enumerate((wg_ref, wu_ref)):
            go(remote(ref.at[:, units_of(xo, 1)], stage.at[i], wx_sem.at[1, i], st_sem.at[0], x=xo))
        go(remote(wd_ref.at[units_of(xo, 0), :], wd.at[c, :, rows], wx_sem.at[0, 2], dr_sem.at[mine], x=xo))
        go(remote(wd_ref.at[units_of(xo, 1), :], stage_d, wx_sem.at[1, 2], st_sem.at[1], x=xo))

    def gate_up(to, go):
        g, t, b = to
        s = slot(z, lax.rem(x + b, nx))
        rows = lanes(s, depth)
        for i, ref in enumerate((wg_ref, wu_ref)):
            src = stage.at[i] if b and t else wgu.at[c, i, rows, :] if b else ref.at[:, units_of(x, t)]
            zd = half(g) * 2 + lax.rem(z0 + t, 2)
            go(remote(src, wgu.at[c, i, rows, :], gs_sem.at[g, t, b, i], gr_sem.at[s], z=zd))

    def downward(to, go):
        g, t, b = to
        s = slot(z, lax.rem(x + b, nx))
        cols = lanes(s, depth)
        src = stage_d if b and t else wd.at[c, :, cols] if b else wd_ref.at[units_of(x, t), :]
        zd = half(g) * 2 + lax.rem(z0 + t, 2)
        go(remote(src, wd.at[c, :, cols], ds_sem.at[g, t, b], dr_sem.at[s], z=zd))

    def aside_came(last):
        rows = lanes(slot(z, xo), depth)
        early = (wgu.at[c, :, rows, :], gr_sem.at[slot(z, xo)]), (stage, st_sem.at[0])
        late = (wd.at[c, :, rows], dr_sem.at[slot(z, xo)]), (stage_d, st_sem.at[1])
        for block, sem in late if last else early:
            remote(block, block, wx_sem.at[0, 0], sem, x=xo).wait_recv()

    q_me = x * 2 + z0
    own_weights = [
        pltpu.make_async_copy(ref.at[:, pl.ds(offset(q_me), quarter)], wgu.at[c, i, lanes(mine, depth), :], in_sem.at[2 + i])
        for i, ref in enumerate((wg_ref, wu_ref))
    ]
    own_weights.append(
        pltpu.make_async_copy(wd_ref.at[pl.ds(offset(q_me), quarter), :], wd.at[c, :, lanes(mine, depth)], in_sem.at[4])
    )

    swap(start)

    @pl.when(outer)
    def _():
        ask(0, start)
        flow(0, 0, start)

    @pl.when(inner)
    def _():
        for g in range(1, halves):
            flow(0, g, start)

    for copy in own_weights:
        copy.start()

    remote(q_all.at[x], q_all.at[xo], q_sem.at[0], q_sem.at[1], x=xo).wait_recv()

    @pl.when(outer)
    def _():
        ask(1, start)

    swapped()
    aside(start)

    @pl.when(inner)
    def _():
        for g in range(1, halves):
            flow(1, g, start)

    @pl.when(outer)
    def _():
        flow(1, 0, start)
        for e in range(nx):
            for g in range(1, halves):
                flow(e, g, start)
        for g in range(halves):
            for e in range(nx):
                flow(e, g, sent)
        for n, to in enumerate(far[:FIRST]):
            if n == len(far) // 2:
                aside_came(False)
            gate_up(to, start)
            gate_up(to, sent)

    def attend(s, low, high):
        vt[...] = kv[s, 1].astype(jnp.float32).T.astype(jnp.bfloat16)

        def pair(h, _):
            both = [2 * h, 2 * h + 1]
            scores = [
                lax.dot_general(kv[s, 0], qm[i], (((1,), (1,)), ((), ())), preferred_element_type=jnp.float32)
                for i in both
            ]
            olds = [m_ref[i] for i in both]
            highs = [jnp.maximum(o, jnp.max(t, axis=0, keepdims=True)) for o, t in zip(olds, scores)]
            weights = [jnp.exp(t - g) for t, g in zip(scores, highs)]
            mixed = [jnp.dot(vt[...], w.astype(jnp.bfloat16), preferred_element_type=jnp.float32) for w in weights]
            for i, o, g, w, t in zip(both, olds, highs, weights, mixed):
                shrink = jnp.exp(o - g)
                l_ref[i] = l_ref[i] * shrink + jnp.sum(w, axis=0, keepdims=True)
                m_ref[i] = g
                acc[i] = acc[i] * shrink + t
            return 0

        lax.fori_loop(low, high, pair, 0)

    def turn(j):
        mixed = jnp.logical_and(j >= nx, j < 3 * nx) if nz > 2 else False
        k = jnp.where(mixed, 1 + lax.rem(j, 2), j // nx)
        e = jnp.where(mixed, (j - nx) // 2, lax.rem(j, nx))
        zz, _off = nearest(k, z, nz)
        return zz, slot(zz, lax.rem(x + e, nx))

    def ready(low):
        for h in range(low, low + nx):
            q = q_all[h].astype(jnp.float32) * HD**-0.5
            qm[2 * h] = jnp.where(first_map, q, 0.0).astype(jnp.bfloat16)
            qm[2 * h + 1] = jnp.where(first_map, 0.0, q).astype(jnp.bfloat16)

    first_map = lax.broadcasted_iota(jnp.int32, (tokens, 2 * HD), 1) < HD

    def step(n, _):
        j = jnp.where(n < 2 * nx, lax.rem(n, nx), n - nx)
        zz, s = turn(j)

        @pl.when(n == nx)
        def _():
            for e in range(nx):
                remote(q_all.at[0], q_all.at[0], qo_sem.at[0], qr_sem.at[e], x=xo).wait_recv()
            ready(nx)

        @pl.when(zz != z)
        def _():
            remote(kv.at[s], kv.at[s], kx_sem.at[0], kv_sem.at[s], x=xo).wait_recv()

        def issue(at, some):
            @pl.when(j == min(at, nz * nx - 1))
            def _():
                for to in some:
                    gate_up(to, start)

        issue(2, near[:1])
        issue(3, [to for to in far if to[1:] == (1, 0)])
        issue(4, [to for to in far if to[1:] == (0, 0)])

        @pl.when(j == min(5, nz * nx - 1))
        def _():
            aside_came(False)

        issue(5, near[1:])
        issue(5, [to for to in far if to[1:] == (1, 1)])
        issue(6, [to for to in far if to[1:] == (0, 1)])
        attend(s, jnp.where(jnp.logical_and(n >= nx, n < 2 * nx), nx, 0), jnp.where(n < nx, nx, 2 * nx))
        return 0

    head = tp * nx + x
    me = (x * ny + y) * nc + c

    def spread(go):
        for b in range(nx):
            for e in range(ny):
                for f in range(nc):
                    xd, yd, cd = lax.rem(x + b, nx), lax.rem(y + e, ny), lax.rem(c + f, nc)
                    for p in range(0 if b + e + f else 1, 2):
                        n = ((b * ny + e) * nc + f) * 2 + p
                        src = ho.at[p * nx + xd, lanes(yd * nc + cd, own_rows), :]
                        zd = z + p * (1 - 2 * z0)
                        go(remote(src, hg.at[:, lanes(head, wide)], hs_sem.at[n], hr_sem.at[me], z=zd, x=xd, y=yd, c=cd))

    @pl.when(inner)
    def _():
        kv[mine, 0] = k_ref[:, lanes(x, wide)]
        kv[mine, 1] = v_ref[:, lanes(x, wide)]
        q_all[x] = q_ref[:, lanes(x, wide)]
        m_ref[...] = jnp.full_like(m_ref, -jnp.inf)
        l_ref[...] = jnp.zeros_like(l_ref)
        acc[...] = jnp.zeros_like(acc)
        ready(0)
        lax.fori_loop(0, nz * nx + nx, step, 0)

        def finish(h, _):
            first = acc[2 * h] / l_ref[2 * h]
            second = acc[2 * h + 1] / l_ref[2 * h + 1]
            differ = first - lam_ref[x] * second
            scale = lax.rsqrt(jnp.mean(differ * differ, axis=0, keepdims=True) + 1e-05)
            ho[h] = (differ * scale * gain_ref[...]).T.astype(jnp.bfloat16)
            return 0

        lax.fori_loop(0, 2 * nx, finish, 0)
        spread(start)
        hg[:, lanes(head, wide)] = ho[x, lanes(tp, own_rows), :]

    for copy in local_in:
        copy.wait()
    for b in range(nx):
        for e in range(ny):
            for f in range(nc):
                xd, yd, cd = lax.rem(x + b, nx), lax.rem(y + e, ny), lax.rem(c + f, nc)
                other = (xd * ny + yd) * nc + cd
                block = hg.at[:, lanes((yd * nc + cd) * nx + xd, wide)]

                def came():
                    remote(block, block, hs_sem.at[0], hr_sem.at[other], x=xo).wait_recv()

                if b + e + f:
                    came()
                else:
                    pl.when(outer)(came)

    state = res[...].astype(jnp.float32) + jnp.dot(hg[...], wout[...], preferred_element_type=jnp.float32)
    hidden[...] = state.astype(jnp.bfloat16)
    stream = hidden[...].astype(jnp.float32)
    scaled = stream * lax.rsqrt(jnp.mean(stream * stream, axis=1, keepdims=True) + 1e-05)
    cube = z0 * 4 + x * 2 + y
    xs[cube] = (scaled * norm_ref[...]).astype(jnp.bfloat16)

    bits = dict(z=(z0, 4), x=(x, 2), y=(y, 1))
    across = dict(z=dict(z=z + 1 - 2 * z0), x=dict(x=xo), y=dict(y=1 - y))
    paths = (("x", "y"), ("y", "x"))
    split = width // 256 * 128
    columns = (pl.ds(0, split), pl.ds(split, width - split))

    def flip(axis):
        bit, mask = bits[axis]
        return (1 - 2 * bit) * mask

    over = cube + flip("z")

    def lend(p, go):
        block = xs.at[cube, :, columns[p]]
        go(remote(block, block, xz_sem.at[p, 0], xz_sem.at[p, 1], **across["z"]))

    def gather(h, p, k, go):
        held = [(cube, over)[h]]
        if k:
            held += [held[0] + flip(paths[p][0])]
        for n, i in enumerate(held):
            block = xs.at[i, :, columns[p]]
            go(remote(block, block, xs_sem.at[h, p, k, n], xr_sem.at[h, p, k], **across[paths[p][k]]))

    def gathered(h, p, k):
        block = xs.at[pl.ds(0, 2**k), :, columns[p]]
        remote(block, block, xs_sem.at[h, p, k, 0], xr_sem.at[h, p, k], x=xo).wait_recv()

    for p in range(2):
        lend(p, start)
        gather(0, p, 0, start)

    @pl.when(outer)
    def _():
        if FIRST <= len(far) // 2:
            aside_came(False)
        for to in far[FIRST:] + near:
            gate_up(to, start)

    for p in range(2):
        gathered(0, p, 0)
        gather(0, p, 1, start)
    for p in range(2):
        block = xs.at[over, :, columns[p]]
        remote(block, block, xz_sem.at[p, 0], xz_sem.at[p, 1], x=xo).wait_recv()
        gather(1, p, 0, start)
    for p in range(2):
        gathered(1, p, 0)
        gather(1, p, 1, start)
    aside_came(True)

    @pl.when(outer)
    def _():
        for to in near + [to for to in far if to[1] == 0]:
            downward(to, start)

    @pl.when(inner)
    def _():
        for to in far:
            if to[1]:
                downward(to, start)

    for copy in own_weights:
        copy.wait()

    def pass_on(s, go):
        block = wgu.at[c, :, lanes(s, depth), :]
        go(remote(block, block, gp_sem.at[s], gq_sem.at[s], c=co))

    def fill(j, _):
        s = lax.rem(half(0) * 2 * nx + j, nz * nx)

        @pl.when(s // nx != z)
        def _():
            block = wgu.at[c, :, lanes(s, depth), :]
            remote(block, block, gp_sem.at[s], gr_sem.at[s], c=co).wait_recv()

        pass_on(s, start)
        return 0

    def filled(s, _):
        block = wgu.at[co, :, lanes(s, depth), :]
        remote(block, block, gp_sem.at[s], gq_sem.at[s], c=co).wait_recv()
        return 0

    lax.fori_loop(0, nz * nx, fill, 0)
    lax.fori_loop(0, nz * nx, filled, 0)
    for h in range(2):
        for p in range(2):
            gathered(h, p, 1)

    blocks, group = 8, 4
    rows = group * own_rows
    spare = q_me * quarter - jnp.minimum(q_me * quarter, units - quarter)
    keep = lax.broadcasted_iota(jnp.int32, (rows, quarter), 1) >= spare

    def expand(i, _):
        both = xs[pl.ds(group * i, group)].reshape(rows, width)
        for cc in range(nc):
            gate = jnp.dot(both, wgu[cc, 0], preferred_element_type=jnp.float32)
            up = jnp.dot(both, wgu[cc, 1], preferred_element_type=jnp.float32)
            made = gate / (1.0 + jnp.exp(-gate)) * up
            hb[lanes(i, rows), cc * quarter : (cc + 1) * quarter] = jnp.where(keep, made, 0.0).astype(jnp.bfloat16)
        return 0

    @pl.when(outer)
    def _():
        for to in far:
            if to[1]:
                downward(to, start)

    @pl.when(inner)
    def _():
        for to in near + [to for to in far if to[1] == 0]:
            downward(to, start)

    lax.fori_loop(0, blocks // group, expand, 0)
    def place(p, flips):
        return cube + sum(flip(axis) for axis in flips)

    def choices(axes):
        sets = [()]
        for axis in axes:
            sets = sets + [t + (axis,) for t in sets]
        return sets

    held_in = (r1, r2, r3)
    spare_z = (("x", "y", "z"), ("y", "x", "z"))
    even = (("x", "y", "z"), ("y", "z", "x"), ("z", "x", "y"))
    orders = [even if g == halves - 1 else spare_z for g in range(halves)]
    span = width // halves
    tiles = span // 128
    cuts = [[0] + [128 * ((tiles * (i + 1) + len(o) - 1) // len(o)) for i in range(len(o))] for o in orders]

    def share(g, p):
        return pl.ds(pl.multiple_of(half(g) * span + cuts[g][p], 128), cuts[g][p + 1] - cuts[g][p])

    def down_on(g, go):
        block = wd.at[c, :, lanes(half(g), span)]
        go(remote(block, block, dp_sem.at[g], dq_sem.at[g], c=co))

    def down_fill(g):
        for n in range(2 * nx):
            s = half(g) * 2 * nx + n

            @pl.when(s // nx != z)
            def _():
                block = wd.at[c, :, lanes(s, depth)]
                remote(block, block, dp_sem.at[g], dr_sem.at[s], c=co).wait_recv()

        down_on(g, start)
        block = wd.at[co, :, lanes(half(g), span)]
        remote(block, block, dp_sem.at[g], dq_sem.at[g], c=co).wait_recv()

    def reduce_send(g, p, k, go):
        axis, rest = orders[g][p][k], orders[g][p][k + 1 :]
        for n, t in enumerate(choices(rest)):
            spot = sum((bits[a][0] if a not in t else 1 - bits[a][0]) * 2**i for i, a in enumerate(rest))
            src = part.at[place(p, t + (axis,)), :, share(g, p)]
            dst = held_in[k].at[spot, :, share(g, p)]
            go(remote(src, dst, rs_sem.at[g, p, k, n], rr_sem.at[g, p, k], **across[axis]))

    def reduce_take(g, p, k):
        axis, rest = orders[g][p][k], orders[g][p][k + 1 :]
        cols = share(g, p)
        block = held_in[k].at[:, :, cols]
        remote(block, block, rs_sem.at[g, p, k, 0], rr_sem.at[g, p, k], x=xo).wait_recv()
        for t in reversed(choices(rest)) if rest else ():
            spot = sum((bits[a][0] if a not in t else 1 - bits[a][0]) * 2**i for i, a in enumerate(rest))
            i = place(p, t)
            part[i, :, cols] = (
                part[i, :, cols].astype(jnp.float32) + held_in[k][spot, :, cols].astype(jnp.float32)
            ).astype(jnp.bfloat16)
        if not rest:
            out_ref[:, cols] = (
                hidden[:, cols].astype(jnp.float32)
                + part[cube, :, cols].astype(jnp.float32)
                + held_in[k][0, :, cols].astype(jnp.float32)
            ).astype(jnp.bfloat16)

    for g in range(halves):
        down_fill(g)
        for p in range(len(orders[g])):
            def contract(i, _):
                weights = wd[:, :, share(g, p)].reshape(nc * quarter, cuts[g][p + 1] - cuts[g][p])
                made = jnp.dot(hb[lanes(i, rows), :], weights, preferred_element_type=jnp.float32)
                part[pl.ds(group * i, group), :, share(g, p)] = made.astype(jnp.bfloat16).reshape(group, own_rows, -1)
                return 0

            lax.fori_loop(0, blocks // group, contract, 0)
            reduce_send(g, p, 0, start)
        for p in range(len(orders[g])):
            reduce_take(g, p, 0)
            reduce_send(g, p, 1, start)
        if g:
            for p in range(len(orders[g - 1])):
                reduce_take(g - 1, p, 1)
                reduce_send(g - 1, p, 2, start)
    for p in range(len(orders[halves - 1])):
        reduce_take(halves - 1, p, 1)
        reduce_send(halves - 1, p, 2, start)
    for g in range(halves):
        for p in range(len(orders[g])):
            reduce_take(g, p, 2)

    swap(sent)

    @pl.when(outer)
    def _():
        for e in range(nx):
            ask(e, sent)

    @pl.when(inner)
    def _():
        for e in range(nx):
            for g in range(1, halves):
                flow(e, g, sent)
        for to in far:
            gate_up(to, sent)
        spread(sent)

    aside(sent)
    @pl.when(outer)
    def _():
        for to in far[FIRST:]:
            gate_up(to, sent)

    for to in near:
        gate_up(to, sent)
    for to in near + far:
        downward(to, sent)
    for p in range(2):
        lend(p, sent)
        for h in range(2):
            for k in range(2):
                gather(h, p, k, sent)
    for k in range(3):
        for g in range(halves):
            for p in range(len(orders[g])):
                reduce_send(g, p, k, sent)
    for g in range(halves):
        down_on(g, sent)

    def passed(s, _):
        pass_on(s, sent)
        return 0

    lax.fori_loop(0, nz * nx, passed, 0)


def layer(
    nz, nx, ny, nc, residual, queries, key_pairs, values, lambdas, head_gain, w_out, norm_gain, w_gate, w_up, w_down
):
    tokens = queries.shape[0]
    wide = head_gain.shape[0]
    width = residual.shape[1]
    depth, units = w_gate.shape
    own_rows = tokens // (ny * nc)
    quarter = -(-units // (2 * nx * 128)) * 128
    vmem = pl.BlockSpec(memory_space=pltpu.VMEM)
    hbm = pl.BlockSpec(memory_space=pl.ANY)
    dma = pltpu.SemaphoreType.DMA
    bf16 = lambda *shape: pltpu.VMEM(shape, jnp.bfloat16)
    f32 = lambda *shape: pltpu.VMEM(shape, jnp.float32)
    n = nz * nx
    return pl.pallas_call(
        functools.partial(layer_kernel, nz, nx, ny, nc),
        out_shape=jax.ShapeDtypeStruct((own_rows, width), jnp.bfloat16),
        in_specs=[pl.BlockSpec(memory_space=pltpu.SMEM)] + [vmem] * 5 + [hbm] * 5,
        out_specs=vmem,
        scratch_shapes=[
            bf16(2 * nx, tokens, wide), bf16(4 * nx, tokens, wide), bf16(n, 2, tokens, wide), bf16(wide, tokens),
            f32(4 * nx, 1, tokens), f32(4 * nx, 1, tokens), f32(4 * nx, wide, tokens),
            bf16(2 * nx, tokens, wide), bf16(own_rows, w_out.shape[0]),
            bf16(*w_out.shape), bf16(own_rows, width), bf16(own_rows, width),
            bf16(8, own_rows, width), bf16(nc, 2, width, quarter), bf16(nc, quarter, width),
            bf16(2, depth, quarter), bf16(quarter, depth),
            bf16(8 * own_rows, nc * quarter), bf16(8, own_rows, width),
            bf16(4, own_rows, width), bf16(2, own_rows, width), bf16(1, own_rows, width),
            dma((2,)), dma((nx,)), dma((nx,)), dma((2,)), dma((nz // 2, nx)), dma((n,)),
            dma((nz // 2, 2, nx, 2)), dma((n,)), dma((n,)), dma((n,)),
            dma((nz // 2, 2, nx)), dma((n,)), dma((nz // 2,)), dma((nz // 2,)),
            dma((2, 3)), dma((2,)), dma((2 * nx * ny * nc,)), dma((nx * ny * nc,)), dma((5,)),
            dma((2, 2)), dma((2, 2, 2, 2)), dma((2, 2, 2)), dma((nz // 2, 3, 3, 4)), dma((nz // 2, 3, 3)),
        ],
        compiler_params=pltpu.CompilerParams(
            collective_id=2, has_side_effects=True, vmem_limit_bytes=62 * 1024 * 1024
        ),
        name="layer",
    )(
        lambdas, queries, key_pairs, values, head_gain.reshape(wide, 1), norm_gain.reshape(1, width),
        residual, w_out, w_gate, w_up, w_down,
    )


def solution(mesh):
    sp, tp = mesh.shape["sp"], mesh.shape["tp"]
    coords = [getattr(d, "coords", None) for d in mesh.devices.flat]
    known = all(p is not None for p in coords)
    nx = len({p[0] for p in coords}) if known else 2
    ny = len({p[1] for p in coords}) if known else 2
    if sp % nx:
        nx = 1
    if tp % ny:
        ny = 1
    nz, nc = sp // nx, tp // ny
    zx, yc = ("z", "x"), ("y", "c")

    def placed(tp_axes):
        split = P(zx, tp_axes)
        return (P(zx, None), split, split, split, P(tp_axes), P(), P(), P(), split, split, P(tp_axes, zx))

    def run(*args):
        heads, units = args[4].shape[0], args[8].shape[1] // tp
        if nx == ny == nc == 2 and nz % 2 == 0 and heads == tp * nx and units % 128 == 0:
            box = Mesh(np.asarray(mesh.devices).reshape(nz, nx, ny, nc), ("z", "x", "y", "c"))
            body, tp_axes = functools.partial(layer, nz, nx, ny, nc), yc
        else:
            box = Mesh(np.asarray(mesh.devices).reshape(nz, nx, tp), ("z", "x", "tp"))
            body, tp_axes = functools.partial(per_device, nz, nx), ("tp",)
        return jax.shard_map(
            body, mesh=box, in_specs=placed(tp_axes), out_specs=P(zx + tp_axes, None), check_vma=False
        )(*args)

    return run
```

```python
import functools

import jax
import jax.numpy as jnp
import numpy as np
from jax import lax
from jax.experimental import pallas as pl
from jax.experimental.pallas import tpu as pltpu
from jax.sharding import Mesh, PartitionSpec as P

HD = 64


def attend_chunk(q, k, v, m_ref, l_ref, acc_ref, slot, rows):
    scores = lax.dot_general(
        q, k, (((1,), (1,)), ((), ())), preferred_element_type=jnp.float32
    )
    old = m_ref[slot, rows, :]
    high = jnp.maximum(old, jnp.max(scores, axis=1, keepdims=True))
    shrink = jnp.exp(old - high)
    weights = jnp.exp(scores - high[:, :1])
    l_ref[slot, rows, :] = l_ref[slot, rows, :] * shrink + jnp.sum(weights, axis=1, keepdims=True)
    m_ref[slot, rows, :] = high
    acc_ref[slot, rows, :] = acc_ref[slot, rows, :] * shrink + jnp.dot(
        weights.astype(jnp.bfloat16), v, preferred_element_type=jnp.float32
    )


def finish_heads(heads, width, lam_ref, gain_ref, l_ref, acc_ref, out_ref):
    for h in range(heads):
        first = acc_ref[2 * h] / l_ref[2 * h]
        second = acc_ref[2 * h + 1] / l_ref[2 * h + 1]
        differ = first - lam_ref[h] * second
        scale = lax.rsqrt(jnp.mean(differ * differ, axis=1, keepdims=True) + 1e-05)
        out_ref[:, h * width : (h + 1) * width] = (differ * scale * gain_ref[...]).astype(out_ref.dtype)


def nearest(k, me, n):
    low, high = me, n - 1 - me
    edge = jnp.minimum(low, high)
    side = jnp.where(high >= low, 1, -1)
    near = jnp.where(k % 2 == 1, 1, -1) * ((k + 1) // 2)
    off = side * jnp.where(k <= 2 * edge, near, k - edge)
    return me + off, off


def gather_attend_kernel(
    nz, nx, heads, block,
    lam_ref, q_ref, kv_ref, gain_ref, pair_ref, down_ref,
    out_ref, pair_out, down_out,
    kv_all, m_ref, l_ref, acc_ref,
    up_sem, low_sem, side_sem, kv_sem, pz_sem, dz_sem, px_sem, dx_sem, p_sem, d_sem,
):
    z, x = lax.axis_index("z"), lax.axis_index("x")
    rows_all = q_ref.shape[0]
    width = out_ref.shape[1] // heads
    keys = heads * 2 * HD
    depth = pair_ref.shape[2]

    def remote(src, dst, send, recv, zz, xx):
        return pltpu.make_async_remote_copy(
            src_ref=src, dst_ref=dst, send_sem=send, recv_sem=recv,
            device_id={"z": zz, "x": xx}, device_id_type=pl.DeviceIdType.MESH,
        )

    barrier = pltpu.get_barrier_semaphore()
    for a in range(nz):
        for b in range(nx):
            if a + b > 0:
                pl.semaphore_signal(
                    barrier, inc=1,
                    device_id={"z": lax.rem(z + a, nz), "x": lax.rem(x + b, nx)},
                    device_id_type=pl.DeviceIdType.MESH,
                )
    pl.semaphore_wait(barrier, nz * nx - 1)

    def slot(zz, xx):
        return zz * nx + xx

    def flow(src, k, zz, go):
        off = zz - z
        here = kv_all.at[slot(zz, x)]

        @pl.when(jnp.logical_and(off <= 0, z < nz - 1))
        def _():
            go(remote(src, here, up_sem.at[k], kv_sem.at[slot(zz, x)], jnp.minimum(z + 1, nz - 1), x))

        @pl.when(jnp.logical_and(off >= 0, z > 0))
        def _():
            go(remote(src, here, low_sem.at[k], kv_sem.at[slot(zz, x)], jnp.maximum(z - 1, 0), x))

        for e in range(1, nx):
            go(remote(src, here, side_sem.at[e - 1, k], kv_sem.at[slot(zz, x)], z, lax.rem(x + e, nx)))

    def pair_place(s):
        return pair_out.at[:, pl.ds(pl.multiple_of(s * depth, depth), depth), :]

    def along(d, go):
        to = lax.rem(z + d, nz)
        s = slot(z, x)
        go(remote(pair_ref.at[to], pair_place(s), pz_sem.at[d], p_sem.at[s], to, x))
        go(remote(down_ref.at[to], down_out.at[s], dz_sem.at[d], d_sem.at[s], to, x))

    def across(src_pair, src_down, d, s, go):
        for e in range(1, nx):
            to = lax.rem(x + e, nx)
            go(remote(src_pair, pair_place(s), px_sem.at[e - 1, d], p_sem.at[s], z, to))
            go(remote(src_down, down_out.at[s], dx_sem.at[e - 1, d], d_sem.at[s], z, to))

    def arrived(src_pair, src_down, s):
        remote(src_pair, pair_place(s), pz_sem.at[0], p_sem.at[s], z, x).wait_recv()
        remote(src_down, down_out.at[s], dz_sem.at[0], d_sem.at[s], z, x).wait_recv()

    start = lambda copy: copy.start()
    sent = lambda copy: copy.wait_send()

    flow(kv_ref, 0, z, start)
    mine = slot(z, x)
    pair_out[:, pl.ds(pl.multiple_of(mine * depth, depth), depth), :] = pair_ref[z]
    down_out[mine] = down_ref[z]
    kv_all[mine] = kv_ref[...]
    m_ref[...] = jnp.full_like(m_ref, -jnp.inf)
    l_ref[...] = jnp.zeros_like(l_ref)
    acc_ref[...] = jnp.zeros_like(acc_ref)

    def attend(s):
        for h in range(heads):
            v = kv_all[s, :, keys + h * width : keys + (h + 1) * width]
            for m in range(2):
                lane = (2 * h + m) * HD
                k = kv_all[s, :, lane : lane + HD]
                for r in range(0, rows_all, block):
                    rows = pl.ds(r, block)
                    q = q_ref[rows, lane : lane + HD] * jnp.bfloat16(HD**-0.5)
                    attend_chunk(q, k, v, m_ref, l_ref, acc_ref, 2 * h + m, rows)

    def step(k, _):
        zz, _off = nearest(k, z, nz)
        here = kv_all.at[slot(zz, x)]

        @pl.when(k > 0)
        def _():
            remote(kv_ref, here, up_sem.at[k], kv_sem.at[slot(zz, x)], z, x).wait_recv()
            flow(here, k, zz, start)

        @pl.when(k == min(1, nz - 1))
        def _():
            for d in range(1, nz):
                along(d, start)
            across(pair_ref.at[z], down_ref.at[z], 0, mine, start)

        def column(e, _):
            other = lax.rem(x - e + nx, nx)

            @pl.when(e > 0)
            def _():
                remote(kv_ref, here, up_sem.at[k], kv_sem.at[slot(zz, other)], z, x).wait_recv()

            attend(slot(zz, other))
            return 0

        lax.fori_loop(0, nx, column, 0)
        return 0

    lax.fori_loop(0, nz, step, 0)
    for d in range(1, nz):
        zz = lax.rem(z - d + nz, nz)
        s = slot(zz, x)
        arrived(pair_ref.at[z], down_ref.at[z], s)
        across(pair_place(s), down_out.at[s], d, s, start)
    finish_heads(heads, width, lam_ref, gain_ref, l_ref, acc_ref, out_ref)
    for d in range(nz):
        zz = lax.rem(z - d + nz, nz)
        for e in range(1, nx):
            arrived(pair_ref.at[z], down_ref.at[z], slot(zz, lax.rem(x - e + nx, nx)))
    for d in range(nz):
        zz = lax.rem(z - d + nz, nz)
        s = slot(zz, x)
        across(pair_place(s), down_out.at[s], d, s, sent)
        if d:
            along(d, sent)

    def settle(k, _):
        zz, _off = nearest(k, z, nz)
        flow(kv_ref, k, zz, sent)
        return 0

    lax.fori_loop(0, nz, settle, 0)


def gather_attend(nz, nx, queries, kv, lambdas, head_gain, pairs, downs):
    rows = queries.shape[0]
    heads = lambdas.shape[0]
    width = head_gain.shape[0]
    _, _, depth, mine = pairs.shape
    blocks = nz * nx
    vmem = pl.BlockSpec(memory_space=pltpu.VMEM)
    dma = pltpu.SemaphoreType.DMA
    side = max(nx - 1, 1)
    return pl.pallas_call(
        functools.partial(gather_attend_kernel, nz, nx, heads, 256),
        out_shape=[
            jax.ShapeDtypeStruct((rows, heads * width), jnp.bfloat16),
            jax.ShapeDtypeStruct((2, blocks * depth, mine), jnp.bfloat16),
            jax.ShapeDtypeStruct((blocks,) + downs.shape[1:], jnp.bfloat16),
        ],
        in_specs=[pl.BlockSpec(memory_space=pltpu.SMEM)] + [vmem] * 5,
        out_specs=[vmem] * 3,
        scratch_shapes=[pltpu.VMEM((blocks,) + kv.shape, jnp.bfloat16)]
        + [pltpu.VMEM((2 * heads, rows, width), jnp.float32)] * 3
        + [
            dma((nz,)), dma((nz,)), dma((side, nz)), dma((blocks,)),
            dma((nz,)), dma((nz,)), dma((side, nz)), dma((side, nz)), dma((blocks,)), dma((blocks,)),
        ],
        compiler_params=pltpu.CompilerParams(
            collective_id=0, has_side_effects=True, vmem_limit_bytes=60 * 1024 * 1024
        ),
        cost_estimate=pl.CostEstimate(
            flops=rows * rows * blocks * heads * 4096, bytes_accessed=4000000, transcendentals=0
        ),
        name="gather_attend",
    )(lambdas, queries, kv, head_gain.reshape(1, width), pairs, downs)


def gather_rows_kernel(nz, nt, own_ref, out_ref, up_sem, low_sem, y_sem, c_sem, got_sem):
    z, t = lax.axis_index("z"), lax.axis_index("tp")
    rows = own_ref.shape[0]
    partner = t + 1 - 2 * lax.rem(t, 2)

    barrier = pltpu.get_barrier_semaphore()
    for a in range(nz):
        for b in range(nt):
            if a + b > 0:
                pl.semaphore_signal(
                    barrier, inc=1,
                    device_id={"z": lax.rem(z + a, nz), "tp": lax.rem(t + b, nt)},
                    device_id_type=pl.DeviceIdType.MESH,
                )
    pl.semaphore_wait(barrier, nz * nt - 1)

    def place(zz, tt):
        s = zz * nt + tt
        return out_ref.at[pl.ds(pl.multiple_of(s * rows, rows), rows), :], got_sem.at[s]

    def remote(src, zz, tt, send, to_z, to_t):
        dst, recv = place(zz, tt)
        return pltpu.make_async_remote_copy(
            src_ref=src, dst_ref=dst, send_sem=send, recv_sem=recv,
            device_id={"z": to_z, "tp": to_t}, device_id_type=pl.DeviceIdType.MESH,
        )

    def flow(src, k, zz, go):
        @pl.when(jnp.logical_and(zz <= z, z < nz - 1))
        def _():
            go(remote(src, zz, t, up_sem.at[k], jnp.minimum(z + 1, nz - 1), t))

        @pl.when(jnp.logical_and(zz >= z, z > 0))
        def _():
            go(remote(src, zz, t, low_sem.at[k], jnp.maximum(z - 1, 0), t))

        for e in range(1, nt // 2):
            go(remote(src, zz, t, y_sem.at[k, e], z, lax.rem(t + 2 * e, nt)))
        go(remote(src, zz, t, c_sem.at[k, 0], z, partner))

    start = lambda copy: copy.start()
    sent = lambda copy: copy.wait_send()

    def await_block(zz, tt):
        remote(own_ref, zz, tt, c_sem.at[0, 0], z, partner).wait_recv()

    flow(own_ref, 0, z, start)
    mine, _sem = place(z, t)
    mine[...] = own_ref[...]

    def same_core(e):
        return lax.rem(t - 2 * e + nt, nt)

    def step(k, _):
        zz, _off = nearest(k, z, nz)

        @pl.when(k > 0)
        def _():
            await_block(zz, t)
            flow(place(zz, t)[0], k, zz, start)

        for e in range(1, nt // 2):
            tt = same_core(e)
            await_block(zz, tt)
            remote(place(zz, tt)[0], zz, tt, c_sem.at[k, e], z, partner).start()
        return 0

    lax.fori_loop(0, nz, step, 0)

    def settle(k, _):
        zz, _off = nearest(k, z, nz)
        flow(own_ref, k, zz, sent)
        for e in range(nt // 2):
            await_block(zz, lax.rem(partner - 2 * e + nt, nt))
            if e:
                tt = same_core(e)
                remote(own_ref, zz, tt, c_sem.at[k, e], z, partner).wait_send()
        return 0

    lax.fori_loop(0, nz, settle, 0)


def gather_rows(nz, nt, own):
    rows, width = own.shape
    if nt % 2:
        return lax.all_gather(own, ("z", "tp"), axis=0, tiled=True)
    vmem = pl.BlockSpec(memory_space=pltpu.VMEM)
    dma = pltpu.SemaphoreType.DMA
    return pl.pallas_call(
        functools.partial(gather_rows_kernel, nz, nt),
        out_shape=jax.ShapeDtypeStruct((nz * nt * rows, width), own.dtype),
        in_specs=[vmem],
        out_specs=vmem,
        scratch_shapes=[dma((nz,)), dma((nz,)), dma((nz, nt // 2)), dma((nz, nt // 2)), dma((nz * nt,))],
        compiler_params=pltpu.CompilerParams(
            collective_id=1, has_side_effects=True, vmem_limit_bytes=32 * 1024 * 1024
        ),
        cost_estimate=pl.CostEstimate(flops=10**10, bytes_accessed=4000000, transcendentals=0),
        name="gather_rows",
    )(own)


def per_device(
    nz, nx, residual, queries, key_pairs, values, lambdas, head_gain, w_out, norm_gain, w_gate, w_up, w_down
):
    local_rows = queries.shape[0]
    heads_here = lambdas.shape[0]
    value_width = head_gain.shape[0]
    d_rows, units = w_gate.shape
    mine = units // nz
    width = residual.shape[1]

    kv = jnp.concatenate([key_pairs, values], axis=1)
    pairs = jnp.stack([w_gate.reshape(d_rows, nz, mine), w_up.reshape(d_rows, nz, mine)], axis=2)
    pairs = jnp.transpose(pairs, (1, 2, 0, 3))
    heads_out, both, downs = gather_attend(
        nz, nx, queries, kv, lambdas, head_gain, pairs, w_down.reshape(nz, mine, w_down.shape[1])
    )
    gate, up = both[0], both[1]
    down = jnp.transpose(downs, (1, 0, 2)).reshape(mine, width)
    tp_index = lax.axis_index("tp")
    own_rows = local_rows // lax.axis_size("tp")
    w_mine = lax.dynamic_slice_in_dim(
        w_out, tp_index * heads_here * value_width, heads_here * value_width, 0
    )
    projected = lax.psum_scatter(
        jnp.dot(heads_out, w_mine, preferred_element_type=jnp.float32).astype(jnp.bfloat16),
        "tp",
        scatter_dimension=0,
        tiled=True,
    ).astype(jnp.float32)
    residual_own = lax.dynamic_slice_in_dim(residual, tp_index * own_rows, own_rows, 0)
    hidden_own = (residual_own.astype(jnp.float32) + projected).astype(jnp.bfloat16)
    stream_f = hidden_own.astype(jnp.float32)
    scaled = stream_f * lax.rsqrt(jnp.mean(stream_f * stream_f, axis=-1, keepdims=True) + 1e-05)
    normed_rows = gather_rows(nz, lax.axis_size("tp"), (scaled * norm_gain).astype(jnp.bfloat16))
    gate_sum = jnp.dot(normed_rows, gate, preferred_element_type=jnp.float32)
    up_sum = jnp.dot(normed_rows, up, preferred_element_type=jnp.float32)
    hidden_units = (jax.nn.silu(gate_sum) * up_sum).astype(jnp.bfloat16)
    ffn_out = lax.psum_scatter(
        jnp.dot(hidden_units, down, preferred_element_type=jnp.float32).astype(jnp.bfloat16),
        ("z", "tp"),
        scatter_dimension=0,
        tiled=True,
    ).astype(jnp.float32)
    return (hidden_own.astype(jnp.float32) + ffn_out).astype(jnp.bfloat16)


FIRST = 2


def layer_kernel(
    nz, nx, ny, nc,
    lam_ref, q_ref, k_ref, v_ref, gain_ref, norm_ref, res_ref, wout_ref, wg_ref, wu_ref, wd_ref,
    out_ref,
    q_all, qm, kv, vt, m_ref, l_ref, acc, ho, hg, wout, res, hidden, xs, wgu, wd, stage, stage_d, hb, part, r1, r2, r3,
    q_sem, qo_sem, qr_sem, kx_sem, kf_sem, kv_sem,
    gs_sem, gr_sem, gp_sem, gq_sem, ds_sem, dr_sem, dp_sem, dq_sem,
    wx_sem, st_sem, hs_sem, hr_sem, in_sem, xz_sem, xs_sem, xr_sem, rs_sem, rr_sem,
):
    z, x = lax.axis_index("z"), lax.axis_index("x")
    y, c = lax.axis_index("y"), lax.axis_index("c")
    z0 = lax.rem(z, 2)
    tokens = q_ref.shape[0]
    wide = v_ref.shape[1] // nx
    own_rows, width = out_ref.shape
    depth = wg_ref.shape[0]
    units, quarter = wg_ref.shape[1], wgu.shape[3]
    tp = y * nc + c
    xo, co = 1 - x, 1 - c
    here = dict(z=z, x=x, y=y, c=c)

    def remote(src, dst, send, recv, **to):
        return pltpu.make_async_remote_copy(
            src_ref=src, dst_ref=dst, send_sem=send, recv_sem=recv,
            device_id={**here, **to}, device_id_type=pl.DeviceIdType.MESH,
        )

    def lanes(i, n):
        return pl.ds(pl.multiple_of(i * n, n), n)

    local_in = [
        pltpu.make_async_copy(wout_ref, wout, in_sem.at[0]),
        pltpu.make_async_copy(res_ref.at[lanes(tp, own_rows), :], res, in_sem.at[1]),
    ]
    for copy in local_in:
        copy.start()

    barrier = pltpu.get_barrier_semaphore()
    peers = [dict(z=lax.rem(z + a, nz), x=lax.rem(x + b, nx)) for a in range(nz) for b in range(nx) if a + b]
    peers += [
        dict(x=lax.rem(x + b, nx), y=lax.rem(y + e, ny), c=lax.rem(c + f, nc))
        for b in range(nx) for e in range(ny) for f in range(nc) if e + f
    ]
    peers += [dict(p, z=z + 1 - 2 * z0) for p in peers if "y" in p]
    for to in peers:
        pl.semaphore_signal(barrier, inc=1, device_id={**here, **to}, device_id_type=pl.DeviceIdType.MESH)
    pl.semaphore_wait(barrier, len(peers))

    start = lambda copy: copy.start()
    sent = lambda copy: copy.wait_send()

    def slot(zz, xx):
        return zz * nx + xx

    mine = slot(z, x)

    def swap(go):
        go(remote(q_ref.at[:, lanes(xo, wide)], q_all.at[x], q_sem.at[0], q_sem.at[1], x=xo))
        go(remote(k_ref.at[:, lanes(xo, wide)], kv.at[mine, 0], kx_sem.at[0], kv_sem.at[mine], x=xo))
        go(remote(v_ref.at[:, lanes(xo, wide)], kv.at[mine, 1], kx_sem.at[1], kv_sem.at[mine], x=xo))

    halves = nz // 2
    inner = z0 == jnp.where(z < nz // 2, 1, 0)
    outer = jnp.logical_not(inner)

    def half(g):
        return lax.rem(z // 2 + g, halves)

    def flow(e, g, go):
        s = slot(z, lax.rem(x + e, nx))
        zd = 2 * half(g) + jnp.where(2 * half(g) < nz // 2, 1, 0)
        if e or go is sent:
            go(remote(kv.at[s], kv.at[s], kf_sem.at[g, e], kv_sem.at[s], z=zd))
        else:
            for i, ref in enumerate((k_ref, v_ref)):
                go(remote(ref.at[:, lanes(x, wide)], kv.at[s, i], kf_sem.at[g, e], kv_sem.at[s], z=zd))

    def relay(e, go):
        s = slot(z + 1 - 2 * z0, lax.rem(x + e, nx))
        if go is start:
            remote(kv.at[s], kv.at[s], kx_sem.at[0], kv_sem.at[s], x=xo).wait_recv()
        for g in range(1, halves):
            zd = 2 * half(g) + jnp.where(2 * half(g) < nz // 2, 1, 0)
            go(remote(kv.at[s], kv.at[s], kf_sem.at[g, nx + e], kv_sem.at[s], z=zd))

    def ask(e, go):
        src = q_all.at[xo] if e else q_ref.at[:, lanes(x, wide)]
        go(remote(src, q_all.at[nx + (xo if e else x)], qo_sem.at[e], qr_sem.at[xo if e else x], z=z + 1 - 2 * z0))

    def swapped():
        remote(kv.at[slot(z, xo)], kv.at[slot(z, xo)], kx_sem.at[0], kv_sem.at[slot(z, xo)], x=xo).wait_recv()

    def offset(q):
        return pl.multiple_of(jnp.minimum(q * quarter, units - quarter), 128)

    near = [(0, 1, b) for b in range(nx)]
    far = [(g, t, b) for b in range(nx) for g in range(1, halves) for t in range(2)]

    def units_of(xd, t):
        return pl.ds(offset(xd * 2 + lax.rem(z0 + t, 2)), quarter)

    def aside(go):
        rows = lanes(mine, depth)
        for i, ref in enumerate((wg_ref, wu_ref)):
            go(remote(ref.at[:, units_of(xo, 0)], wgu.at[c, i, rows, :], wx_sem.at[0, i], gr_sem.at[mine], x=xo))
        for i, ref in enumerate((wg_ref, wu_ref)):
            go(remote(ref.at[:, units_of(xo, 1)], stage.at[i], wx_sem.at[1, i], st_sem.at[0], x=xo))
        go(remote(wd_ref.at[units_of(xo, 0), :], wd.at[c, :, rows], wx_sem.at[0, 2], dr_sem.at[mine], x=xo))
        go(remote(wd_ref.at[units_of(xo, 1), :], stage_d, wx_sem.at[1, 2], st_sem.at[1], x=xo))

    def gate_up(to, go):
        g, t, b = to
        s = slot(z, lax.rem(x + b, nx))
        rows = lanes(s, depth)
        for i, ref in enumerate((wg_ref, wu_ref)):
            src = stage.at[i] if b and t else wgu.at[c, i, rows, :] if b else ref.at[:, units_of(x, t)]
            zd = half(g) * 2 + lax.rem(z0 + t, 2)
            go(remote(src, wgu.at[c, i, rows, :], gs_sem.at[g, t, b, i], gr_sem.at[s], z=zd))

    def downward(to, go):
        g, t, b = to
        s = slot(z, lax.rem(x + b, nx))
        cols = lanes(s, depth)
        src = stage_d if b and t else wd.at[c, :, cols] if b else wd_ref.at[units_of(x, t), :]
        zd = half(g) * 2 + lax.rem(z0 + t, 2)
        go(remote(src, wd.at[c, :, cols], ds_sem.at[g, t, b], dr_sem.at[s], z=zd))

    def aside_came(last):
        rows = lanes(slot(z, xo), depth)
        early = (wgu.at[c, :, rows, :], gr_sem.at[slot(z, xo)]), (stage, st_sem.at[0])
        late = (wd.at[c, :, rows], dr_sem.at[slot(z, xo)]), (stage_d, st_sem.at[1])
        for block, sem in late if last else early:
            remote(block, block, wx_sem.at[0, 0], sem, x=xo).wait_recv()

    q_me = x * 2 + z0
    own_weights = [
        pltpu.make_async_copy(ref.at[:, pl.ds(offset(q_me), quarter)], wgu.at[c, i, lanes(mine, depth), :], in_sem.at[2 + i])
        for i, ref in enumerate((wg_ref, wu_ref))
    ]
    own_weights.append(
        pltpu.make_async_copy(wd_ref.at[pl.ds(offset(q_me), quarter), :], wd.at[c, :, lanes(mine, depth)], in_sem.at[4])
    )

    swap(start)

    @pl.when(outer)
    def _():
        ask(0, start)
        flow(0, 0, start)

    @pl.when(inner)
    def _():
        for g in range(1, halves):
            flow(0, g, start)

    for copy in own_weights:
        copy.start()

    remote(q_all.at[x], q_all.at[xo], q_sem.at[0], q_sem.at[1], x=xo).wait_recv()

    @pl.when(outer)
    def _():
        ask(1, start)

    swapped()
    aside(start)

    @pl.when(inner)
    def _():
        for g in range(1, halves):
            flow(1, g, start)

    @pl.when(outer)
    def _():
        flow(1, 0, start)
        for e in range(nx):
            flow(e, 0, sent)
        for to in near + far[:FIRST]:
            if to == near[1]:
                aside_came(False)
            gate_up(to, start)
            gate_up(to, sent)

    def attend(s, low, high):
        vt[...] = kv[s, 1].astype(jnp.float32).T.astype(jnp.bfloat16)

        def pair(h, _):
            both = [2 * h, 2 * h + 1]
            scores = [
                lax.dot_general(kv[s, 0], qm[i], (((1,), (1,)), ((), ())), preferred_element_type=jnp.float32)
                for i in both
            ]
            olds = [m_ref[i] for i in both]
            highs = [jnp.maximum(o, jnp.max(t, axis=0, keepdims=True)) for o, t in zip(olds, scores)]
            weights = [jnp.exp(t - g) for t, g in zip(scores, highs)]
            mixed = [jnp.dot(vt[...], w.astype(jnp.bfloat16), preferred_element_type=jnp.float32) for w in weights]
            for i, o, g, w, t in zip(both, olds, highs, weights, mixed):
                shrink = jnp.exp(o - g)
                l_ref[i] = l_ref[i] * shrink + jnp.sum(w, axis=0, keepdims=True)
                m_ref[i] = g
                acc[i] = acc[i] * shrink + t
            return 0

        lax.fori_loop(low, high, pair, 0)

    def turn(j):
        mixed = jnp.logical_and(j >= nx, j < 3 * nx) if nz > 2 else False
        k = jnp.where(mixed, 1 + lax.rem(j, 2), j // nx)
        e = jnp.where(mixed, (j - nx) // 2, lax.rem(j, nx))
        zz, _off = nearest(k, z, nz)
        return zz, slot(zz, lax.rem(x + e, nx))

    def ready(low):
        for h in range(low, low + nx):
            q = q_all[h].astype(jnp.float32) * HD**-0.5
            qm[2 * h] = jnp.where(first_map, q, 0.0).astype(jnp.bfloat16)
            qm[2 * h + 1] = jnp.where(first_map, 0.0, q).astype(jnp.bfloat16)

    first_map = lax.broadcasted_iota(jnp.int32, (tokens, 2 * HD), 1) < HD

    def step(n, _):
        j = jnp.where(n < 2 * nx, lax.rem(n, nx), n - nx)
        zz, s = turn(j)

        @pl.when(n == nx)
        def _():
            for e in range(nx):
                remote(q_all.at[0], q_all.at[0], qo_sem.at[0], qr_sem.at[e], x=xo).wait_recv()
            ready(nx)

        for e in range(nx):
            @pl.when(n == nx + e)
            def _():
                relay(e, start)

        @pl.when(zz // 2 != z // 2)
        def _():
            remote(kv.at[s], kv.at[s], kx_sem.at[0], kv_sem.at[s], x=xo).wait_recv()

        def issue(at, some):
            @pl.when(j == min(at, nz * nx - 1))
            def _():
                for to in some:
                    gate_up(to, start)

        issue(2, near[:1])

        @pl.when(j == min(4, nz * nx - 1))
        def _():
            for e in range(nx):
                relay(e, sent)

        issue(4, [to for to in far if to[1:] == (1, 0)])

        @pl.when(j == min(5, nz * nx - 1))
        def _():
            aside_came(False)

        issue(5, near[1:])
        issue(6, [to for to in far if to[1:] == (1, 1)])
        attend(s, jnp.where(jnp.logical_and(n >= nx, n < 2 * nx), nx, 0), jnp.where(n < nx, nx, 2 * nx))
        return 0

    head = tp * nx + x
    me = (x * ny + y) * nc + c

    def spread(go):
        for b in range(nx):
            for e in range(ny):
                for f in range(nc):
                    xd, yd, cd = lax.rem(x + b, nx), lax.rem(y + e, ny), lax.rem(c + f, nc)
                    for p in range(0 if b + e + f else 1, 2):
                        n = ((b * ny + e) * nc + f) * 2 + p
                        src = ho.at[p * nx + xd, lanes(yd * nc + cd, own_rows), :]
                        zd = z + p * (1 - 2 * z0)
                        go(remote(src, hg.at[:, lanes(head, wide)], hs_sem.at[n], hr_sem.at[me], z=zd, x=xd, y=yd, c=cd))

    @pl.when(inner)
    def _():
        kv[mine, 0] = k_ref[:, lanes(x, wide)]
        kv[mine, 1] = v_ref[:, lanes(x, wide)]
        q_all[x] = q_ref[:, lanes(x, wide)]
        m_ref[...] = jnp.full_like(m_ref, -jnp.inf)
        l_ref[...] = jnp.zeros_like(l_ref)
        acc[...] = jnp.zeros_like(acc)
        ready(0)
        lax.fori_loop(0, nz * nx + nx, step, 0)

        def finish(h, _):
            first = acc[2 * h] / l_ref[2 * h]
            second = acc[2 * h + 1] / l_ref[2 * h + 1]
            differ = first - lam_ref[x] * second
            scale = lax.rsqrt(jnp.mean(differ * differ, axis=0, keepdims=True) + 1e-05)
            ho[h] = (differ * scale * gain_ref[...]).T.astype(jnp.bfloat16)
            return 0

        lax.fori_loop(0, 2 * nx, finish, 0)
        spread(start)
        hg[:, lanes(head, wide)] = ho[x, lanes(tp, own_rows), :]

    for copy in local_in:
        copy.wait()
    for b in range(nx):
        for e in range(ny):
            for f in range(nc):
                xd, yd, cd = lax.rem(x + b, nx), lax.rem(y + e, ny), lax.rem(c + f, nc)
                other = (xd * ny + yd) * nc + cd
                block = hg.at[:, lanes((yd * nc + cd) * nx + xd, wide)]

                def came():
                    remote(block, block, hs_sem.at[0], hr_sem.at[other], x=xo).wait_recv()

                if b + e + f:
                    came()
                else:
                    pl.when(outer)(came)

    state = res[...].astype(jnp.float32) + jnp.dot(hg[...], wout[...], preferred_element_type=jnp.float32)
    hidden[...] = state.astype(jnp.bfloat16)
    stream = hidden[...].astype(jnp.float32)
    scaled = stream * lax.rsqrt(jnp.mean(stream * stream, axis=1, keepdims=True) + 1e-05)
    cube = z0 * 4 + x * 2 + y
    xs[cube] = (scaled * norm_ref[...]).astype(jnp.bfloat16)

    bits = dict(z=(z0, 4), x=(x, 2), y=(y, 1))
    across = dict(z=dict(z=z + 1 - 2 * z0), x=dict(x=xo), y=dict(y=1 - y))
    paths = (("x", "y"), ("y", "x"))
    split = width // 256 * 128
    columns = (pl.ds(0, split), pl.ds(split, width - split))

    def flip(axis):
        bit, mask = bits[axis]
        return (1 - 2 * bit) * mask

    over = cube + flip("z")

    def lend(p, go):
        block = xs.at[cube, :, columns[p]]
        go(remote(block, block, xz_sem.at[p, 0], xz_sem.at[p, 1], **across["z"]))

    def gather(h, p, k, go):
        held = [(cube, over)[h]]
        if k:
            held += [held[0] + flip(paths[p][0])]
        for n, i in enumerate(held):
            block = xs.at[i, :, columns[p]]
            go(remote(block, block, xs_sem.at[h, p, k, n], xr_sem.at[h, p, k], **across[paths[p][k]]))

    def gathered(h, p, k):
        block = xs.at[pl.ds(0, 2**k), :, columns[p]]
        remote(block, block, xs_sem.at[h, p, k, 0], xr_sem.at[h, p, k], x=xo).wait_recv()

    for p in range(2):
        lend(p, start)
        gather(0, p, 0, start)

    @pl.when(outer)
    def _():
        for to in far[FIRST:]:
            gate_up(to, start)

    for p in range(2):
        gathered(0, p, 0)
        gather(0, p, 1, start)

    @pl.when(inner)
    def _():
        for to in far:
            if to[1] == 0:
                gate_up(to, start)

    for p in range(2):
        block = xs.at[over, :, columns[p]]
        remote(block, block, xz_sem.at[p, 0], xz_sem.at[p, 1], x=xo).wait_recv()
        gather(1, p, 0, start)
    for p in range(2):
        gathered(1, p, 0)
        gather(1, p, 1, start)
    def pass_on(s, go):
        block = wgu.at[c, :, lanes(s, depth), :]
        go(remote(block, block, gp_sem.at[s], gq_sem.at[s], c=co))

    def fill(j, _):
        s = lax.rem(z * nx + jnp.where(z < nz // 2, j, nx - 1 - j + nz * nx), nz * nx)

        @pl.when(s // nx != z)
        def _():
            block = wgu.at[c, :, lanes(s, depth), :]
            remote(block, block, gp_sem.at[s], gr_sem.at[s], c=co).wait_recv()

        pass_on(s, start)
        return 0

    def filled(s, _):
        block = wgu.at[co, :, lanes(s, depth), :]
        remote(block, block, gp_sem.at[s], gq_sem.at[s], c=co).wait_recv()
        return 0

    aside_came(True)

    @pl.when(outer)
    def _():
        for to in far[FIRST:]:
            gate_up(to, sent)
        for to in near + [to for to in far if to[1] == 0] + [to for to in far if to[1]]:
            downward(to, start)

    @pl.when(inner)
    def _():
        for to in far:
            if to[1]:
                downward(to, start)

    for copy in own_weights:
        copy.wait()
    lax.fori_loop(0, nz * nx, fill, 0)
    @pl.when(inner)
    def _():
        for to in near + far:
            gate_up(to, sent)
        for to in near + [to for to in far if to[1] == 0]:
            downward(to, start)

    lax.fori_loop(0, nz * nx, filled, 0)
    for h in range(2):
        for p in range(2):
            gathered(h, p, 1)

    blocks, group = 8, 4
    rows = group * own_rows
    spare = q_me * quarter - jnp.minimum(q_me * quarter, units - quarter)
    keep = lax.broadcasted_iota(jnp.int32, (rows, quarter), 1) >= spare

    def expand(i, _):
        both = xs[pl.ds(group * i, group)].reshape(rows, width)
        for cc in range(nc):
            gate = jnp.dot(both, wgu[cc, 0], preferred_element_type=jnp.float32)
            up = jnp.dot(both, wgu[cc, 1], preferred_element_type=jnp.float32)
            made = gate / (1.0 + jnp.exp(-gate)) * up
            hb[lanes(i, rows), cc * quarter : (cc + 1) * quarter] = jnp.where(keep, made, 0.0).astype(jnp.bfloat16)
        return 0

    lax.fori_loop(0, blocks // group, expand, 0)
    def place(p, flips):
        return cube + sum(flip(axis) for axis in flips)

    def choices(axes):
        sets = [()]
        for axis in axes:
            sets = sets + [t + (axis,) for t in sets]
        return sets

    held_in = (r1, r2, r3)
    spare_z = (("x", "y", "z"), ("y", "x", "z"))
    even = (("x", "y", "z"), ("y", "z", "x"), ("z", "x", "y"))
    orders = [even if g == halves - 1 else spare_z for g in range(halves)]
    span = width // halves
    tiles = span // 128
    cuts = [[0] + [128 * ((tiles * (i + 1) + len(o) - 1) // len(o)) for i in range(len(o))] for o in orders]

    def share(g, p):
        return pl.ds(pl.multiple_of(half(g) * span + cuts[g][p], 128), cuts[g][p + 1] - cuts[g][p])

    def down_on(s, go):
        block = wd.at[c, :, lanes(s, depth)]
        go(remote(block, block, dp_sem.at[s], dq_sem.at[s], c=co))

    def down_fill(g):
        def one(n, _):
            s = half(g) * 2 * nx + n

            @pl.when(s // nx != z)
            def _():
                block = wd.at[c, :, lanes(s, depth)]
                remote(block, block, dp_sem.at[s], dr_sem.at[s], c=co).wait_recv()

            down_on(s, start)
            return 0

        def other(n, _):
            s = half(g) * 2 * nx + n
            block = wd.at[co, :, lanes(s, depth)]
            remote(block, block, dp_sem.at[s], dq_sem.at[s], c=co).wait_recv()
            return 0

        lax.fori_loop(0, 2 * nx, one, 0)
        lax.fori_loop(0, 2 * nx, other, 0)

    def reduce_send(g, p, k, go):
        axis, rest = orders[g][p][k], orders[g][p][k + 1 :]
        for n, t in enumerate(choices(rest)):
            spot = sum((bits[a][0] if a not in t else 1 - bits[a][0]) * 2**i for i, a in enumerate(rest))
            src = part.at[place(p, t + (axis,)), :, share(g, p)]
            dst = held_in[k].at[spot, :, share(g, p)]
            go(remote(src, dst, rs_sem.at[g, p, k, n], rr_sem.at[g, p, k], **across[axis]))

    def reduce_take(g, p, k):
        axis, rest = orders[g][p][k], orders[g][p][k + 1 :]
        cols = share(g, p)
        block = held_in[k].at[:, :, cols]
        remote(block, block, rs_sem.at[g, p, k, 0], rr_sem.at[g, p, k], x=xo).wait_recv()
        for t in reversed(choices(rest)) if rest else ():
            spot = sum((bits[a][0] if a not in t else 1 - bits[a][0]) * 2**i for i, a in enumerate(rest))
            i = place(p, t)
            part[i, :, cols] = (
                part[i, :, cols].astype(jnp.float32) + held_in[k][spot, :, cols].astype(jnp.float32)
            ).astype(jnp.bfloat16)
        if not rest:
            out_ref[:, cols] = (
                hidden[:, cols].astype(jnp.float32)
                + part[cube, :, cols].astype(jnp.float32)
                + held_in[k][0, :, cols].astype(jnp.float32)
            ).astype(jnp.bfloat16)

    for g in range(halves):
        down_fill(g)
        for p in range(len(orders[g])):
            def contract(i, _):
                weights = wd[:, :, share(g, p)].reshape(nc * quarter, cuts[g][p + 1] - cuts[g][p])
                made = jnp.dot(hb[lanes(i, rows), :], weights, preferred_element_type=jnp.float32)
                part[pl.ds(group * i, group), :, share(g, p)] = made.astype(jnp.bfloat16).reshape(group, own_rows, -1)
                return 0

            lax.fori_loop(0, blocks // group, contract, 0)
            reduce_send(g, p, 0, start)
        for p in range(len(orders[g])):
            reduce_take(g, p, 0)
            reduce_send(g, p, 1, start)
        if g:
            for p in range(len(orders[g - 1])):
                reduce_take(g - 1, p, 1)
                reduce_send(g - 1, p, 2, start)
    for p in range(len(orders[halves - 1])):
        reduce_take(halves - 1, p, 1)
        reduce_send(halves - 1, p, 2, start)
    for g in range(halves):
        for p in range(len(orders[g])):
            reduce_take(g, p, 2)

    swap(sent)

    @pl.when(outer)
    def _():
        for e in range(nx):
            ask(e, sent)

    @pl.when(inner)
    def _():
        for e in range(nx):
            for g in range(1, halves):
                flow(e, g, sent)
        spread(sent)

    aside(sent)
    for to in near + far:
        downward(to, sent)
    for p in range(2):
        lend(p, sent)
        for h in range(2):
            for k in range(2):
                gather(h, p, k, sent)
    for k in range(3):
        for g in range(halves):
            for p in range(len(orders[g])):
                reduce_send(g, p, k, sent)

    def passed(s, _):
        pass_on(s, sent)
        down_on(s, sent)
        return 0

    lax.fori_loop(0, nz * nx, passed, 0)


def layer(
    nz, nx, ny, nc, residual, queries, key_pairs, values, lambdas, head_gain, w_out, norm_gain, w_gate, w_up, w_down
):
    tokens = queries.shape[0]
    wide = head_gain.shape[0]
    width = residual.shape[1]
    depth, units = w_gate.shape
    own_rows = tokens // (ny * nc)
    quarter = -(-units // (2 * nx * 128)) * 128
    vmem = pl.BlockSpec(memory_space=pltpu.VMEM)
    hbm = pl.BlockSpec(memory_space=pl.ANY)
    dma = pltpu.SemaphoreType.DMA
    bf16 = lambda *shape: pltpu.VMEM(shape, jnp.bfloat16)
    f32 = lambda *shape: pltpu.VMEM(shape, jnp.float32)
    n = nz * nx
    return pl.pallas_call(
        functools.partial(layer_kernel, nz, nx, ny, nc),
        out_shape=jax.ShapeDtypeStruct((own_rows, width), jnp.bfloat16),
        in_specs=[pl.BlockSpec(memory_space=pltpu.SMEM)] + [vmem] * 5 + [hbm] * 5,
        out_specs=vmem,
        scratch_shapes=[
            bf16(2 * nx, tokens, wide), bf16(4 * nx, tokens, wide), bf16(n, 2, tokens, wide), bf16(wide, tokens),
            f32(4 * nx, 1, tokens), f32(4 * nx, 1, tokens), f32(4 * nx, wide, tokens),
            bf16(2 * nx, tokens, wide), bf16(own_rows, w_out.shape[0]),
            bf16(*w_out.shape), bf16(own_rows, width), bf16(own_rows, width),
            bf16(8, own_rows, width), bf16(nc, 2, width, quarter), bf16(nc, quarter, width),
            bf16(2, depth, quarter), bf16(quarter, depth),
            bf16(8 * own_rows, nc * quarter), bf16(8, own_rows, width),
            bf16(4, own_rows, width), bf16(2, own_rows, width), bf16(1, own_rows, width),
            dma((2,)), dma((nx,)), dma((nx,)), dma((2,)), dma((nz // 2, 2 * nx)), dma((n,)),
            dma((nz // 2, 2, nx, 2)), dma((n,)), dma((n,)), dma((n,)),
            dma((nz // 2, 2, nx)), dma((n,)), dma((n,)), dma((n,)),
            dma((2, 3)), dma((2,)), dma((2 * nx * ny * nc,)), dma((nx * ny * nc,)), dma((5,)),
            dma((2, 2)), dma((2, 2, 2, 2)), dma((2, 2, 2)), dma((nz // 2, 3, 3, 4)), dma((nz // 2, 3, 3)),
        ],
        compiler_params=pltpu.CompilerParams(
            collective_id=2, has_side_effects=True, vmem_limit_bytes=62 * 1024 * 1024
        ),
        name="layer",
    )(
        lambdas, queries, key_pairs, values, head_gain.reshape(wide, 1), norm_gain.reshape(1, width),
        residual, w_out, w_gate, w_up, w_down,
    )


def solution(mesh):
    sp, tp = mesh.shape["sp"], mesh.shape["tp"]
    coords = [getattr(d, "coords", None) for d in mesh.devices.flat]
    known = all(p is not None for p in coords)
    nx = len({p[0] for p in coords}) if known else 2
    ny = len({p[1] for p in coords}) if known else 2
    if sp % nx:
        nx = 1
    if tp % ny:
        ny = 1
    nz, nc = sp // nx, tp // ny
    zx, yc = ("z", "x"), ("y", "c")

    def placed(tp_axes):
        split = P(zx, tp_axes)
        return (P(zx, None), split, split, split, P(tp_axes), P(), P(), P(), split, split, P(tp_axes, zx))

    def run(*args):
        heads, units = args[4].shape[0], args[8].shape[1] // tp
        if nx == ny == nc == 2 and nz % 2 == 0 and heads == tp * nx and units % 128 == 0:
            box = Mesh(np.asarray(mesh.devices).reshape(nz, nx, ny, nc), ("z", "x", "y", "c"))
            body, tp_axes = functools.partial(layer, nz, nx, ny, nc), yc
        else:
            box = Mesh(np.asarray(mesh.devices).reshape(nz, nx, tp), ("z", "x", "tp"))
            body, tp_axes = functools.partial(per_device, nz, nx), ("tp",)
        return jax.shard_map(
            body, mesh=box, in_specs=placed(tp_axes), out_specs=P(zx + tp_axes, None), check_vma=False
        )(*args)

    return run
```

```python
import functools

import jax
import jax.numpy as jnp
import numpy as np
from jax import lax
from jax.experimental import pallas as pl
from jax.experimental.pallas import tpu as pltpu
from jax.sharding import Mesh, PartitionSpec as P

HD = 64


def attend_chunk(q, k, v, m_ref, l_ref, acc_ref, slot, rows):
    scores = lax.dot_general(
        q, k, (((1,), (1,)), ((), ())), preferred_element_type=jnp.float32
    )
    old = m_ref[slot, rows, :]
    high = jnp.maximum(old, jnp.max(scores, axis=1, keepdims=True))
    shrink = jnp.exp(old - high)
    weights = jnp.exp(scores - high[:, :1])
    l_ref[slot, rows, :] = l_ref[slot, rows, :] * shrink + jnp.sum(weights, axis=1, keepdims=True)
    m_ref[slot, rows, :] = high
    acc_ref[slot, rows, :] = acc_ref[slot, rows, :] * shrink + jnp.dot(
        weights.astype(jnp.bfloat16), v, preferred_element_type=jnp.float32
    )


def finish_heads(heads, width, lam_ref, gain_ref, l_ref, acc_ref, out_ref):
    for h in range(heads):
        first = acc_ref[2 * h] / l_ref[2 * h]
        second = acc_ref[2 * h + 1] / l_ref[2 * h + 1]
        differ = first - lam_ref[h] * second
        scale = lax.rsqrt(jnp.mean(differ * differ, axis=1, keepdims=True) + 1e-05)
        out_ref[:, h * width : (h + 1) * width] = (differ * scale * gain_ref[...]).astype(out_ref.dtype)


def nearest(k, me, n):
    low, high = me, n - 1 - me
    edge = jnp.minimum(low, high)
    side = jnp.where(high >= low, 1, -1)
    near = jnp.where(k % 2 == 1, 1, -1) * ((k + 1) // 2)
    off = side * jnp.where(k <= 2 * edge, near, k - edge)
    return me + off, off


def gather_attend_kernel(
    nz, nx, heads, block,
    lam_ref, q_ref, kv_ref, gain_ref, pair_ref, down_ref,
    out_ref, pair_out, down_out,
    kv_all, m_ref, l_ref, acc_ref,
    up_sem, low_sem, side_sem, kv_sem, pz_sem, dz_sem, px_sem, dx_sem, p_sem, d_sem,
):
    z, x = lax.axis_index("z"), lax.axis_index("x")
    rows_all = q_ref.shape[0]
    width = out_ref.shape[1] // heads
    keys = heads * 2 * HD
    depth = pair_ref.shape[2]

    def remote(src, dst, send, recv, zz, xx):
        return pltpu.make_async_remote_copy(
            src_ref=src, dst_ref=dst, send_sem=send, recv_sem=recv,
            device_id={"z": zz, "x": xx}, device_id_type=pl.DeviceIdType.MESH,
        )

    barrier = pltpu.get_barrier_semaphore()
    for a in range(nz):
        for b in range(nx):
            if a + b > 0:
                pl.semaphore_signal(
                    barrier, inc=1,
                    device_id={"z": lax.rem(z + a, nz), "x": lax.rem(x + b, nx)},
                    device_id_type=pl.DeviceIdType.MESH,
                )
    pl.semaphore_wait(barrier, nz * nx - 1)

    def slot(zz, xx):
        return zz * nx + xx

    def flow(src, k, zz, go):
        off = zz - z
        here = kv_all.at[slot(zz, x)]

        @pl.when(jnp.logical_and(off <= 0, z < nz - 1))
        def _():
            go(remote(src, here, up_sem.at[k], kv_sem.at[slot(zz, x)], jnp.minimum(z + 1, nz - 1), x))

        @pl.when(jnp.logical_and(off >= 0, z > 0))
        def _():
            go(remote(src, here, low_sem.at[k], kv_sem.at[slot(zz, x)], jnp.maximum(z - 1, 0), x))

        for e in range(1, nx):
            go(remote(src, here, side_sem.at[e - 1, k], kv_sem.at[slot(zz, x)], z, lax.rem(x + e, nx)))

    def pair_place(s):
        return pair_out.at[:, pl.ds(pl.multiple_of(s * depth, depth), depth), :]

    def along(d, go):
        to = lax.rem(z + d, nz)
        s = slot(z, x)
        go(remote(pair_ref.at[to], pair_place(s), pz_sem.at[d], p_sem.at[s], to, x))
        go(remote(down_ref.at[to], down_out.at[s], dz_sem.at[d], d_sem.at[s], to, x))

    def across(src_pair, src_down, d, s, go):
        for e in range(1, nx):
            to = lax.rem(x + e, nx)
            go(remote(src_pair, pair_place(s), px_sem.at[e - 1, d], p_sem.at[s], z, to))
            go(remote(src_down, down_out.at[s], dx_sem.at[e - 1, d], d_sem.at[s], z, to))

    def arrived(src_pair, src_down, s):
        remote(src_pair, pair_place(s), pz_sem.at[0], p_sem.at[s], z, x).wait_recv()
        remote(src_down, down_out.at[s], dz_sem.at[0], d_sem.at[s], z, x).wait_recv()

    start = lambda copy: copy.start()
    sent = lambda copy: copy.wait_send()

    flow(kv_ref, 0, z, start)
    mine = slot(z, x)
    pair_out[:, pl.ds(pl.multiple_of(mine * depth, depth), depth), :] = pair_ref[z]
    down_out[mine] = down_ref[z]
    kv_all[mine] = kv_ref[...]
    m_ref[...] = jnp.full_like(m_ref, -jnp.inf)
    l_ref[...] = jnp.zeros_like(l_ref)
    acc_ref[...] = jnp.zeros_like(acc_ref)

    def attend(s):
        for h in range(heads):
            v = kv_all[s, :, keys + h * width : keys + (h + 1) * width]
            for m in range(2):
                lane = (2 * h + m) * HD
                k = kv_all[s, :, lane : lane + HD]
                for r in range(0, rows_all, block):
                    rows = pl.ds(r, block)
                    q = q_ref[rows, lane : lane + HD] * jnp.bfloat16(HD**-0.5)
                    attend_chunk(q, k, v, m_ref, l_ref, acc_ref, 2 * h + m, rows)

    def step(k, _):
        zz, _off = nearest(k, z, nz)
        here = kv_all.at[slot(zz, x)]

        @pl.when(k > 0)
        def _():
            remote(kv_ref, here, up_sem.at[k], kv_sem.at[slot(zz, x)], z, x).wait_recv()
            flow(here, k, zz, start)

        @pl.when(k == min(1, nz - 1))
        def _():
            for d in range(1, nz):
                along(d, start)
            across(pair_ref.at[z], down_ref.at[z], 0, mine, start)

        def column(e, _):
            other = lax.rem(x - e + nx, nx)

            @pl.when(e > 0)
            def _():
                remote(kv_ref, here, up_sem.at[k], kv_sem.at[slot(zz, other)], z, x).wait_recv()

            attend(slot(zz, other))
            return 0

        lax.fori_loop(0, nx, column, 0)
        return 0

    lax.fori_loop(0, nz, step, 0)
    for d in range(1, nz):
        zz = lax.rem(z - d + nz, nz)
        s = slot(zz, x)
        arrived(pair_ref.at[z], down_ref.at[z], s)
        across(pair_place(s), down_out.at[s], d, s, start)
    finish_heads(heads, width, lam_ref, gain_ref, l_ref, acc_ref, out_ref)
    for d in range(nz):
        zz = lax.rem(z - d + nz, nz)
        for e in range(1, nx):
            arrived(pair_ref.at[z], down_ref.at[z], slot(zz, lax.rem(x - e + nx, nx)))
    for d in range(nz):
        zz = lax.rem(z - d + nz, nz)
        s = slot(zz, x)
        across(pair_place(s), down_out.at[s], d, s, sent)
        if d:
            along(d, sent)

    def settle(k, _):
        zz, _off = nearest(k, z, nz)
        flow(kv_ref, k, zz, sent)
        return 0

    lax.fori_loop(0, nz, settle, 0)


def gather_attend(nz, nx, queries, kv, lambdas, head_gain, pairs, downs):
    rows = queries.shape[0]
    heads = lambdas.shape[0]
    width = head_gain.shape[0]
    _, _, depth, mine = pairs.shape
    blocks = nz * nx
    vmem = pl.BlockSpec(memory_space=pltpu.VMEM)
    dma = pltpu.SemaphoreType.DMA
    side = max(nx - 1, 1)
    return pl.pallas_call(
        functools.partial(gather_attend_kernel, nz, nx, heads, 256),
        out_shape=[
            jax.ShapeDtypeStruct((rows, heads * width), jnp.bfloat16),
            jax.ShapeDtypeStruct((2, blocks * depth, mine), jnp.bfloat16),
            jax.ShapeDtypeStruct((blocks,) + downs.shape[1:], jnp.bfloat16),
        ],
        in_specs=[pl.BlockSpec(memory_space=pltpu.SMEM)] + [vmem] * 5,
        out_specs=[vmem] * 3,
        scratch_shapes=[pltpu.VMEM((blocks,) + kv.shape, jnp.bfloat16)]
        + [pltpu.VMEM((2 * heads, rows, width), jnp.float32)] * 3
        + [
            dma((nz,)), dma((nz,)), dma((side, nz)), dma((blocks,)),
            dma((nz,)), dma((nz,)), dma((side, nz)), dma((side, nz)), dma((blocks,)), dma((blocks,)),
        ],
        compiler_params=pltpu.CompilerParams(
            collective_id=0, has_side_effects=True, vmem_limit_bytes=60 * 1024 * 1024
        ),
        cost_estimate=pl.CostEstimate(
            flops=rows * rows * blocks * heads * 4096, bytes_accessed=4000000, transcendentals=0
        ),
        name="gather_attend",
    )(lambdas, queries, kv, head_gain.reshape(1, width), pairs, downs)


def gather_rows_kernel(nz, nt, own_ref, out_ref, up_sem, low_sem, y_sem, c_sem, got_sem):
    z, t = lax.axis_index("z"), lax.axis_index("tp")
    rows = own_ref.shape[0]
    partner = t + 1 - 2 * lax.rem(t, 2)

    barrier = pltpu.get_barrier_semaphore()
    for a in range(nz):
        for b in range(nt):
            if a + b > 0:
                pl.semaphore_signal(
                    barrier, inc=1,
                    device_id={"z": lax.rem(z + a, nz), "tp": lax.rem(t + b, nt)},
                    device_id_type=pl.DeviceIdType.MESH,
                )
    pl.semaphore_wait(barrier, nz * nt - 1)

    def place(zz, tt):
        s = zz * nt + tt
        return out_ref.at[pl.ds(pl.multiple_of(s * rows, rows), rows), :], got_sem.at[s]

    def remote(src, zz, tt, send, to_z, to_t):
        dst, recv = place(zz, tt)
        return pltpu.make_async_remote_copy(
            src_ref=src, dst_ref=dst, send_sem=send, recv_sem=recv,
            device_id={"z": to_z, "tp": to_t}, device_id_type=pl.DeviceIdType.MESH,
        )

    def flow(src, k, zz, go):
        @pl.when(jnp.logical_and(zz <= z, z < nz - 1))
        def _():
            go(remote(src, zz, t, up_sem.at[k], jnp.minimum(z + 1, nz - 1), t))

        @pl.when(jnp.logical_and(zz >= z, z > 0))
        def _():
            go(remote(src, zz, t, low_sem.at[k], jnp.maximum(z - 1, 0), t))

        for e in range(1, nt // 2):
            go(remote(src, zz, t, y_sem.at[k, e], z, lax.rem(t + 2 * e, nt)))
        go(remote(src, zz, t, c_sem.at[k, 0], z, partner))

    start = lambda copy: copy.start()
    sent = lambda copy: copy.wait_send()

    def await_block(zz, tt):
        remote(own_ref, zz, tt, c_sem.at[0, 0], z, partner).wait_recv()

    flow(own_ref, 0, z, start)
    mine, _sem = place(z, t)
    mine[...] = own_ref[...]

    def same_core(e):
        return lax.rem(t - 2 * e + nt, nt)

    def step(k, _):
        zz, _off = nearest(k, z, nz)

        @pl.when(k > 0)
        def _():
            await_block(zz, t)
            flow(place(zz, t)[0], k, zz, start)

        for e in range(1, nt // 2):
            tt = same_core(e)
            await_block(zz, tt)
            remote(place(zz, tt)[0], zz, tt, c_sem.at[k, e], z, partner).start()
        return 0

    lax.fori_loop(0, nz, step, 0)

    def settle(k, _):
        zz, _off = nearest(k, z, nz)
        flow(own_ref, k, zz, sent)
        for e in range(nt // 2):
            await_block(zz, lax.rem(partner - 2 * e + nt, nt))
            if e:
                tt = same_core(e)
                remote(own_ref, zz, tt, c_sem.at[k, e], z, partner).wait_send()
        return 0

    lax.fori_loop(0, nz, settle, 0)


def gather_rows(nz, nt, own):
    rows, width = own.shape
    if nt % 2:
        return lax.all_gather(own, ("z", "tp"), axis=0, tiled=True)
    vmem = pl.BlockSpec(memory_space=pltpu.VMEM)
    dma = pltpu.SemaphoreType.DMA
    return pl.pallas_call(
        functools.partial(gather_rows_kernel, nz, nt),
        out_shape=jax.ShapeDtypeStruct((nz * nt * rows, width), own.dtype),
        in_specs=[vmem],
        out_specs=vmem,
        scratch_shapes=[dma((nz,)), dma((nz,)), dma((nz, nt // 2)), dma((nz, nt // 2)), dma((nz * nt,))],
        compiler_params=pltpu.CompilerParams(
            collective_id=1, has_side_effects=True, vmem_limit_bytes=32 * 1024 * 1024
        ),
        cost_estimate=pl.CostEstimate(flops=10**10, bytes_accessed=4000000, transcendentals=0),
        name="gather_rows",
    )(own)


def per_device(
    nz, nx, residual, queries, key_pairs, values, lambdas, head_gain, w_out, norm_gain, w_gate, w_up, w_down
):
    local_rows = queries.shape[0]
    heads_here = lambdas.shape[0]
    value_width = head_gain.shape[0]
    d_rows, units = w_gate.shape
    mine = units // nz
    width = residual.shape[1]

    kv = jnp.concatenate([key_pairs, values], axis=1)
    pairs = jnp.stack([w_gate.reshape(d_rows, nz, mine), w_up.reshape(d_rows, nz, mine)], axis=2)
    pairs = jnp.transpose(pairs, (1, 2, 0, 3))
    heads_out, both, downs = gather_attend(
        nz, nx, queries, kv, lambdas, head_gain, pairs, w_down.reshape(nz, mine, w_down.shape[1])
    )
    gate, up = both[0], both[1]
    down = jnp.transpose(downs, (1, 0, 2)).reshape(mine, width)
    tp_index = lax.axis_index("tp")
    own_rows = local_rows // lax.axis_size("tp")
    w_mine = lax.dynamic_slice_in_dim(
        w_out, tp_index * heads_here * value_width, heads_here * value_width, 0
    )
    projected = lax.psum_scatter(
        jnp.dot(heads_out, w_mine, preferred_element_type=jnp.float32).astype(jnp.bfloat16),
        "tp",
        scatter_dimension=0,
        tiled=True,
    ).astype(jnp.float32)
    residual_own = lax.dynamic_slice_in_dim(residual, tp_index * own_rows, own_rows, 0)
    hidden_own = (residual_own.astype(jnp.float32) + projected).astype(jnp.bfloat16)
    stream_f = hidden_own.astype(jnp.float32)
    scaled = stream_f * lax.rsqrt(jnp.mean(stream_f * stream_f, axis=-1, keepdims=True) + 1e-05)
    normed_rows = gather_rows(nz, lax.axis_size("tp"), (scaled * norm_gain).astype(jnp.bfloat16))
    gate_sum = jnp.dot(normed_rows, gate, preferred_element_type=jnp.float32)
    up_sum = jnp.dot(normed_rows, up, preferred_element_type=jnp.float32)
    hidden_units = (jax.nn.silu(gate_sum) * up_sum).astype(jnp.bfloat16)
    ffn_out = lax.psum_scatter(
        jnp.dot(hidden_units, down, preferred_element_type=jnp.float32).astype(jnp.bfloat16),
        ("z", "tp"),
        scatter_dimension=0,
        tiled=True,
    ).astype(jnp.float32)
    return (hidden_own.astype(jnp.float32) + ffn_out).astype(jnp.bfloat16)


FIRST = 2


def layer_kernel(
    nz, nx, ny, nc,
    lam_ref, q_ref, k_ref, v_ref, gain_ref, norm_ref, res_ref, wout_ref, wg_ref, wu_ref, wd_ref,
    out_ref,
    q_all, qm, kv, vt, m_ref, l_ref, acc, ho, hg, wout, res, hidden, xs, wgu, wd, stage, stage_d, hb, part, r1, r2, r3,
    q_sem, qo_sem, qr_sem, kx_sem, kf_sem, kv_sem,
    gs_sem, gr_sem, gp_sem, gq_sem, ds_sem, dr_sem, dp_sem, dq_sem,
    wx_sem, st_sem, hs_sem, hr_sem, in_sem, xz_sem, xs_sem, xr_sem, rs_sem, rr_sem,
):
    z, x = lax.axis_index("z"), lax.axis_index("x")
    y, c = lax.axis_index("y"), lax.axis_index("c")
    z0 = lax.rem(z, 2)
    tokens = q_ref.shape[0]
    wide = v_ref.shape[1] // nx
    own_rows, width = out_ref.shape
    depth = wg_ref.shape[0]
    units, quarter = wg_ref.shape[1], wgu.shape[3]
    tp = y * nc + c
    xo, co = 1 - x, 1 - c
    here = dict(z=z, x=x, y=y, c=c)

    def remote(src, dst, send, recv, **to):
        return pltpu.make_async_remote_copy(
            src_ref=src, dst_ref=dst, send_sem=send, recv_sem=recv,
            device_id={**here, **to}, device_id_type=pl.DeviceIdType.MESH,
        )

    def lanes(i, n):
        return pl.ds(pl.multiple_of(i * n, n), n)

    local_in = [
        pltpu.make_async_copy(wout_ref, wout, in_sem.at[0]),
        pltpu.make_async_copy(res_ref.at[lanes(tp, own_rows), :], res, in_sem.at[1]),
    ]
    for copy in local_in:
        copy.start()

    barrier = pltpu.get_barrier_semaphore()
    peers = [dict(z=lax.rem(z + a, nz), x=lax.rem(x + b, nx)) for a in range(nz) for b in range(nx) if a + b]
    peers += [
        dict(x=lax.rem(x + b, nx), y=lax.rem(y + e, ny), c=lax.rem(c + f, nc))
        for b in range(nx) for e in range(ny) for f in range(nc) if e + f
    ]
    peers += [dict(p, z=z + 1 - 2 * z0) for p in peers if "y" in p]
    for to in peers:
        pl.semaphore_signal(barrier, inc=1, device_id={**here, **to}, device_id_type=pl.DeviceIdType.MESH)
    pl.semaphore_wait(barrier, len(peers))

    start = lambda copy: copy.start()
    sent = lambda copy: copy.wait_send()

    def slot(zz, xx):
        return zz * nx + xx

    mine = slot(z, x)

    def swap(go):
        go(remote(q_ref.at[:, lanes(xo, wide)], q_all.at[x], q_sem.at[0], q_sem.at[1], x=xo))
        go(remote(k_ref.at[:, lanes(xo, wide)], kv.at[mine, 0], kx_sem.at[0], kv_sem.at[mine], x=xo))
        go(remote(v_ref.at[:, lanes(xo, wide)], kv.at[mine, 1], kx_sem.at[1], kv_sem.at[mine], x=xo))

    halves = nz // 2
    inner = z0 == jnp.where(z < nz // 2, 1, 0)
    outer = jnp.logical_not(inner)

    def half(g):
        return lax.rem(z // 2 + g, halves)

    def flow(e, g, go):
        s = slot(z, lax.rem(x + e, nx))
        zd = 2 * half(g) + jnp.where(2 * half(g) < nz // 2, 1, 0)
        if e or go is sent:
            go(remote(kv.at[s], kv.at[s], kf_sem.at[g, e], kv_sem.at[s], z=zd))
        else:
            for i, ref in enumerate((k_ref, v_ref)):
                go(remote(ref.at[:, lanes(x, wide)], kv.at[s, i], kf_sem.at[g, e], kv_sem.at[s], z=zd))

    def relay(e, go):
        s = slot(z + 1 - 2 * z0, lax.rem(x + e, nx))
        if go is start:
            remote(kv.at[s], kv.at[s], kx_sem.at[0], kv_sem.at[s], x=xo).wait_recv()
        for g in range(1, halves):
            zd = 2 * half(g) + jnp.where(2 * half(g) < nz // 2, 1, 0)
            go(remote(kv.at[s], kv.at[s], kf_sem.at[g, nx + e], kv_sem.at[s], z=zd))

    def ask(e, go):
        src = q_all.at[xo] if e else q_ref.at[:, lanes(x, wide)]
        go(remote(src, q_all.at[nx + (xo if e else x)], qo_sem.at[e], qr_sem.at[xo if e else x], z=z + 1 - 2 * z0))

    def swapped():
        remote(kv.at[slot(z, xo)], kv.at[slot(z, xo)], kx_sem.at[0], kv_sem.at[slot(z, xo)], x=xo).wait_recv()

    def offset(q):
        return pl.multiple_of(jnp.minimum(q * quarter, units - quarter), 128)

    near = [(0, 1, b) for b in range(nx)]
    far = [(g, t, b) for b in range(nx) for g in range(1, halves) for t in range(2)]

    def units_of(xd, t):
        return pl.ds(offset(xd * 2 + lax.rem(z0 + t, 2)), quarter)

    def aside(go):
        rows = lanes(mine, depth)
        for i, ref in enumerate((wg_ref, wu_ref)):
            go(remote(ref.at[:, units_of(xo, 0)], wgu.at[c, i, rows, :], wx_sem.at[0, i], gr_sem.at[mine], x=xo))
        for i, ref in enumerate((wg_ref, wu_ref)):
            go(remote(ref.at[:, units_of(xo, 1)], stage.at[i], wx_sem.at[1, i], st_sem.at[0], x=xo))
        go(remote(wd_ref.at[units_of(xo, 0), :], wd.at[c, :, rows], wx_sem.at[0, 2], dr_sem.at[mine], x=xo))
        go(remote(wd_ref.at[units_of(xo, 1), :], stage_d, wx_sem.at[1, 2], st_sem.at[1], x=xo))

    def gate_up(to, go):
        g, t, b = to
        s = slot(z, lax.rem(x + b, nx))
        rows = lanes(s, depth)
        for i, ref in enumerate((wg_ref, wu_ref)):
            src = stage.at[i] if b and t else wgu.at[c, i, rows, :] if b else ref.at[:, units_of(x, t)]
            zd = half(g) * 2 + lax.rem(z0 + t, 2)
            go(remote(src, wgu.at[c, i, rows, :], gs_sem.at[g, t, b, i], gr_sem.at[s], z=zd))

    def downward(to, go):
        g, t, b = to
        s = slot(z, lax.rem(x + b, nx))
        cols = lanes(s, depth)
        src = stage_d if b and t else wd.at[c, :, cols] if b else wd_ref.at[units_of(x, t), :]
        zd = half(g) * 2 + lax.rem(z0 + t, 2)
        go(remote(src, wd.at[c, :, cols], ds_sem.at[g, t, b], dr_sem.at[s], z=zd))

    def aside_came(last):
        rows = lanes(slot(z, xo), depth)
        early = (wgu.at[c, :, rows, :], gr_sem.at[slot(z, xo)]), (stage, st_sem.at[0])
        late = (wd.at[c, :, rows], dr_sem.at[slot(z, xo)]), (stage_d, st_sem.at[1])
        for block, sem in late if last else early:
            remote(block, block, wx_sem.at[0, 0], sem, x=xo).wait_recv()

    q_me = x * 2 + z0
    own_weights = [
        pltpu.make_async_copy(ref.at[:, pl.ds(offset(q_me), quarter)], wgu.at[c, i, lanes(mine, depth), :], in_sem.at[2 + i])
        for i, ref in enumerate((wg_ref, wu_ref))
    ]
    own_weights.append(
        pltpu.make_async_copy(wd_ref.at[pl.ds(offset(q_me), quarter), :], wd.at[c, :, lanes(mine, depth)], in_sem.at[4])
    )

    swap(start)

    @pl.when(outer)
    def _():
        ask(0, start)
        flow(0, 0, start)

    @pl.when(inner)
    def _():
        for g in range(1, halves):
            flow(0, g, start)

    for copy in own_weights:
        copy.start()

    remote(q_all.at[x], q_all.at[xo], q_sem.at[0], q_sem.at[1], x=xo).wait_recv()

    @pl.when(outer)
    def _():
        ask(1, start)

    swapped()
    aside(start)

    @pl.when(inner)
    def _():
        for g in range(1, halves):
            flow(1, g, start)

    @pl.when(outer)
    def _():
        flow(1, 0, start)
        for e in range(nx):
            flow(e, 0, sent)
        for to in near + far[:FIRST]:
            if to == near[1]:
                aside_came(False)
            gate_up(to, start)
            gate_up(to, sent)

    def attend(s, low, high):
        vt[...] = kv[s, 1].astype(jnp.float32).T.astype(jnp.bfloat16)

        def pair(h, _):
            both = [2 * h, 2 * h + 1]
            scores = [
                lax.dot_general(kv[s, 0], qm[i], (((1,), (1,)), ((), ())), preferred_element_type=jnp.float32)
                for i in both
            ]
            olds = [m_ref[i] for i in both]
            highs = [jnp.maximum(o, jnp.max(t, axis=0, keepdims=True)) for o, t in zip(olds, scores)]
            weights = [jnp.exp(t - g) for t, g in zip(scores, highs)]
            mixed = [jnp.dot(vt[...], w.astype(jnp.bfloat16), preferred_element_type=jnp.float32) for w in weights]
            for i, o, g, w, t in zip(both, olds, highs, weights, mixed):
                shrink = jnp.exp(o - g)
                l_ref[i] = l_ref[i] * shrink + jnp.sum(w, axis=0, keepdims=True)
                m_ref[i] = g
                acc[i] = acc[i] * shrink + t
            return 0

        lax.fori_loop(low, high, pair, 0)

    def turn(j):
        mixed = jnp.logical_and(j >= nx, j < 3 * nx) if nz > 2 else False
        k = jnp.where(mixed, 1 + lax.rem(j, 2), j // nx)
        e = jnp.where(mixed, (j - nx) // 2, lax.rem(j, nx))
        zz, _off = nearest(k, z, nz)
        return zz, slot(zz, lax.rem(x + e, nx))

    def ready(low):
        for h in range(low, low + nx):
            q = q_all[h].astype(jnp.float32) * HD**-0.5
            qm[2 * h] = jnp.where(first_map, q, 0.0).astype(jnp.bfloat16)
            qm[2 * h + 1] = jnp.where(first_map, 0.0, q).astype(jnp.bfloat16)

    first_map = lax.broadcasted_iota(jnp.int32, (tokens, 2 * HD), 1) < HD

    def step(n, _):
        j = jnp.where(n < 2 * nx, lax.rem(n, nx), n - nx)
        zz, s = turn(j)

        @pl.when(n == nx)
        def _():
            for e in range(nx):
                remote(q_all.at[0], q_all.at[0], qo_sem.at[0], qr_sem.at[e], x=xo).wait_recv()
            ready(nx)

        for e in range(nx):
            @pl.when(n == nx + e)
            def _():
                relay(e, start)

        @pl.when(zz // 2 != z // 2)
        def _():
            remote(kv.at[s], kv.at[s], kx_sem.at[0], kv_sem.at[s], x=xo).wait_recv()

        def issue(at, some):
            @pl.when(j == min(at, nz * nx - 1))
            def _():
                for to in some:
                    gate_up(to, start)

        issue(2, near[:1])

        @pl.when(j == min(4, nz * nx - 1))
        def _():
            for e in range(nx):
                relay(e, sent)

        issue(4, [to for to in far if to[1:] == (1, 0)])

        @pl.when(j == min(5, nz * nx - 1))
        def _():
            aside_came(False)

        issue(5, near[1:])
        issue(6, [to for to in far if to[1:] == (1, 1)])
        attend(s, jnp.where(jnp.logical_and(n >= nx, n < 2 * nx), nx, 0), jnp.where(n < nx, nx, 2 * nx))
        return 0

    head = tp * nx + x
    me = (x * ny + y) * nc + c

    def spread(go):
        for b in range(nx):
            for e in range(ny):
                for f in range(nc):
                    xd, yd, cd = lax.rem(x + b, nx), lax.rem(y + e, ny), lax.rem(c + f, nc)
                    for p in range(0 if b + e + f else 1, 2):
                        n = ((b * ny + e) * nc + f) * 2 + p
                        src = ho.at[p * nx + xd, lanes(yd * nc + cd, own_rows), :]
                        zd = z + p * (1 - 2 * z0)
                        go(remote(src, hg.at[:, lanes(head, wide)], hs_sem.at[n], hr_sem.at[me], z=zd, x=xd, y=yd, c=cd))

    @pl.when(inner)
    def _():
        kv[mine, 0] = k_ref[:, lanes(x, wide)]
        kv[mine, 1] = v_ref[:, lanes(x, wide)]
        q_all[x] = q_ref[:, lanes(x, wide)]
        m_ref[...] = jnp.full_like(m_ref, -jnp.inf)
        l_ref[...] = jnp.zeros_like(l_ref)
        acc[...] = jnp.zeros_like(acc)
        ready(0)
        lax.fori_loop(0, nz * nx + nx, step, 0)

        def finish(h, _):
            first = acc[2 * h] / l_ref[2 * h]
            second = acc[2 * h + 1] / l_ref[2 * h + 1]
            differ = first - lam_ref[x] * second
            scale = lax.rsqrt(jnp.mean(differ * differ, axis=0, keepdims=True) + 1e-05)
            ho[h] = (differ * scale * gain_ref[...]).T.astype(jnp.bfloat16)
            return 0

        lax.fori_loop(0, 2 * nx, finish, 0)
        spread(start)
        hg[:, lanes(head, wide)] = ho[x, lanes(tp, own_rows), :]

    for copy in local_in:
        copy.wait()
    for b in range(nx):
        for e in range(ny):
            for f in range(nc):
                xd, yd, cd = lax.rem(x + b, nx), lax.rem(y + e, ny), lax.rem(c + f, nc)
                other = (xd * ny + yd) * nc + cd
                block = hg.at[:, lanes((yd * nc + cd) * nx + xd, wide)]

                def came():
                    remote(block, block, hs_sem.at[0], hr_sem.at[other], x=xo).wait_recv()

                if b + e + f:
                    came()
                else:
                    pl.when(outer)(came)

    state = res[...].astype(jnp.float32) + jnp.dot(hg[...], wout[...], preferred_element_type=jnp.float32)
    hidden[...] = state.astype(jnp.bfloat16)
    stream = hidden[...].astype(jnp.float32)
    scaled = stream * lax.rsqrt(jnp.mean(stream * stream, axis=1, keepdims=True) + 1e-05)
    cube = z0 * 4 + x * 2 + y
    xs[cube] = (scaled * norm_ref[...]).astype(jnp.bfloat16)

    bits = dict(z=(z0, 4), x=(x, 2), y=(y, 1))
    across = dict(z=dict(z=z + 1 - 2 * z0), x=dict(x=xo), y=dict(y=1 - y))
    paths = (("x", "y"), ("y", "x"))
    split = width // 256 * 128
    columns = (pl.ds(0, split), pl.ds(split, width - split))

    def flip(axis):
        bit, mask = bits[axis]
        return (1 - 2 * bit) * mask

    over = cube + flip("z")

    def lend(p, go):
        block = xs.at[cube, :, columns[p]]
        go(remote(block, block, xz_sem.at[p, 0], xz_sem.at[p, 1], **across["z"]))

    def gather(h, p, k, go):
        held = [(cube, over)[h]]
        if k:
            held += [held[0] + flip(paths[p][0])]
        for n, i in enumerate(held):
            block = xs.at[i, :, columns[p]]
            go(remote(block, block, xs_sem.at[h, p, k, n], xr_sem.at[h, p, k], **across[paths[p][k]]))

    def gathered(h, p, k):
        block = xs.at[pl.ds(0, 2**k), :, columns[p]]
        remote(block, block, xs_sem.at[h, p, k, 0], xr_sem.at[h, p, k], x=xo).wait_recv()

    for p in range(2):
        lend(p, start)
        gather(0, p, 0, start)

    @pl.when(outer)
    def _():
        for to in far[FIRST:]:
            gate_up(to, start)

    for p in range(2):
        gathered(0, p, 0)
        gather(0, p, 1, start)

    @pl.when(inner)
    def _():
        for to in far:
            if to[1] == 0:
                gate_up(to, start)

    for p in range(2):
        block = xs.at[over, :, columns[p]]
        remote(block, block, xz_sem.at[p, 0], xz_sem.at[p, 1], x=xo).wait_recv()
        gather(1, p, 0, start)
    for p in range(2):
        gathered(1, p, 0)
        gather(1, p, 1, start)
    def pass_on(s, go):
        block = wgu.at[c, :, lanes(s, depth), :]
        go(remote(block, block, gp_sem.at[s], gq_sem.at[s], c=co))

    def fill(j, _):
        s = lax.rem(z * nx + jnp.where(z < nz // 2, j, nx - 1 - j + nz * nx), nz * nx)

        @pl.when(s // nx != z)
        def _():
            block = wgu.at[c, :, lanes(s, depth), :]
            remote(block, block, gp_sem.at[s], gr_sem.at[s], c=co).wait_recv()

        pass_on(s, start)
        return 0

    def filled(s, _):
        block = wgu.at[co, :, lanes(s, depth), :]
        remote(block, block, gp_sem.at[s], gq_sem.at[s], c=co).wait_recv()
        return 0

    aside_came(True)

    @pl.when(outer)
    def _():
        for to in far[FIRST:]:
            gate_up(to, sent)
        for to in near + [to for to in far if to[1] == 0] + [to for to in far if to[1]]:
            downward(to, start)

    @pl.when(inner)
    def _():
        for to in far:
            if to[1]:
                downward(to, start)

    for copy in own_weights:
        copy.wait()
    lax.fori_loop(0, nz * nx, fill, 0)
    @pl.when(inner)
    def _():
        for to in near + far:
            gate_up(to, sent)
        for to in near + [to for to in far if to[1] == 0]:
            downward(to, start)

    lax.fori_loop(0, nz * nx, filled, 0)
    for h in range(2):
        for p in range(2):
            gathered(h, p, 1)

    blocks, group = 8, 4
    rows = group * own_rows
    spare = q_me * quarter - jnp.minimum(q_me * quarter, units - quarter)
    keep = lax.broadcasted_iota(jnp.int32, (rows, quarter), 1) >= spare

    def expand(i, _):
        both = xs[pl.ds(group * i, group)].reshape(rows, width)
        for cc in range(nc):
            gate = jnp.dot(both, wgu[cc, 0], preferred_element_type=jnp.float32)
            up = jnp.dot(both, wgu[cc, 1], preferred_element_type=jnp.float32)
            made = gate / (1.0 + jnp.exp(-gate)) * up
            hb[lanes(i, rows), cc * quarter : (cc + 1) * quarter] = jnp.where(keep, made, 0.0).astype(jnp.bfloat16)
        return 0

    lax.fori_loop(0, blocks // group, expand, 0)
    def place(p, flips):
        return cube + sum(flip(axis) for axis in flips)

    def choices(axes):
        sets = [()]
        for axis in axes:
            sets = sets + [t + (axis,) for t in sets]
        return sets

    held_in = (r1, r2, r3)
    spare_z = (("x", "y", "z"), ("y", "x", "z"))
    even = (("x", "y", "z"), ("y", "z", "x"), ("z", "x", "y"))
    orders = [even if g == halves - 1 else spare_z for g in range(halves)]
    span = width // halves
    tiles = span // 128
    cuts = [[0] + [128 * ((tiles * (i + 1) + len(o) - 1) // len(o)) for i in range(len(o))] for o in orders]

    def share(g, p):
        return pl.ds(pl.multiple_of(half(g) * span + cuts[g][p], 128), cuts[g][p + 1] - cuts[g][p])

    def down_on(s, go):
        block = wd.at[c, :, lanes(s, depth)]
        go(remote(block, block, dp_sem.at[s], dq_sem.at[s], c=co))

    def down_fill(g):
        def one(n, _):
            s = half(g) * 2 * nx + n

            @pl.when(s // nx != z)
            def _():
                block = wd.at[c, :, lanes(s, depth)]
                remote(block, block, dp_sem.at[s], dr_sem.at[s], c=co).wait_recv()

            down_on(s, start)
            return 0

        def other(n, _):
            s = half(g) * 2 * nx + n
            block = wd.at[co, :, lanes(s, depth)]
            remote(block, block, dp_sem.at[s], dq_sem.at[s], c=co).wait_recv()
            return 0

        lax.fori_loop(0, 2 * nx, one, 0)
        lax.fori_loop(0, 2 * nx, other, 0)

    def reduce_send(g, p, k, go):
        axis, rest = orders[g][p][k], orders[g][p][k + 1 :]
        for n, t in enumerate(choices(rest)):
            spot = sum((bits[a][0] if a not in t else 1 - bits[a][0]) * 2**i for i, a in enumerate(rest))
            src = part.at[place(p, t + (axis,)), :, share(g, p)]
            dst = held_in[k].at[spot, :, share(g, p)]
            go(remote(src, dst, rs_sem.at[g, p, k, n], rr_sem.at[g, p, k], **across[axis]))

    def reduce_take(g, p, k):
        axis, rest = orders[g][p][k], orders[g][p][k + 1 :]
        cols = share(g, p)
        block = held_in[k].at[:, :, cols]
        remote(block, block, rs_sem.at[g, p, k, 0], rr_sem.at[g, p, k], x=xo).wait_recv()
        for t in reversed(choices(rest)) if rest else ():
            spot = sum((bits[a][0] if a not in t else 1 - bits[a][0]) * 2**i for i, a in enumerate(rest))
            i = place(p, t)
            part[i, :, cols] = (
                part[i, :, cols].astype(jnp.float32) + held_in[k][spot, :, cols].astype(jnp.float32)
            ).astype(jnp.bfloat16)
        if not rest:
            out_ref[:, cols] = (
                hidden[:, cols].astype(jnp.float32)
                + part[cube, :, cols].astype(jnp.float32)
                + held_in[k][0, :, cols].astype(jnp.float32)
            ).astype(jnp.bfloat16)

    for g in range(halves):
        down_fill(g)
        for p in range(len(orders[g])):
            def contract(i, _):
                weights = wd[:, :, share(g, p)].reshape(nc * quarter, cuts[g][p + 1] - cuts[g][p])
                made = jnp.dot(hb[lanes(i, rows), :], weights, preferred_element_type=jnp.float32)
                part[pl.ds(group * i, group), :, share(g, p)] = made.astype(jnp.bfloat16).reshape(group, own_rows, -1)
                return 0

            lax.fori_loop(0, blocks // group, contract, 0)
            reduce_send(g, p, 0, start)
        if g:
            for p in range(len(orders[g - 1])):
                reduce_take(g - 1, p, 1)
                reduce_send(g - 1, p, 2, start)
        for p in range(len(orders[g])):
            reduce_take(g, p, 0)
            reduce_send(g, p, 1, start)
    for p in range(len(orders[halves - 1])):
        reduce_take(halves - 1, p, 1)
        reduce_send(halves - 1, p, 2, start)
    for g in range(halves):
        for p in range(len(orders[g])):
            reduce_take(g, p, 2)

    swap(sent)

    @pl.when(outer)
    def _():
        for e in range(nx):
            ask(e, sent)

    @pl.when(inner)
    def _():
        for e in range(nx):
            for g in range(1, halves):
                flow(e, g, sent)
        spread(sent)

    aside(sent)
    for to in near + far:
        downward(to, sent)
    for p in range(2):
        lend(p, sent)
        for h in range(2):
            for k in range(2):
                gather(h, p, k, sent)
    for k in range(3):
        for g in range(halves):
            for p in range(len(orders[g])):
                reduce_send(g, p, k, sent)

    def passed(s, _):
        pass_on(s, sent)
        down_on(s, sent)
        return 0

    lax.fori_loop(0, nz * nx, passed, 0)


def layer(
    nz, nx, ny, nc, residual, queries, key_pairs, values, lambdas, head_gain, w_out, norm_gain, w_gate, w_up, w_down
):
    tokens = queries.shape[0]
    wide = head_gain.shape[0]
    width = residual.shape[1]
    depth, units = w_gate.shape
    own_rows = tokens // (ny * nc)
    quarter = -(-units // (2 * nx * 128)) * 128
    vmem = pl.BlockSpec(memory_space=pltpu.VMEM)
    hbm = pl.BlockSpec(memory_space=pl.ANY)
    dma = pltpu.SemaphoreType.DMA
    bf16 = lambda *shape: pltpu.VMEM(shape, jnp.bfloat16)
    f32 = lambda *shape: pltpu.VMEM(shape, jnp.float32)
    n = nz * nx
    return pl.pallas_call(
        functools.partial(layer_kernel, nz, nx, ny, nc),
        out_shape=jax.ShapeDtypeStruct((own_rows, width), jnp.bfloat16),
        in_specs=[pl.BlockSpec(memory_space=pltpu.SMEM)] + [vmem] * 5 + [hbm] * 5,
        out_specs=vmem,
        scratch_shapes=[
            bf16(2 * nx, tokens, wide), bf16(4 * nx, tokens, wide), bf16(n, 2, tokens, wide), bf16(wide, tokens),
            f32(4 * nx, 1, tokens), f32(4 * nx, 1, tokens), f32(4 * nx, wide, tokens),
            bf16(2 * nx, tokens, wide), bf16(own_rows, w_out.shape[0]),
            bf16(*w_out.shape), bf16(own_rows, width), bf16(own_rows, width),
            bf16(8, own_rows, width), bf16(nc, 2, width, quarter), bf16(nc, quarter, width),
            bf16(2, depth, quarter), bf16(quarter, depth),
            bf16(8 * own_rows, nc * quarter), bf16(8, own_rows, width),
            bf16(4, own_rows, width), bf16(2, own_rows, width), bf16(1, own_rows, width),
            dma((2,)), dma((nx,)), dma((nx,)), dma((2,)), dma((nz // 2, 2 * nx)), dma((n,)),
            dma((nz // 2, 2, nx, 2)), dma((n,)), dma((n,)), dma((n,)),
            dma((nz // 2, 2, nx)), dma((n,)), dma((n,)), dma((n,)),
            dma((2, 3)), dma((2,)), dma((2 * nx * ny * nc,)), dma((nx * ny * nc,)), dma((5,)),
            dma((2, 2)), dma((2, 2, 2, 2)), dma((2, 2, 2)), dma((nz // 2, 3, 3, 4)), dma((nz // 2, 3, 3)),
        ],
        compiler_params=pltpu.CompilerParams(
            collective_id=2, has_side_effects=True, vmem_limit_bytes=62 * 1024 * 1024
        ),
        name="layer",
    )(
        lambdas, queries, key_pairs, values, head_gain.reshape(wide, 1), norm_gain.reshape(1, width),
        residual, w_out, w_gate, w_up, w_down,
    )


def solution(mesh):
    sp, tp = mesh.shape["sp"], mesh.shape["tp"]
    coords = [getattr(d, "coords", None) for d in mesh.devices.flat]
    known = all(p is not None for p in coords)
    nx = len({p[0] for p in coords}) if known else 2
    ny = len({p[1] for p in coords}) if known else 2
    if sp % nx:
        nx = 1
    if tp % ny:
        ny = 1
    nz, nc = sp // nx, tp // ny
    zx, yc = ("z", "x"), ("y", "c")

    def placed(tp_axes):
        split = P(zx, tp_axes)
        return (P(zx, None), split, split, split, P(tp_axes), P(), P(), P(), split, split, P(tp_axes, zx))

    def run(*args):
        heads, units = args[4].shape[0], args[8].shape[1] // tp
        if nx == ny == nc == 2 and nz % 2 == 0 and heads == tp * nx and units % 128 == 0:
            box = Mesh(np.asarray(mesh.devices).reshape(nz, nx, ny, nc), ("z", "x", "y", "c"))
            body, tp_axes = functools.partial(layer, nz, nx, ny, nc), yc
        else:
            box = Mesh(np.asarray(mesh.devices).reshape(nz, nx, tp), ("z", "x", "tp"))
            body, tp_axes = functools.partial(per_device, nz, nx), ("tp",)
        return jax.shard_map(
            body, mesh=box, in_specs=placed(tp_axes), out_specs=P(zx + tp_axes, None), check_vma=False
        )(*args)

    return run
```
